256 devices in a mesh: sp: 32 (over z, x), tp: 8 (over y, core).
Axes of the slice: x: 4, y: 4, z: 8, core: 2. Of those that a mesh axis runs over, the one named last changes fastest.
Arguments:
- resid: bfloat16 [12288, 2048], P('sp'), may hold values from -6 to 6
- cotangent: bfloat16 [12288, 2048], P('sp'), may hold values from -0.59765625 to 0.59765625
- routes: int32 [12288, 2], P('sp'), may hold values from 0 to 31, all different within a row; in each aligned block of 384 rows (0 to 383, 384 to 767, ...) at most 48 rows name the same one
- route_weight: float32 [12288, 2], P('sp'), may hold values from 0.3 to 2.2
- w_gate: bfloat16 [32, 2048, 1024], P('sp', None, 'tp'), may hold values from -0.125 to 0.125
- w_up: bfloat16 [32, 2048, 1024], P('sp', None, 'tp'), may hold values from -0.125 to 0.125
- w_down: bfloat16 [32, 1024, 2048], P('sp', 'tp'), may hold values from -0.1875 to 0.1875
- out_proj: bfloat16 [2048, 2816], P(None, 'tp'), may hold values from -0.109375 to 0.109375
- gate_pre: bfloat16 [12288, 2816], P('sp', 'tp'), may hold values from -8 to 8
- log_decay: float32 [12288, 2816], P('sp', 'tp'), may hold values from -1 to 0
- state_before: float32 [12288, 2816], P('sp', 'tp'), may hold values from -6 to 6
- step_input: bfloat16 [12288, 2816], P('sp', 'tp'), may hold values from -6 to 6
Outputs:
- grad_gate: float32 [32, 2048, 1024], P('sp', None, 'tp')
- grad_up: float32 [32, 2048, 1024], P('sp', None, 'tp')
- grad_down: float32 [32, 1024, 2048], P('sp', 'tp')
- grad_proj: float32 [2048, 2816], P('sp', 'tp')
- grad_gate_pre: bfloat16 [12288, 2816], P('sp', 'tp')
- grad_step_input: float32 [12288, 2816], P('sp', 'tp')
- grad_log_decay: float32 [12288, 2816], P('sp', 'tp')
The draws below stay inside these ranges and needn't reach their ends.
Inputs may be any that keep to these rules, and one draw needn't show every extreme that they name: `routes`: each row names 2 different experts. In the rows of one device no expert is named more than 48 times; some expert is named exactly 48 times in the rows of some devices.
All inputs are finite; a program needn't handle non-finite values.
Results may differ from the reference program's by a relative error of at most 0.02.
Values may be sent and summed in bfloat16 or wider, within the bound.
No kernel may reach another device: no remote copies, remote signals or barrier semaphores. Data moves between devices by JAX's collectives and lax.ppermute only.
A program may use at most 128 MiB of HBM per device.

```python
import math
import jax
import jax.numpy as jnp
import numpy as np
from jax import lax

D = 2048
HEADS = 32
HEAD_DIM = 88
FE = 1024
TOP = 2
TOK_DEV = 384
STATE_CHANNELS = 2816
SEQUENCE_TOKENS = 12288
EXPERTS = 32
CAP = 48
N_SP = 32
N_TP = 8


def draw_log_decay(key, part):
    random_subkeys = jax.random.split(jax.random.fold_in(key, 17), 7)
    head_fast_prob = 0.5
    is_fast = jax.random.bernoulli(random_subkeys[0], head_fast_prob, (HEADS,))
    is_fast = jnp.repeat(is_fast, HEAD_DIM)
    slow_rate = jnp.exp(jax.random.uniform(random_subkeys[1], (STATE_CHANNELS,), jnp.float32, -0.69, 0.0)) * (0.15 / SEQUENCE_TOKENS)
    fast_rate = jax.random.uniform(random_subkeys[2], (STATE_CHANNELS,), jnp.float32, 1.0 / 50.0, 1.0 / 30.0)
    decay_rates = jnp.where(is_fast, fast_rate, slow_rate)
    jagged_level = jnp.exp(jax.random.uniform(random_subkeys[3], (SEQUENCE_TOKENS, STATE_CHANNELS), jnp.float32, -0.7, 0.7))
    block_multiplier = jnp.exp(jax.random.uniform(random_subkeys[4], (SEQUENCE_TOKENS // TOK_DEV, 1), jnp.float32, -0.69, 0.69))
    block_multiplier = jnp.repeat(block_multiplier, TOK_DEV, axis=0)
    spike_location = jax.random.randint(random_subkeys[5], (3,), 0, SEQUENCE_TOKENS)
    token_position = jnp.arange(SEQUENCE_TOKENS, dtype=jnp.int32)
    spike_flag = jnp.any(token_position[:, None] == spike_location[None, :], axis=1)
    spike_penalty = jax.random.uniform(random_subkeys[6], (SEQUENCE_TOKENS, STATE_CHANNELS), jnp.float32, 0.22, 0.69)
    return -(decay_rates[None, :] * jagged_level * block_multiplier) - jnp.where(spike_flag[:, None], spike_penalty, 0.0)


def with_spikes(drawn, own_key, source, target, shards_of, factor):
    def block_of(axis_at):
        return (jnp.arange(drawn.shape[axis_at]) // (drawn.shape[axis_at] // shards_of)).reshape((-1,) + (1,) * (drawn.ndim - 1 - axis_at))

    one_side = jax.random.permutation(own_key, shards_of)[block_of(target)]
    far = (block_of(target) + shards_of // 2) % shards_of
    return jnp.where((block_of(source) == one_side) | (block_of(source) == far), factor * drawn, drawn)


def steps_of(stream_key, extent, cuts, least, high):
    level = 1.0
    for dim, blocks in cuts:
        heights = jax.random.uniform(jax.random.fold_in(jax.random.fold_in(stream_key, 6), dim), (blocks,), jnp.float32, least / len(cuts), high / len(cuts))
        level = level * jnp.repeat(jnp.exp(heights), extent[dim] // blocks).reshape((-1,) + (1,) * (len(extent) - 1 - dim))
    return level


def shared_out(key, own, number, rows, number_of, top, bound, skew):
    order = jax.random.permutation(key, number_of)
    crowded, usual = portions_of(number_of, rows * top, bound, skew, True), portions_of(number_of, rows * top, bound, skew, False)
    places = jnp.arange(number_of)

    def named(tallies, turn):
        used = int((tallies > 0).sum())
        fixed = max(1, used // 4)
        moved = fixed + (places - fixed + turn * (used - fixed)) % max(1, number_of - fixed)
        return jnp.zeros((number_of,), jnp.int32).at[order[jnp.where(places < fixed, places, moved)]].set(jnp.asarray(tallies, jnp.int32))

    tallies = jnp.where(number % 4 == 0, named(crowded, number // 4), named(usual, number - number // 4 - 1))
    mixed = jax.random.permutation(jax.random.fold_in(own, 3), number_of)
    donor, taker = mixed[0:number_of // 2 * 2:2], mixed[1:number_of // 2 * 2:2]
    margin = jnp.minimum(tallies[donor] - 1, bound - tallies[taker]) // 2
    margin = jnp.where((donor == order[0]) | (taker == order[0]) | (tallies[taker] == 0), 0, jnp.maximum(margin, 0))
    moved = jax.random.randint(jax.random.fold_in(own, 4), (number_of // 2,), 0, 1 << 20) % (margin + 1)
    tallies = tallies.at[donor].add(-moved).at[taker].add(moved)
    items = jnp.searchsorted(jnp.cumsum(tallies), jnp.arange(rows * top), side="right").astype(jnp.int32)
    grid = items.reshape(top, rows).T
    grid = grid[jax.random.permutation(jax.random.fold_in(own, 1), rows)]
    turn = jax.random.randint(jax.random.fold_in(own, 2), (rows, 1), 0, top)
    return jnp.take_along_axis(grid, (jnp.arange(top)[None, :] + turn) % top, axis=1)


def portions_of(number_of, total, bound, skew, full):
    loads = [(1 << 20) // math.isqrt(standing ** skew) + 1 for standing in range(1, number_of + 1)]
    largest = bound if full else min(bound, max(-(-total // number_of), total * loads[0] // sum(loads)))
    least = 1 if total - largest >= number_of - 1 else 0
    counts, spare = [largest] + [least] * (number_of - 1), total - largest - least * (number_of - 1)
    while spare > 0:
        free = [i for i in range(1, number_of) if counts[i] < largest] or [i for i in range(1, number_of) if counts[i] < bound]
        mass, budget = sum([loads[i] for i in free]), spare
        for i in free:
            more = min(bound - counts[i], max(1, budget * loads[i] // mass), spare)
            counts[i] = counts[i] + more
            spare = spare - more
    return np.array(counts)


def centred(key, extent, width, bound, pieces=(), held_as=jnp.bfloat16):
    entries = jax.random.normal(key, extent, jnp.float32) * width
    if len(pieces) > 0:
        entries = steps_of(key, extent, pieces, -0.22, 0.18) * entries
    return jnp.clip(entries, min=-bound, max=bound).astype(held_as)


def heavy_noise(own_key, extent, width, limit, pieces, heavy, held_as=jnp.bfloat16):
    result = width * jax.random.normal(own_key, extent, jnp.float32)
    if pieces:
        result = result * steps_of(own_key, extent, pieces, -0.22, 0.18)
    return jnp.clip(with_spikes(result, jax.random.fold_in(own_key, 3), *heavy), -limit, limit).astype(held_as)


def setup_inputs(seed: int = 0) -> dict:
    splits = jax.random.split(jax.random.key(seed), 13)
    resid = centred(splits[0], (SEQUENCE_TOKENS, D), 1.0, 6.0, ((0, 32),))
    cotangent = heavy_noise(splits[1], (SEQUENCE_TOKENS, D), 0.1, 0.59765625, ((0, 32),), (0, 1, 32, 2.75))
    routes_keys = jax.random.split(jax.random.fold_in(splits[2], 1), SEQUENCE_TOKENS // TOK_DEV)
    routes_turns = jax.random.permutation(jax.random.fold_in(splits[2], 3), SEQUENCE_TOKENS // TOK_DEV)
    routes = jax.vmap(lambda own, number: shared_out(jax.random.fold_in(splits[2], 2), own, number, TOK_DEV, EXPERTS, TOP, CAP, 2))(routes_keys, routes_turns).reshape((SEQUENCE_TOKENS, TOP))
    route_weight = jnp.clip(jnp.exp(math.log(2.2) - 1.9924301 * jax.random.uniform(splits[3], (SEQUENCE_TOKENS, TOP), jnp.float32) ** steps_of(splits[3], (SEQUENCE_TOKENS, TOP), ((0, 32),), -0.2, 0.2)), 0.3, 2.2)
    w_gate = centred(splits[4], (EXPERTS, D, FE), D ** -0.5, 0.125, ((0, 32), (2, 8)))
    w_up = centred(splits[5], (EXPERTS, D, FE), D ** -0.5, 0.125, ((0, 32), (2, 8)))
    w_down = centred(splits[6], (EXPERTS, FE, D), FE ** -0.5, 0.1875, ((0, 32), (1, 8)))
    out_proj = centred(splits[7], (D, STATE_CHANNELS), STATE_CHANNELS ** -0.5, 0.109375, ((1, 8),))
    gate_pre = centred(splits[8], (SEQUENCE_TOKENS, STATE_CHANNELS), 1.5, 8.0, ((0, 32), (1, 8)))
    log_decay = draw_log_decay(jax.random.fold_in(splits[12], 71), 0)
    state_before = centred(splits[10], (SEQUENCE_TOKENS, STATE_CHANNELS), 1.0, 6.0, ((0, 32), (1, 8)), jnp.float32)
    step_input = centred(splits[11], (SEQUENCE_TOKENS, STATE_CHANNELS), 1.0, 6.0, ((0, 32), (1, 8)))
    return {"resid": resid, "cotangent": cotangent, "routes": routes, "route_weight": route_weight, "w_gate": w_gate, "w_up": w_up, "w_down": w_down, "out_proj": out_proj, "gate_pre": gate_pre, "log_decay": log_decay, "state_before": state_before, "step_input": step_input}


def slot_table(routes, route_weight):
    flat_ids = routes.reshape(N_SP, TOK_DEV * TOP)
    onehot = (flat_ids[:, :, None] == jnp.arange(EXPERTS, dtype=jnp.int32)[None, None, :]).astype(jnp.int32)
    ranking = lax.optimization_barrier(jnp.sum((jnp.cumsum(onehot, axis=1) - onehot) * onehot, axis=2)).reshape(-1)
    expert_ids = routes.reshape(-1)
    token_ids = jnp.arange(SEQUENCE_TOKENS * TOP, dtype=jnp.int32) // TOP
    block_ids = token_ids // TOK_DEV
    slot_token = jnp.full((EXPERTS, N_SP, CAP), SEQUENCE_TOKENS, jnp.int32).at[expert_ids, block_ids, ranking].set(token_ids)
    slot_weight = jnp.zeros((EXPERTS, N_SP, CAP), jnp.float32).at[expert_ids, block_ids, ranking].set(route_weight.reshape(-1))
    return (slot_token, slot_weight)

def one_expert(operands):
    token_ids, weights, resid_pad, cot_pad, gate_w, up_w, down_w = operands
    in_rows = resid_pad[token_ids]
    cot_rows = (weights[:, None] * cot_pad[token_ids].astype(jnp.float32)).astype(jnp.bfloat16)
    gate_act = jnp.dot(in_rows, gate_w, preferred_element_type=jnp.float32)
    up_act = jnp.dot(in_rows, up_w, preferred_element_type=jnp.float32)
    sigmoid_a = jax.nn.sigmoid(gate_act)
    hidden = (jax.nn.silu(gate_act) * up_act).astype(jnp.bfloat16)
    grad_down = jnp.dot(hidden.T, cot_rows, preferred_element_type=jnp.float32)
    d_hidden = jnp.dot(cot_rows, down_w.T, preferred_element_type=jnp.float32)
    slope = sigmoid_a * (1.0 + gate_act * (1.0 - sigmoid_a))
    d_gate_act = (d_hidden * up_act * slope).astype(jnp.bfloat16)
    d_up_act = (d_hidden * jax.nn.silu(gate_act)).astype(jnp.bfloat16)
    grad_gate = jnp.dot(in_rows.T, d_gate_act, preferred_element_type=jnp.float32)
    grad_up = jnp.dot(in_rows.T, d_up_act, preferred_element_type=jnp.float32)
    row_count = in_rows.shape[0]
    group = FE // N_TP
    parts = jnp.einsum('rpf,dpf->prd', d_gate_act.reshape(row_count, N_TP, group).astype(jnp.float32), gate_w.reshape(D, N_TP, group).astype(jnp.float32))
    parts = parts + jnp.einsum('rpf,dpf->prd', d_up_act.reshape(row_count, N_TP, group).astype(jnp.float32), up_w.reshape(D, N_TP, group).astype(jnp.float32))
    rounded = lax.optimization_barrier(parts.astype(jnp.bfloat16))
    expert_grad = lax.optimization_barrier(jnp.sum(rounded.astype(jnp.float32), axis=0)).astype(jnp.bfloat16)
    return (grad_gate, grad_up, grad_down, expert_grad)

def reverse_link(former, latter):
    return (former[0] * latter[0], latter[0] * former[1] + latter[1])

def reference(resid, cotangent, routes, route_weight, w_gate, w_up, w_down, out_proj, gate_pre, log_decay, state_before, step_input):
    slot_token, slot_weight = slot_table(routes, route_weight)
    resid_pad = jnp.concatenate([resid, jnp.zeros((1, D), jnp.bfloat16)], axis=0)
    cot_pad = jnp.concatenate([cotangent, jnp.zeros((1, D), jnp.bfloat16)], axis=0)

    def per_expert(operands):
        token_ids, weights, gate_w, up_w, down_w = operands
        return one_expert((token_ids.reshape(-1), weights.reshape(-1), resid_pad, cot_pad, gate_w, up_w, down_w))
    grad_gate, grad_up, grad_down, expert_grad = lax.map(per_expert, (slot_token, slot_weight, w_gate, w_up, w_down))
    routed = jnp.zeros((SEQUENCE_TOKENS + 1, D), jnp.float32).at[slot_token.reshape(-1)].add(expert_grad.reshape(-1, D).astype(jnp.float32))[:SEQUENCE_TOKENS]
    resid_grad = (cotangent.astype(jnp.float32) + routed).astype(jnp.bfloat16)
    decays = jnp.exp(log_decay)
    states = decays * state_before + step_input.astype(jnp.float32)
    gelu_val, gelu_back = jax.vjp(jax.nn.gelu, gate_pre.astype(jnp.float32))
    mixed = (gelu_val * states).astype(jnp.bfloat16)
    d_mixed = jnp.dot(resid_grad, out_proj, preferred_element_type=jnp.float32)
    grad_gate_pre = gelu_back(d_mixed * states)[0].astype(jnp.bfloat16)
    grad_proj = jnp.dot(resid_grad.T, mixed, preferred_element_type=jnp.float32)
    direct = d_mixed * gelu_val
    following = jnp.concatenate([decays[1:], jnp.zeros((1, STATE_CHANNELS), jnp.float32)], axis=0)
    scanned = lax.associative_scan(reverse_link, (jnp.flip(following, 0), jnp.flip(direct, 0)), axis=0)
    grad_step_input = jnp.flip(scanned[1], 0)
    grad_log_decay = grad_step_input * decays * state_before
    return (grad_gate, grad_up, grad_down, grad_proj, grad_gate_pre, grad_step_input, grad_log_decay)
```

```python
import functools

import jax
import jax.numpy as jnp
from jax import lax
from jax.experimental import pallas as pl
from jax.experimental.pallas import tpu as pltpu
from jax.sharding import Mesh, PartitionSpec as P


BF16 = jnp.bfloat16
F32 = jnp.float32
SP = ("z", "x")
TP = ("y", "c")
ALL = ("z", "x", "y", "c")

TOK = 384
D = 2048
CAP = 48
N_EXP = 32
N_TP = 8
PART = CAP // N_TP
ROWS = N_EXP * PART
CH = 352
GELU_C = 0.7978845608028654
GELU_A = 0.044715


def iota(shape, dim):
    return lax.broadcasted_iota(jnp.int32, shape, dim)


def dot(a, b):
    return jnp.dot(a, b, preferred_element_type=F32)


def dot_nt(a, b):
    return lax.dot_general(a, b, (((1,), (1,)), ((), ())), preferred_element_type=F32)


def dot_tn(a, b):
    return lax.dot_general(a, b, (((0,), (0,)), ((), ())), preferred_element_type=F32)


FIRST = (6, 4, 2)


def dispatch_kernel(tp_ref, routes_ref, weight_ref, res_a, res_b, cot_a, cot_b, out_ref, pick_ref, scale_ref):
    @pl.when(pl.program_id(0) == 0)
    def _():
        r0, r1 = routes_ref[0:1, :], routes_ref[1:2, :]
        e = iota((N_EXP, TOK), 0)
        oh0, oh1 = e == r0, e == r1
        member = jnp.where(oh0 | oh1, 1.0, 0.0).astype(BF16)
        before = jnp.where(iota((TOK, TOK), 0) < iota((TOK, TOK), 1), 1.0, 0.0).astype(BF16)
        rank = dot(member, before)
        s0 = r0 * CAP + jnp.sum(jnp.where(oh0, rank, 0.0), axis=0, keepdims=True).astype(jnp.int32)
        s1 = r1 * CAP + jnp.sum(jnp.where(oh1, rank, 0.0), axis=0, keepdims=True).astype(jnp.int32)
        row = iota((8 * N_EXP, TOK), 0)
        q = row & 7
        for j in range(3):
            first = q < FIRST[j]
            i = 8 * j + q - jnp.where(first, 6 * j, 6 * (j + 1))
            slot = (row >> 3) * CAP + PART * tp_ref[0] + i
            m0, m1 = slot == s0, slot == s1
            hit = m0 | m1
            pick_ref[j, :, :TOK] = jnp.where(hit & first, 1.0, 0.0).astype(BF16)
            pick_ref[j, :, TOK:] = jnp.where(hit & ~first, 1.0, 0.0).astype(BF16)
            w = jnp.where(m0, weight_ref[0:1, :], 0.0) + jnp.where(m1, weight_ref[1:2, :], 0.0)
            w = jnp.sum(w, axis=1, keepdims=True)
            cot_row = (q[:, 0:1] < FIRST[j]) if j % 2 else (q[:, 0:1] >= FIRST[j])
            scale_ref[j] = jnp.broadcast_to(jnp.where(cot_row, w, 1.0), (8 * N_EXP, 128))

    classes = (res_a, cot_a, res_b, cot_b)
    for j in range(3):
        rhs = jnp.concatenate([classes[j][...], classes[j + 1][...]], axis=0)
        got = dot(pick_ref[j], rhs) * scale_ref[j][:, 0:1]
        out_ref[:, 8 * j : 8 * j + 8, :] = got.reshape(N_EXP, 8, got.shape[1]).astype(BF16)


def dispatch(tp, routes_t, weight_t, resid, cotangent):
    bn = 256
    half = D // 2 // bn
    return pl.pallas_call(
        dispatch_kernel,
        grid_spec=pltpu.PrefetchScalarGridSpec(
            num_scalar_prefetch=1,
            grid=(half,),
            in_specs=[
                pl.BlockSpec((2, TOK), lambda n, s: (0, 0)),
                pl.BlockSpec((2, TOK), lambda n, s: (0, 0)),
                pl.BlockSpec((TOK, bn), lambda n, s: (0, n)),
                pl.BlockSpec((TOK, bn), lambda n, s: (0, n + half)),
                pl.BlockSpec((TOK, bn), lambda n, s: (0, n)),
                pl.BlockSpec((TOK, bn), lambda n, s: (0, n + half)),
            ],
            out_specs=pl.BlockSpec((N_EXP, 24, bn), lambda n, s: (0, 0, n)),
            scratch_shapes=[
                pltpu.VMEM((3, 8 * N_EXP, 2 * TOK), BF16),
                pltpu.VMEM((3, 8 * N_EXP, 128), F32),
            ],
        ),
        out_shape=jax.ShapeDtypeStruct((N_EXP, 24, D // 2), BF16),
        name="dispatch",
    )(tp, routes_t, weight_t, resid, resid, cotangent, cotangent)


def place_kernel(routes_ref, out_ref):
    r0, r1 = routes_ref[:, 0:1], routes_ref[:, 1:2]
    e = iota((TOK, N_EXP), 1)
    oh0, oh1 = e == r0, e == r1
    member = jnp.where(oh0 | oh1, 1.0, 0.0).astype(BF16)
    before = jnp.where(iota((TOK, TOK), 1) < iota((TOK, TOK), 0), 1.0, 0.0).astype(BF16)
    rank = dot(before, member)

    def line(oh, r):
        k = jnp.sum(jnp.where(oh, rank, 0.0), axis=1, keepdims=True).astype(jnp.int32)
        t = (k * 43) >> 8
        return r * 64 + t * 8 + (k - t * PART)

    col = iota((TOK, 8 * N_TP * N_EXP), 1)
    hit = (col == line(oh0, r0)) | (col == line(oh1, r1))
    out_ref[...] = jnp.where(hit, 1.0, 0.0).astype(BF16)


def place(routes):
    return pl.pallas_call(
        place_kernel,
        out_shape=jax.ShapeDtypeStruct((TOK, 8 * N_TP * N_EXP), BF16),
        name="place",
    )(routes)


def expert_kernel(got_ref, *refs):
    weights, (out_ref, rows_ref, acts_ref, wbuf, sems) = refs[:10], refs[10:]
    copies = []
    for side in range(2):
        own, prev, following, far_a, far_b = weights[5 * side : 5 * side + 5]
        lanes = pl.ds(128 * side, 128)
        for j, src in enumerate((own, prev, following)):
            copies.append((j, pltpu.make_async_copy(src, wbuf.at[j, :, lanes], sems.at[side, j])))
        copies.append((3, pltpu.make_async_copy(far_a, wbuf.at[3, pl.ds(0, 3072), lanes], sems.at[side, 3])))
        copies.append((3, pltpu.make_async_copy(far_b, wbuf.at[3, pl.ds(3072, 3072), lanes], sems.at[side, 4])))
    for _, copy in copies:
        copy.start()

    tiles = [
        got_ref[:, 8 * j : 8 * j + 8, :].astype(F32).reshape(8 * N_EXP, D // 2).astype(BF16) for j in range(3)
    ]
    k = iota((ROWS, 8 * N_EXP), 0)
    col = iota((ROWS, 8 * N_EXP), 1)
    source, q = col >> 3, col & 7

    def picked(cls):
        total = None
        for j in (cls - 1, cls):
            if 0 <= j < 3:
                i = 8 * j + q - 6 * cls
                sel = jnp.where((k == source * PART + i) & (i >= 0) & (i < PART), 1.0, 0.0).astype(BF16)
                part = dot(sel, tiles[j])
                total = part if total is None else total + part
        return total.astype(BF16)

    for cls in range(4):
        rows_ref[cls % 2, :, (cls // 2) * (D // 2) : (cls // 2 + 1) * (D // 2)] = picked(cls)
    in_rows, cot_rows = rows_ref[0], rows_ref[1]

    grad = jnp.zeros((ROWS, D), F32)
    for j in range(4):
        for at, copy in copies:
            if at == j:
                copy.wait()
        gate_w, up_w, down_w = (wbuf[j, D * n : D * (n + 1), :] for n in range(3))
        gate = dot(in_rows, gate_w)
        up = dot(in_rows, up_w)
        d_hidden = dot(cot_rows, down_w)
        sig = jax.nn.sigmoid(gate)
        silu = gate * sig
        d_gate = (d_hidden * up * (sig * (1.0 + gate * (1.0 - sig)))).astype(BF16)
        d_up = (d_hidden * silu).astype(BF16)
        acts_ref[j, 0] = d_gate
        acts_ref[j, 1] = d_up
        acts_ref[j, 2] = (silu * up).astype(BF16)
        grad = grad + dot_nt(d_gate, gate_w) + dot_nt(d_up, up_w)

    line = iota((8 * N_EXP, ROWS), 0)
    spread = (iota((8 * N_EXP, ROWS), 1) == (line >> 3) * PART + (line & 7)) & ((line & 7) < PART)
    back = dot(jnp.where(spread, 1.0, 0.0).astype(BF16), grad.astype(BF16)).reshape(N_EXP, 8, D)
    for t in range(N_TP):
        for h in range(2):
            at = 256 * t + 128 * h
            out_ref[:, t, 8 * h : 8 * h + 8, :] = back[:, :, at : at + 128].astype(BF16)


def experts(got, weights):
    return pl.pallas_call(
        expert_kernel,
        in_specs=[pl.BlockSpec(memory_space=pltpu.VMEM)] + [pl.BlockSpec(memory_space=pl.ANY)] * 10,
        out_shape=(
            jax.ShapeDtypeStruct((N_EXP, N_TP, 16, 128), BF16),
            jax.ShapeDtypeStruct((2, ROWS, D), BF16),
            jax.ShapeDtypeStruct((4, 3, ROWS, 256), BF16),
        ),
        scratch_shapes=[
            pltpu.VMEM((4, 3 * D, 256), BF16),
            pltpu.SemaphoreType.DMA((2, 5)),
        ],
        compiler_params=pltpu.CompilerParams(vmem_limit_bytes=48 * 1024 * 1024),
        name="experts",
    )(got, *weights)


def weight_grad_kernel(*refs):
    rows, acts = refs[0:4], refs[4:8]
    keep_g, send_g, keep_u, send_u, keep_d, send_d, xbuf, hbuf, sems = refs[8:]
    copies = []
    for n in range(4):
        at = pl.ds(ROWS * n, ROWS)
        copies.append(pltpu.make_async_copy(rows[n], xbuf.at[:, at, :], sems.at[0, n]))
        copies.append(pltpu.make_async_copy(acts[n], hbuf.at[:, at, :], sems.at[1, n]))
    for copy in copies:
        copy.start()
    for copy in copies:
        copy.wait()
    for n, (keep, send) in enumerate(((keep_g, send_g), (keep_u, send_u))):
        both = dot_tn(xbuf[0], hbuf[n])
        keep[...] = both[:, :128]
        send[...] = both[:, 128:]
    both = dot_tn(hbuf[2], xbuf[1])
    keep_d[...] = both[:128]
    send_d[...] = both[128:]


def weight_grads(rows, acts):
    tall = jax.ShapeDtypeStruct((D, 128), F32)
    wide = jax.ShapeDtypeStruct((128, D), F32)
    return pl.pallas_call(
        weight_grad_kernel,
        in_specs=[pl.BlockSpec(memory_space=pl.ANY)] * 8,
        out_shape=(tall, tall, tall, tall, wide, wide),
        scratch_shapes=[
            pltpu.VMEM((2, 4 * ROWS, D), BF16),
            pltpu.VMEM((3, 4 * ROWS, 256), BF16),
            pltpu.SemaphoreType.DMA((2, 4)),
        ],
        compiler_params=pltpu.CompilerParams(vmem_limit_bytes=56 * 1024 * 1024),
        name="weight_grads",
    )(*rows, *acts)


def combine_kernel(tp_ref, place_ref, back_ref, cot_ref, out_ref):
    halves = [
        back_ref[:, 8 * h : 8 * h + 8, :].astype(F32).reshape(8 * N_TP * N_EXP, 128).astype(BF16) for h in range(2)
    ]
    routed = dot(place_ref[...], jnp.concatenate(halves, axis=1))
    out_ref[...] = (cot_ref[...].astype(F32) + routed).astype(BF16)


def combine(tp, placed, back, cotangent):
    cols = D // N_TP
    return pl.pallas_call(
        combine_kernel,
        grid_spec=pltpu.PrefetchScalarGridSpec(
            num_scalar_prefetch=1,
            grid=(1,),
            in_specs=[
                pl.BlockSpec(placed.shape, lambda n, s: (0, 0)),
                pl.BlockSpec(back.shape, lambda n, s: (0, 0, 0)),
                pl.BlockSpec((TOK, cols), lambda n, s: (0, s[0])),
            ],
            out_specs=pl.BlockSpec((TOK, cols), lambda n, s: (0, 0)),
        ),
        out_shape=jax.ShapeDtypeStruct((TOK, cols), BF16),
        name="combine",
    )(tp, placed, back, cotangent)


def prepare_kernel(gate_ref, log_ref, before_ref, step_ref, mixed_ref, gelu_ref, slope_ref, prefix_ref):
    x = gate_ref[...].astype(F32)
    inner = GELU_C * (x + GELU_A * (x * x * x))
    th = jnp.tanh(inner)
    gelu = 0.5 * x * (1.0 + th)
    back = 0.5 * (1.0 + th) + 0.5 * x * (1.0 - th * th) * (GELU_C * (1.0 + 3.0 * GELU_A * (x * x)))
    states = jnp.exp(log_ref[...]) * before_ref[...] + step_ref[...].astype(F32)
    mixed_ref[...] = (gelu * states).astype(BF16)
    gelu_ref[...] = gelu
    slope_ref[...] = states * back

    row = iota((8, CH), 0)

    def block(n, carry):
        at = pl.multiple_of(n * 8, 8)
        total = log_ref[pl.ds(at, 8), :]
        for d in (1, 2, 4):
            total = total + jnp.where(row >= d, pltpu.roll(total, d, 0), 0.0)
        total = total + carry
        prefix_ref[pl.ds(at, 8), :] = jnp.exp(total)
        return total[7:8, :]

    lax.fori_loop(0, TOK // 8, block, jnp.zeros((1, CH), F32), unroll=4)


def prepare(gate_pre, log_decay, state_before, step_input):
    shape = gate_pre.shape
    return pl.pallas_call(
        prepare_kernel,
        out_shape=(
            jax.ShapeDtypeStruct(shape, BF16),
            jax.ShapeDtypeStruct(shape, F32),
            jax.ShapeDtypeStruct(shape, F32),
            jax.ShapeDtypeStruct(shape, F32),
        ),
        name="prepare",
    )(gate_pre, log_decay, state_before, step_input)


def project_kernel(order_ref, grad_ref, proj_ref, mixed_ref, gelu_ref, slope_ref, prefix_ref,
                   gp_ref, ggp_ref, direct_ref, link_ref, acc_ref):
    k = pl.program_id(0)
    grad = grad_ref[0]
    gp_ref[...] = dot_tn(grad, mixed_ref[...]).astype(BF16)
    part = dot(grad, proj_ref[...])

    @pl.when(k == 0)
    def _():
        acc_ref[...] = part

    @pl.when(k > 0)
    def _():
        acc_ref[...] = acc_ref[...] + part

    @pl.when(k == N_TP - 1)
    def _():
        d_mixed = acc_ref[...]
        ggp_ref[...] = (d_mixed * slope_ref[...]).astype(BF16)
        direct = d_mixed * gelu_ref[...]
        direct_ref[...] = direct
        link_ref[0:1, :] = prefix_ref[TOK - 1 : TOK, :]
        link_ref[1:2, :] = jnp.sum(prefix_ref[...] * direct, axis=0, keepdims=True)


def project(order, grads, out_proj, mixed, gelu, slope, prefix):
    cols = D // N_TP
    whole = pl.BlockSpec((TOK, CH), lambda k, s: (0, 0))
    return pl.pallas_call(
        project_kernel,
        grid_spec=pltpu.PrefetchScalarGridSpec(
            num_scalar_prefetch=1,
            grid=(N_TP,),
            in_specs=[
                pl.BlockSpec((1, TOK, cols), lambda k, s: (k, 0, 0)),
                pl.BlockSpec((cols, CH), lambda k, s: (s[k], 0)),
                whole, whole, whole, whole,
            ],
            out_specs=(
                pl.BlockSpec((cols, CH), lambda k, s: (s[k], 0)),
                whole,
                whole,
                pl.BlockSpec((2, CH), lambda k, s: (0, 0)),
            ),
            scratch_shapes=[pltpu.VMEM((TOK, CH), F32)],
        ),
        out_shape=(
            jax.ShapeDtypeStruct((D, CH), BF16),
            jax.ShapeDtypeStruct((TOK, CH), BF16),
            jax.ShapeDtypeStruct((TOK, CH), F32),
            jax.ShapeDtypeStruct((2, CH), F32),
        ),
        name="project",
    )(order, grads, out_proj, mixed, gelu, slope, prefix)


def recur_kernel(at_ref, links_ref, direct_ref, log_ref, before_ref, step_ref, decay_ref):
    mine = at_ref[0]
    arriving = jnp.zeros((1, CH), F32)
    for s in range(N_EXP - 1, 0, -1):
        arriving = jnp.where(s > mine, links_ref[s, 1:2, :] + links_ref[s, 0:1, :] * arriving, arriving)
    row = iota((8, CH), 0)
    blocks = TOK // 8

    def block(n, carry):
        value, first = carry
        at = pl.multiple_of((blocks - 1 - n) * 8, 8)
        decays = jnp.exp(log_ref[pl.ds(at, 8), :])
        a = jnp.where(row < 7, pltpu.roll(decays, 7, 0), first)
        b = direct_ref[pl.ds(at, 8), :]
        for d in (1, 2, 4):
            b = b + a * jnp.where(row < 8 - d, pltpu.roll(b, 8 - d, 0), 0.0)
            a = a * jnp.where(row < 8 - d, pltpu.roll(a, 8 - d, 0), 1.0)
        g = b + a * value
        step_ref[pl.ds(at, 8), :] = g
        decay_ref[pl.ds(at, 8), :] = g * decays * before_ref[pl.ds(at, 8), :]
        return g[0:1, :], decays[0:1, :]

    lax.fori_loop(0, blocks, block, (arriving, jnp.ones((1, CH), F32)), unroll=4)


def recur(at, links, direct, log_decay, state_before):
    return pl.pallas_call(
        recur_kernel,
        in_specs=[pl.BlockSpec(memory_space=pltpu.SMEM)] + [pl.BlockSpec(memory_space=pltpu.VMEM)] * 4,
        out_shape=(
            jax.ShapeDtypeStruct((TOK, CH), F32),
            jax.ShapeDtypeStruct((TOK, CH), F32),
        ),
        name="recur",
    )(at, links, direct, log_decay, state_before)


def shifted(value, axis, by):
    n = lax.axis_size(axis)
    return lax.ppermute(value, axis, [(i, (i + by) % n) for i in range(n)])


def on_device(resid, cotangent, routes, route_weight, w_gate, w_up, w_down, out_proj, gate_pre, log_decay,
              state_before, step_input):
    y, c = lax.axis_index("y"), lax.axis_index("c")
    tp = (2 * y + c).astype(jnp.int32)
    tp_vec = tp[None]

    own = jnp.concatenate([w_gate[0], w_up[0], w_down[0].T], axis=0)
    prev, following = shifted(own, "y", 1), shifted(own, "y", -1)
    half = own.shape[0] // 2
    far_a, far_b = shifted(prev[:half], "y", 1), shifted(following[half:], "y", -1)
    mine = (own, prev, following, far_a, far_b)
    weights = mine + tuple(shifted(w, "c", 1) for w in mine)

    sent = dispatch(tp_vec, routes.T, route_weight.T, resid, cotangent)
    got = lax.all_to_all(sent, SP, split_axis=0, concat_axis=0, tiled=True)

    placed = place(routes)
    mixed, gelu, slope, prefix = prepare(gate_pre, log_decay, state_before, step_input)

    back, rows, acts = experts(got, weights)
    back = lax.all_to_all(back.reshape(N_EXP * N_TP, 16, 128), ALL, split_axis=0, concat_axis=0, tiled=True)
    part = combine(tp_vec, placed, back, cotangent)

    near = jnp.stack([part, shifted(part, "y", 1), shifted(part, "y", -1), shifted(part, "y", 2)])
    grads = jnp.concatenate([near, shifted(near, "c", 1)], axis=0)
    ys = jnp.stack([y, y - 1, y + 1, y + 2]) % 4
    order = jnp.concatenate([2 * ys + c, 2 * ys + 1 - c]).astype(jnp.int32)
    gp, grad_gate_pre, direct, link = project(order, grads, out_proj, mixed, gelu, slope, prefix)

    links = lax.all_to_all(jnp.broadcast_to(link, (N_EXP, *link.shape)), SP, split_axis=0, concat_axis=0, tiled=True)
    summed = lax.all_to_all(gp.reshape(N_EXP, D // N_EXP, CH), SP, split_axis=0, concat_axis=0, tiled=True)
    grad_proj = summed.astype(F32).sum(axis=0)

    sp = (4 * lax.axis_index("z") + lax.axis_index("x")).astype(jnp.int32)
    grad_step_input, grad_log_decay = recur(sp[None], links, direct, log_decay, state_before)

    all_rows = (rows, shifted(rows, "y", -1), shifted(rows, "y", 1), shifted(rows, "y", 2))
    all_acts = (acts[0], shifted(acts[1], "y", -1), shifted(acts[2], "y", 1), shifted(acts[3], "y", 2))
    keep_g, send_g, keep_u, send_u, keep_d, send_d = weight_grads(all_rows, all_acts)
    grad_gate = keep_g + shifted(send_g, "c", 1)
    grad_up = keep_u + shifted(send_u, "c", 1)
    grad_down = keep_d + shifted(send_d, "c", 1)
    return (
        grad_gate[None],
        grad_up[None],
        grad_down[None],
        grad_proj,
        grad_gate_pre,
        grad_step_input,
        grad_log_decay,
    )


def solution(mesh):
    grid = Mesh(mesh.devices.reshape(8, 4, 4, 2), ALL)
    return jax.shard_map(
        on_device,
        mesh=grid,
        in_specs=(
            P(SP, None),
            P(SP, None),
            P(SP, None),
            P(SP, None),
            P(SP, None, TP),
            P(SP, None, TP),
            P(SP, TP, None),
            P(None, TP),
            P(SP, TP),
            P(SP, TP),
            P(SP, TP),
            P(SP, TP),
        ),
        out_specs=(
            P(SP, None, TP),
            P(SP, None, TP),
            P(SP, TP, None),
            P(SP, TP),
            P(SP, TP),
            P(SP, TP),
            P(SP, TP),
        ),
        check_vma=False,
    )
```

```python
import jax
import jax.numpy as jnp
from jax import lax
from jax.experimental import pallas as pl
from jax.experimental.pallas import tpu as pltpu
from jax.sharding import Mesh, PartitionSpec as P


BF16 = jnp.bfloat16
F32 = jnp.float32
SP = ("z", "x")
TP = ("y", "c")
ALL = ("z", "x", "y", "c")

TOK = 384
D = 2048
CAP = 48
N_EXP = 32
N_TP = 8
PART = CAP // N_TP
ROWS = N_EXP * PART
CH = 352
STRIP = 32
GELU_C = 0.7978845608028654
GELU_A = 0.044715


def iota(shape, dim):
    return lax.broadcasted_iota(jnp.int32, shape, dim)


def in_hbm(*arrays):
    held = tuple(pltpu.with_memory_space_constraint(a, pltpu.HBM) for a in arrays)
    return held if len(held) > 1 else held[0]


def vmem(mib):
    return pltpu.CompilerParams(vmem_limit_bytes=mib * 1024 * 1024)


def dot(a, b):
    return jnp.dot(a, b, preferred_element_type=F32)


def dot_nt(a, b):
    return lax.dot_general(a, b, (((1,), (1,)), ((), ())), preferred_element_type=F32)


def dot_tn(a, b):
    return lax.dot_general(a, b, (((0,), (0,)), ((), ())), preferred_element_type=F32)


FIRST = (6, 4, 2)


def pack_kernel(gate_ref, up_ref, down_ref, out_ref, down_buf, turned, sems):
    load = pltpu.make_async_copy(down_ref, down_buf, sems.at[0])
    load.start()
    straight = [
        pltpu.make_async_copy(gate_ref, out_ref.at[pl.ds(0, D)], sems.at[1]),
        pltpu.make_async_copy(up_ref, out_ref.at[pl.ds(D, D)], sems.at[2]),
    ]
    for copy in straight:
        copy.start()
    load.wait()
    turned[...] = down_buf[...].T
    last = pltpu.make_async_copy(turned, out_ref.at[pl.ds(2 * D, D)], sems.at[3])
    last.start()
    for copy in straight + [last]:
        copy.wait()


def pack(gate, up, down):
    anywhere = pl.BlockSpec(memory_space=pl.ANY)
    return pl.pallas_call(
        pack_kernel,
        in_specs=[anywhere] * 3,
        out_specs=anywhere,
        out_shape=pltpu.HBM((3 * D, 128), BF16),
        scratch_shapes=[
            pltpu.VMEM((128, D), BF16),
            pltpu.VMEM((D, 128), BF16),
            pltpu.SemaphoreType.DMA((4,)),
        ],
        compiler_params=vmem(4),
        name="pack",
    )(*in_hbm(gate, up, down))


def dispatch_kernel(tp_ref, routes_ref, weight_ref, res_a, res_b, cot_a, cot_b, out_ref, pick_ref, scale_ref):
    @pl.when(pl.program_id(0) == 0)
    def _():
        r0, r1 = routes_ref[0:1, :], routes_ref[1:2, :]
        e = iota((N_EXP, TOK), 0)
        oh0, oh1 = e == r0, e == r1
        member = jnp.where(oh0 | oh1, 1.0, 0.0).astype(BF16)
        before = jnp.where(iota((TOK, TOK), 0) < iota((TOK, TOK), 1), 1.0, 0.0).astype(BF16)
        rank = dot(member, before)
        s0 = r0 * CAP + jnp.sum(jnp.where(oh0, rank, 0.0), axis=0, keepdims=True).astype(jnp.int32)
        s1 = r1 * CAP + jnp.sum(jnp.where(oh1, rank, 0.0), axis=0, keepdims=True).astype(jnp.int32)
        row = iota((8 * N_EXP, TOK), 0)
        q = row & 7
        for j in range(3):
            first = q < FIRST[j]
            i = 8 * j + q - jnp.where(first, 6 * j, 6 * (j + 1))
            slot = (row >> 3) * CAP + PART * tp_ref[0] + i
            m0, m1 = slot == s0, slot == s1
            hit = m0 | m1
            pick_ref[j, :, :TOK] = jnp.where(hit & first, 1.0, 0.0).astype(BF16)
            pick_ref[j, :, TOK:] = jnp.where(hit & ~first, 1.0, 0.0).astype(BF16)
            w = jnp.where(m0, weight_ref[0:1, :], 0.0) + jnp.where(m1, weight_ref[1:2, :], 0.0)
            w = jnp.sum(w, axis=1, keepdims=True)
            cot_row = (q[:, 0:1] < FIRST[j]) if j % 2 else (q[:, 0:1] >= FIRST[j])
            scale_ref[j] = jnp.broadcast_to(jnp.where(cot_row, w, 1.0), (8 * N_EXP, 128))

    classes = (res_a, cot_a, res_b, cot_b)
    for j in range(3):
        rhs = jnp.concatenate([classes[j][...], classes[j + 1][...]], axis=0)
        got = dot(pick_ref[j], rhs) * scale_ref[j][:, 0:1]
        out_ref[:, 8 * j : 8 * j + 8, :] = got.reshape(N_EXP, 8, got.shape[1]).astype(BF16)


def dispatch(tp, routes_t, weight_t, resid, cotangent):
    bn = 256
    half = D // 2 // bn
    return pl.pallas_call(
        dispatch_kernel,
        grid_spec=pltpu.PrefetchScalarGridSpec(
            num_scalar_prefetch=1,
            grid=(half,),
            in_specs=[
                pl.BlockSpec((2, TOK), lambda n, s: (0, 0)),
                pl.BlockSpec((2, TOK), lambda n, s: (0, 0)),
                pl.BlockSpec((TOK, bn), lambda n, s: (0, n)),
                pl.BlockSpec((TOK, bn), lambda n, s: (0, n + half)),
                pl.BlockSpec((TOK, bn), lambda n, s: (0, n)),
                pl.BlockSpec((TOK, bn), lambda n, s: (0, n + half)),
            ],
            out_specs=pl.BlockSpec((N_EXP, 24, bn), lambda n, s: (0, 0, n)),
            scratch_shapes=[
                pltpu.VMEM((3, 8 * N_EXP, 2 * TOK), BF16),
                pltpu.VMEM((3, 8 * N_EXP, 128), F32),
            ],
        ),
        out_shape=pltpu.HBM((N_EXP, 24, D // 2), BF16),
        compiler_params=vmem(14),
        name="dispatch",
    )(tp, routes_t, weight_t, resid, resid, cotangent, cotangent)


def place_kernel(routes_ref, out_ref):
    r0, r1 = routes_ref[:, 0:1], routes_ref[:, 1:2]
    e = iota((TOK, N_EXP), 1)
    oh0, oh1 = e == r0, e == r1
    member = jnp.where(oh0 | oh1, 1.0, 0.0).astype(BF16)
    before = jnp.where(iota((TOK, TOK), 1) < iota((TOK, TOK), 0), 1.0, 0.0).astype(BF16)
    rank = dot(before, member)

    def line(oh, r):
        k = jnp.sum(jnp.where(oh, rank, 0.0), axis=1, keepdims=True).astype(jnp.int32)
        t = (k * 43) >> 8
        return r * 64 + t * 8 + (k - t * PART)

    col = iota((TOK, 8 * N_TP * N_EXP), 1)
    hit = (col == line(oh0, r0)) | (col == line(oh1, r1))
    out_ref[...] = jnp.where(hit, 1.0, 0.0).astype(BF16)


def place(routes):
    return pl.pallas_call(
        place_kernel,
        out_shape=pltpu.HBM((TOK, 8 * N_TP * N_EXP), BF16),
        compiler_params=vmem(8),
        name="place",
    )(routes)


def select_kernel(got_ref, rows_ref):
    tiles = [
        got_ref[:, 8 * j : 8 * j + 8, :].astype(F32).reshape(8 * N_EXP, D // 2).astype(BF16) for j in range(3)
    ]
    k = iota((ROWS, 8 * N_EXP), 0)
    col = iota((ROWS, 8 * N_EXP), 1)
    source, q = col >> 3, col & 7
    for cls in range(4):
        total = None
        for j in (cls - 1, cls):
            if 0 <= j < 3:
                i = 8 * j + q - 6 * cls
                sel = jnp.where((k == source * PART + i) & (i >= 0) & (i < PART), 1.0, 0.0).astype(BF16)
                part = dot(sel, tiles[j])
                total = part if total is None else total + part
        rows_ref[cls % 2, :, (cls // 2) * (D // 2) : (cls // 2 + 1) * (D // 2)] = total.astype(BF16)


def select(got):
    return pl.pallas_call(
        select_kernel,
        out_shape=pltpu.HBM((2, ROWS, D), BF16),
        compiler_params=vmem(12),
        name="select",
    )(in_hbm(got))


def expert_kernel(rows_ref, *refs):
    weights, out_ref, acts, (wbuf, sems) = refs[:10], refs[10], refs[11:15], refs[15:]
    copies = []
    for side in range(2):
        own, prev, following, far_a, far_b = weights[5 * side : 5 * side + 5]
        lanes = pl.ds(128 * side, 128)
        for j, src in enumerate((own, prev, following)):
            copies.append((j, pltpu.make_async_copy(src, wbuf.at[j, :, lanes], sems.at[side, j])))
        copies.append((3, pltpu.make_async_copy(far_a, wbuf.at[3, pl.ds(0, 3072), lanes], sems.at[side, 3])))
        copies.append((3, pltpu.make_async_copy(far_b, wbuf.at[3, pl.ds(3072, 3072), lanes], sems.at[side, 4])))
    for _, copy in sorted(copies, key=lambda entry: entry[0]):
        copy.start()

    in_rows, cot_rows = rows_ref[0], rows_ref[1]
    grad = jnp.zeros((ROWS, D), F32)
    for j in range(4):
        for at, copy in copies:
            if at == j:
                copy.wait()
        gate_w, up_w, down_w = (wbuf[j, D * n : D * (n + 1), :] for n in range(3))
        gate = dot(in_rows, gate_w)
        up = dot(in_rows, up_w)
        d_hidden = dot(cot_rows, down_w)
        sig = jax.nn.sigmoid(gate)
        silu = gate * sig
        d_gate = (d_hidden * up * (sig * (1.0 + gate * (1.0 - sig)))).astype(BF16)
        d_up = (d_hidden * silu).astype(BF16)
        acts[j][0] = d_gate
        acts[j][1] = d_up
        acts[j][2] = (silu * up).astype(BF16)
        grad = grad + dot_nt(d_gate, gate_w) + dot_nt(d_up, up_w)

    line = iota((8 * N_EXP, ROWS), 0)
    spread = (iota((8 * N_EXP, ROWS), 1) == (line >> 3) * PART + (line & 7)) & ((line & 7) < PART)
    back = dot(jnp.where(spread, 1.0, 0.0).astype(BF16), grad.astype(BF16)).reshape(N_EXP, 8, D)
    for t in range(N_TP):
        for h in range(2):
            at = 256 * t + 128 * h
            out_ref[:, t, 8 * h : 8 * h + 8, :] = back[:, :, at : at + 128].astype(BF16)


def experts(rows, weights):
    act = pltpu.HBM((3, ROWS, 256), BF16)
    return pl.pallas_call(
        expert_kernel,
        in_specs=[pl.BlockSpec(memory_space=pltpu.VMEM)] + [pl.BlockSpec(memory_space=pl.ANY)] * 10,
        out_shape=(pltpu.HBM((N_EXP, N_TP, 16, 128), BF16), act, act, act, act),
        scratch_shapes=[
            pltpu.VMEM((4, 3 * D, 256), BF16),
            pltpu.SemaphoreType.DMA((2, 5)),
        ],
        compiler_params=vmem(32),
        name="experts",
    )(*in_hbm(rows, *weights))


def weight_grad_kernel(*refs):
    rows, far, acts = refs[0:3], refs[3:5], refs[5:9]
    keep_g, send_g, keep_u, send_u, keep_d, send_d, xbuf, hbuf, sems = refs[9:]
    copies = []
    for n in range(4):
        at = pl.ds(ROWS * n, ROWS)
        if n < 3:
            copies.append(pltpu.make_async_copy(rows[n], xbuf.at[:, at, :], sems.at[0, n]))
        copies.append(pltpu.make_async_copy(acts[n], hbuf.at[:, at, :], sems.at[1, n]))
    for n in range(2):
        copies.append(pltpu.make_async_copy(far[n], xbuf.at[n, pl.ds(3 * ROWS, ROWS), :], sems.at[0, 3 + n]))
    for copy in copies:
        copy.start()
    for copy in copies:
        copy.wait()
    for n, (keep, send) in enumerate(((keep_g, send_g), (keep_u, send_u))):
        both = dot_tn(xbuf[0], hbuf[n])
        keep[...] = both[:, :128]
        send[...] = both[:, 128:]
    both = dot_tn(hbuf[2], xbuf[1])
    keep_d[...] = both[:128]
    send_d[...] = both[128:]


def weight_grads(rows, far, acts):
    tall = pltpu.HBM((D, 128), F32)
    wide = pltpu.HBM((128, D), F32)
    return pl.pallas_call(
        weight_grad_kernel,
        in_specs=[pl.BlockSpec(memory_space=pl.ANY)] * 9,
        out_shape=(tall, tall, tall, tall, wide, wide),
        scratch_shapes=[
            pltpu.VMEM((2, 4 * ROWS, D), BF16),
            pltpu.VMEM((3, 4 * ROWS, 256), BF16),
            pltpu.SemaphoreType.DMA((2, 5)),
        ],
        compiler_params=vmem(26),
        name="weight_grads",
    )(*in_hbm(*rows, *far, *acts))


def combine_kernel(tp_ref, place_ref, back_ref, cot_ref, out_ref):
    halves = [
        back_ref[:, 8 * h : 8 * h + 8, :].astype(F32).reshape(8 * N_TP * N_EXP, 128).astype(BF16) for h in range(2)
    ]
    routed = dot(place_ref[...], jnp.concatenate(halves, axis=1))
    out_ref[...] = (cot_ref[...].astype(F32) + routed).T.astype(BF16)


def combine(tp, placed, back, cotangent):
    cols = D // N_TP
    return pl.pallas_call(
        combine_kernel,
        grid_spec=pltpu.PrefetchScalarGridSpec(
            num_scalar_prefetch=1,
            grid=(1,),
            in_specs=[
                pl.BlockSpec(placed.shape, lambda n, s: (0, 0)),
                pl.BlockSpec(back.shape, lambda n, s: (0, 0, 0)),
                pl.BlockSpec((TOK, cols), lambda n, s: (0, s[0])),
            ],
            out_specs=pl.BlockSpec((cols, TOK), lambda n, s: (0, 0)),
        ),
        out_shape=jax.ShapeDtypeStruct((cols, TOK), BF16),
        compiler_params=vmem(12),
        name="combine",
    )(tp, *in_hbm(placed, back), cotangent)


def prepare_kernel(gate_ref, log_ref, before_ref, step_ref, mixed_ref, gelu_ref, slope_ref, prefix_ref):
    lane = iota((STRIP, TOK), 1)

    def strip(n, _):
        at = pl.ds(pl.multiple_of(n * STRIP, STRIP), STRIP)
        x = gate_ref[at, :].astype(F32)
        th = jnp.tanh(GELU_C * (x + GELU_A * (x * x * x)))
        gelu = 0.5 * x * (1.0 + th)
        back = 0.5 * (1.0 + th) + 0.5 * x * (1.0 - th * th) * (GELU_C * (1.0 + 3.0 * GELU_A * (x * x)))
        logs = log_ref[at, :]
        states = jnp.exp(logs) * before_ref[at, :] + step_ref[at, :].astype(F32)
        mixed_ref[at, :] = (gelu * states).astype(BF16)
        gelu_ref[at, :] = gelu
        slope_ref[at, :] = states * back
        total = logs
        d = 1
        while d < TOK:
            total = total + jnp.where(lane >= d, pltpu.roll(total, d, 1), 0.0)
            d *= 2
        prefix_ref[at, :] = jnp.exp(total)
        return 0

    lax.fori_loop(0, CH // STRIP, strip, 0)


def prepare(gate_pre, log_decay, state_before, step_input):
    shape = gate_pre.shape
    wide = pltpu.HBM(shape, F32)
    return pl.pallas_call(
        prepare_kernel,
        out_shape=(pltpu.HBM(shape, BF16), wide, wide, wide),
        compiler_params=vmem(8),
        name="prepare",
    )(gate_pre, log_decay, state_before, step_input)


def project_kernel(order_ref, *refs):
    grads, (proj_ref, mixed_ref, gelu_ref, slope_ref, prefix_ref) = refs[:8], refs[8:13]
    pieces, (ggp_ref, direct_ref, link_ref, block_ref, turn_ref) = refs[13:17], refs[17:]
    d_mixed = jnp.zeros((CH, TOK), F32)
    for k in range(N_TP):
        group = order_ref[k]
        grad = grads[k][...]
        cols = pl.ds(pl.multiple_of(group * 256, 256), 256)
        d_mixed = d_mixed + dot(proj_ref[:, cols], grad)
        block_ref[...] = dot(grad, mixed_ref[...])
        for m in range(4):
            at = pl.ds(pl.multiple_of(((order_ref[8] + m) & 3) * 64, 64), 64)
            pieces[m][pl.ds(group, 1)] = block_ref[at, :].astype(BF16)[None]
    ggp_ref[...] = (d_mixed * slope_ref[...]).astype(BF16)
    direct = d_mixed * gelu_ref[...]
    direct_ref[...] = direct
    turn_ref[...] = jnp.zeros_like(turn_ref)
    turn_ref[0:CH, 0:1] = prefix_ref[:, TOK - 1 : TOK]
    turn_ref[0:CH, 1:2] = jnp.sum(prefix_ref[...] * direct, axis=1, keepdims=True)
    link_ref[...] = turn_ref[...].T[0:2, 0:CH]


def project(order, grads, out_proj, mixed, gelu, slope, prefix):
    piece = pltpu.HBM((8, 64, CH), BF16)
    return pl.pallas_call(
        project_kernel,
        in_specs=[pl.BlockSpec(memory_space=pltpu.SMEM)] + [pl.BlockSpec(memory_space=pltpu.VMEM)] * 13,
        out_shape=(
            piece, piece, piece, piece,
            pltpu.HBM((CH, TOK), BF16),
            pltpu.HBM((CH, TOK), F32),
            pltpu.HBM((2, CH), F32),
        ),
        scratch_shapes=[pltpu.VMEM((256, CH), F32), pltpu.VMEM((TOK, 128), F32)],
        compiler_params=vmem(14),
        name="project",
    )(order, *grads, out_proj, mixed, gelu, slope, prefix)


def recur_kernel(at_ref, links_ref, direct_ref, log_ref, before_ref, step_ref, decay_ref, turn_ref, arrive_ref):
    mine = at_ref[0]
    arriving = jnp.zeros((1, CH), F32)
    for s in range(N_EXP - 1, 0, -1):
        arriving = jnp.where(s > mine, links_ref[s, 1:2, :] + links_ref[s, 0:1, :] * arriving, arriving)
    turn_ref[...] = jnp.zeros_like(turn_ref)
    turn_ref[0:1, 0:CH] = arriving
    arrive_ref[...] = turn_ref[...].T
    lane = iota((STRIP, TOK), 1)

    def strip(n, _):
        at = pl.ds(pl.multiple_of(n * STRIP, STRIP), STRIP)
        decays = jnp.exp(log_ref[at, :])
        a = jnp.where(lane < TOK - 1, pltpu.roll(decays, TOK - 1, 1), 1.0)
        b = direct_ref[at, :]
        d = 1
        while d < TOK:
            b = b + a * jnp.where(lane < TOK - d, pltpu.roll(b, TOK - d, 1), 0.0)
            a = a * jnp.where(lane < TOK - d, pltpu.roll(a, TOK - d, 1), 1.0)
            d *= 2
        g = b + a * arrive_ref[at, 0:1]
        step_ref[at, :] = g
        decay_ref[at, :] = g * decays * before_ref[at, :]
        return 0

    lax.fori_loop(0, CH // STRIP, strip, 0)


def recur(at, links, direct, log_decay, state_before):
    return pl.pallas_call(
        recur_kernel,
        in_specs=[pl.BlockSpec(memory_space=pltpu.SMEM)] + [pl.BlockSpec(memory_space=pltpu.VMEM)] * 4,
        out_shape=(
            jax.ShapeDtypeStruct((CH, TOK), F32),
            jax.ShapeDtypeStruct((CH, TOK), F32),
        ),
        scratch_shapes=[pltpu.VMEM((128, TOK), F32), pltpu.VMEM((TOK, 128), F32)],
        compiler_params=vmem(8),
        name="recur",
    )(at, links, direct, log_decay, state_before)


def shifted(value, axis, by):
    n = lax.axis_size(axis)
    return lax.ppermute(value, axis, [(i, (i + by) % n) for i in range(n)])


def on_device(resid, cotangent, routes, route_weight, w_gate, w_up, w_down, out_proj, gate_pre, log_decay,
              state_before, step_input):
    y, c = lax.axis_index("y"), lax.axis_index("c")
    tp = (2 * y + c).astype(jnp.int32)
    tp_vec = tp[None]

    own = pack(w_gate[0], w_up[0], w_down[0])
    prev, following = shifted(own, "y", 1), shifted(own, "y", -1)
    half = own.shape[0] // 2
    far_a, far_b = shifted(prev[:half], "y", 1), shifted(following[half:], "y", -1)
    mine = (own, prev, following, far_a, far_b)
    weights = mine + tuple(shifted(w, "c", 1) for w in mine)

    sent = dispatch(tp_vec, routes.T, route_weight.T, resid, cotangent)
    got = lax.all_to_all(sent, SP, split_axis=0, concat_axis=0, tiled=True)

    placed = place(routes)
    log_t, before_t = log_decay.T, state_before.T
    mixed, gelu, slope, prefix = prepare(gate_pre.T, log_t, before_t, step_input.T)
    mixed = mixed.T
    ys = jnp.stack([y, y - 1, y + 1, y + 2]) % 4
    order = jnp.concatenate([2 * ys + c, 2 * ys + 1 - c, lax.axis_index("x")[None]]).astype(jnp.int32)
    got, placed, mixed, gelu, slope, prefix, order = lax.optimization_barrier(
        (got, placed, mixed, gelu, slope, prefix, order)
    )

    rows = select(got)
    rows_after = shifted(rows, "y", -1)
    rows_before = shifted(rows, "y", 1)
    back, *acts = experts(rows, weights)
    acts = (acts[0], shifted(acts[1], "y", -1), shifted(acts[2], "y", 1), shifted(acts[3], "y", 2))
    back = lax.all_to_all(back.reshape(N_EXP * N_TP, 16, 128), ALL, split_axis=0, concat_axis=0, tiled=True)
    part = combine(tp_vec, placed, back, cotangent)

    near = (part, shifted(part, "y", 1), shifted(part, "y", -1), shifted(part, "y", 2))
    far_in, far_cot, *near = lax.optimization_barrier((rows_before[0], rows_after[1], *near))
    grads = (*near, *(shifted(g, "c", 1) for g in near))
    *pieces, grad_gate_pre, direct, link = project(order, grads, out_proj.T, mixed, gelu, slope, prefix)

    over_x = [pieces[0]] + [shifted(pieces[m], "x", m) for m in (1, 2, 3)]
    link = jnp.broadcast_to(link, (N_EXP, *link.shape))
    links = lax.all_to_all(link, SP, split_axis=0, concat_axis=0, tiled=True)
    over_x = sum(p.astype(F32) for p in over_x).astype(BF16)
    over_z = lax.all_to_all(over_x, "z", split_axis=0, concat_axis=0, tiled=True)
    grad_proj = over_z.astype(F32).sum(axis=0)

    sp = (4 * lax.axis_index("z") + lax.axis_index("x")).astype(jnp.int32)
    grad_step_input, grad_log_decay = recur(sp[None], links, direct, log_t, before_t)

    far = (shifted(far_in, "y", 1), shifted(far_cot, "y", -1))
    keep_g, send_g, keep_u, send_u, keep_d, send_d = weight_grads(
        (rows, rows_after, rows_before), far, acts
    )
    grad_gate = keep_g + shifted(send_g, "c", 1)
    grad_up = keep_u + shifted(send_u, "c", 1)
    grad_down = keep_d + shifted(send_d, "c", 1)
    return (
        grad_gate[None],
        grad_up[None],
        grad_down[None],
        grad_proj,
        grad_gate_pre.T,
        grad_step_input.T,
        grad_log_decay.T,
    )


def solution(mesh):
    grid = Mesh(mesh.devices.reshape(8, 4, 4, 2), ALL)


    return jax.shard_map(
        on_device,
        mesh=grid,
        in_specs=(
            P(SP, None),
            P(SP, None),
            P(SP, None),
            P(SP, None),
            P(SP, None, TP),
            P(SP, None, TP),
            P(SP, TP, None),
            P(None, TP),
            P(SP, TP),
            P(SP, TP),
            P(SP, TP),
            P(SP, TP),
        ),
        out_specs=(
            P(SP, None, TP),
            P(SP, None, TP),
            P(SP, TP, None),
            P(SP, TP),
            P(SP, TP),
            P(SP, TP),
            P(SP, TP),
        ),
        check_vma=False,
    )
```

```python
import jax
import jax.numpy as jnp
from jax import lax
from jax.experimental import pallas as pl
from jax.experimental.pallas import tpu as pltpu
from jax.sharding import Mesh, PartitionSpec as P


BF16 = jnp.bfloat16
F32 = jnp.float32
SP = ("z", "x")
TP = ("y", "c")
ALL = ("z", "x", "y", "c")

TOK = 384
D = 2048
CAP = 48
N_EXP = 32
N_TP = 8
PART = CAP // N_TP
ROWS = N_EXP * PART
CH = 352
STRIP = 32
GELU_C = 0.7978845608028654
GELU_A = 0.044715


def iota(shape, dim):
    return lax.broadcasted_iota(jnp.int32, shape, dim)


def in_hbm(*arrays):
    held = tuple(pltpu.with_memory_space_constraint(a, pltpu.HBM) for a in arrays)
    return held if len(held) > 1 else held[0]


def vmem(mib):
    return pltpu.CompilerParams(vmem_limit_bytes=mib * 1024 * 1024)


def dot(a, b):
    return jnp.dot(a, b, preferred_element_type=F32)


def dot_nt(a, b):
    return lax.dot_general(a, b, (((1,), (1,)), ((), ())), preferred_element_type=F32)


def dot_tn(a, b):
    return lax.dot_general(a, b, (((0,), (0,)), ((), ())), preferred_element_type=F32)


FIRST = (6, 4, 2)


def pack_kernel(gate_ref, up_ref, down_ref, a_ref, b_ref, abuf, bbuf, down_buf, sems):
    third = D // 2
    loads = [
        pltpu.make_async_copy(down_ref, down_buf, sems.at[0]),
        pltpu.make_async_copy(gate_ref, abuf.at[pl.ds(0, D)], sems.at[1]),
        pltpu.make_async_copy(up_ref.at[pl.ds(0, third)], abuf.at[pl.ds(D, third)], sems.at[2]),
        pltpu.make_async_copy(up_ref.at[pl.ds(third, third)], bbuf.at[pl.ds(0, third)], sems.at[3]),
    ]
    for load in loads:
        load.start()
    loads[1].wait()
    loads[2].wait()
    out_a = pltpu.make_async_copy(abuf, a_ref, sems.at[4])
    out_a.start()
    loads[0].wait()
    bbuf[third:, :] = down_buf[...].T
    loads[3].wait()
    out_b = pltpu.make_async_copy(bbuf, b_ref, sems.at[5])
    out_b.start()
    out_a.wait()
    out_b.wait()


def pack(gate, up, down):
    anywhere = pl.BlockSpec(memory_space=pl.ANY)
    half = pltpu.HBM((3 * D // 2, 128), BF16)
    return pl.pallas_call(
        pack_kernel,
        in_specs=[anywhere] * 3,
        out_specs=(anywhere, anywhere),
        out_shape=(half, half),
        scratch_shapes=[
            pltpu.VMEM((3 * D // 2, 128), BF16),
            pltpu.VMEM((3 * D // 2, 128), BF16),
            pltpu.VMEM((128, D), BF16),
            pltpu.SemaphoreType.DMA((6,)),
        ],
        compiler_params=vmem(4),
        name="pack",
    )(*in_hbm(gate, up, down))


def dispatch_kernel(tp_ref, routes_ref, weight_ref, res_a, res_b, cot_a, cot_b, out_ref, pick_ref, scale_ref):
    @pl.when(pl.program_id(0) == 0)
    def _():
        r0, r1 = routes_ref[0:1, :], routes_ref[1:2, :]
        e = iota((N_EXP, TOK), 0)
        oh0, oh1 = e == r0, e == r1
        member = jnp.where(oh0 | oh1, 1.0, 0.0).astype(BF16)
        before = jnp.where(iota((TOK, TOK), 0) < iota((TOK, TOK), 1), 1.0, 0.0).astype(BF16)
        rank = dot(member, before)
        s0 = r0 * CAP + jnp.sum(jnp.where(oh0, rank, 0.0), axis=0, keepdims=True).astype(jnp.int32)
        s1 = r1 * CAP + jnp.sum(jnp.where(oh1, rank, 0.0), axis=0, keepdims=True).astype(jnp.int32)
        row = iota((8 * N_EXP, TOK), 0)
        q = row & 7
        for j in range(3):
            first = q < FIRST[j]
            i = 8 * j + q - jnp.where(first, 6 * j, 6 * (j + 1))
            slot = (row >> 3) * CAP + PART * tp_ref[0] + i
            m0, m1 = slot == s0, slot == s1
            hit = m0 | m1
            pick_ref[j, :, :TOK] = jnp.where(hit & first, 1.0, 0.0).astype(BF16)
            pick_ref[j, :, TOK:] = jnp.where(hit & ~first, 1.0, 0.0).astype(BF16)
            w = jnp.where(m0, weight_ref[0:1, :], 0.0) + jnp.where(m1, weight_ref[1:2, :], 0.0)
            w = jnp.sum(w, axis=1, keepdims=True)
            cot_row = (q[:, 0:1] < FIRST[j]) if j % 2 else (q[:, 0:1] >= FIRST[j])
            scale_ref[j] = jnp.broadcast_to(jnp.where(cot_row, w, 1.0), (8 * N_EXP, 128))

    classes = (res_a, cot_a, res_b, cot_b)
    for j in range(3):
        rhs = jnp.concatenate([classes[j][...], classes[j + 1][...]], axis=0)
        got = dot(pick_ref[j], rhs) * scale_ref[j][:, 0:1]
        out_ref[:, 8 * j : 8 * j + 8, :] = got.reshape(N_EXP, 8, got.shape[1]).astype(BF16)


def dispatch(tp, routes_t, weight_t, resid, cotangent):
    bn = 256
    half = D // 2 // bn
    return pl.pallas_call(
        dispatch_kernel,
        grid_spec=pltpu.PrefetchScalarGridSpec(
            num_scalar_prefetch=1,
            grid=(half,),
            in_specs=[
                pl.BlockSpec((2, TOK), lambda n, s: (0, 0)),
                pl.BlockSpec((2, TOK), lambda n, s: (0, 0)),
                pl.BlockSpec((TOK, bn), lambda n, s: (0, n)),
                pl.BlockSpec((TOK, bn), lambda n, s: (0, n + half)),
                pl.BlockSpec((TOK, bn), lambda n, s: (0, n)),
                pl.BlockSpec((TOK, bn), lambda n, s: (0, n + half)),
            ],
            out_specs=pl.BlockSpec((N_EXP, 24, bn), lambda n, s: (0, 0, n)),
            scratch_shapes=[
                pltpu.VMEM((3, 8 * N_EXP, 2 * TOK), BF16),
                pltpu.VMEM((3, 8 * N_EXP, 128), F32),
            ],
        ),
        out_shape=pltpu.HBM((N_EXP, 24, D // 2), BF16),
        compiler_params=vmem(14),
        name="dispatch",
    )(tp, routes_t, weight_t, resid, resid, cotangent, cotangent)


def place_kernel(routes_ref, out_ref):
    r0, r1 = routes_ref[:, 0:1], routes_ref[:, 1:2]
    e = iota((TOK, N_EXP), 1)
    oh0, oh1 = e == r0, e == r1
    member = jnp.where(oh0 | oh1, 1.0, 0.0).astype(BF16)
    before = jnp.where(iota((TOK, TOK), 1) < iota((TOK, TOK), 0), 1.0, 0.0).astype(BF16)
    rank = dot(before, member)

    def line(oh, r):
        k = jnp.sum(jnp.where(oh, rank, 0.0), axis=1, keepdims=True).astype(jnp.int32)
        t = (k * 43) >> 8
        return r * 64 + t * 8 + (k - t * PART)

    col = iota((TOK, 8 * N_TP * N_EXP), 1)
    hit = (col == line(oh0, r0)) | (col == line(oh1, r1))
    out_ref[...] = jnp.where(hit, 1.0, 0.0).astype(BF16)


def place(routes):
    return pl.pallas_call(
        place_kernel,
        out_shape=pltpu.HBM((TOK, 8 * N_TP * N_EXP), BF16),
        compiler_params=vmem(8),
        name="place",
    )(routes)


def select_kernel(got_ref, rows_ref):
    tiles = [
        got_ref[:, 8 * j : 8 * j + 8, :].astype(F32).reshape(8 * N_EXP, D // 2).astype(BF16) for j in range(3)
    ]
    k = iota((ROWS, 8 * N_EXP), 0)
    col = iota((ROWS, 8 * N_EXP), 1)
    source, q = col >> 3, col & 7
    for cls in range(4):
        total = None
        for j in (cls - 1, cls):
            if 0 <= j < 3:
                i = 8 * j + q - 6 * cls
                sel = jnp.where((k == source * PART + i) & (i >= 0) & (i < PART), 1.0, 0.0).astype(BF16)
                part = dot(sel, tiles[j])
                total = part if total is None else total + part
        rows_ref[cls % 2, :, (cls // 2) * (D // 2) : (cls // 2 + 1) * (D // 2)] = total.astype(BF16)


def select(got):
    return pl.pallas_call(
        select_kernel,
        out_shape=pltpu.HBM((2, ROWS, D), BF16),
        compiler_params=vmem(12),
        name="select",
    )(in_hbm(got))


def expert_kernel(rows_ref, *refs):
    weights, out_ref, acts, (wbuf, sems) = refs[:16], refs[16], refs[17:21], refs[21:]
    rows_half = 3 * D // 2
    copies = []
    for j in range(4):
        for side in range(2):
            for part in range(2):
                src = weights[8 * side + 2 * j + part]
                dst = wbuf.at[j, pl.ds(rows_half * part, rows_half), pl.ds(128 * side, 128)]
                copies.append((j, pltpu.make_async_copy(src, dst, sems.at[j, 2 * side + part])))
    for _, copy in copies:
        copy.start()

    in_rows, cot_rows = rows_ref[0], rows_ref[1]
    grad = jnp.zeros((ROWS, D), F32)
    for j in range(4):
        for at, copy in copies:
            if at == j:
                copy.wait()
        gate_w, up_w, down_w = (wbuf[j, D * n : D * (n + 1), :] for n in range(3))
        gate = dot(in_rows, gate_w)
        up = dot(in_rows, up_w)
        d_hidden = dot(cot_rows, down_w)
        sig = jax.nn.sigmoid(gate)
        silu = gate * sig
        d_gate = (d_hidden * up * (sig * (1.0 + gate * (1.0 - sig)))).astype(BF16)
        d_up = (d_hidden * silu).astype(BF16)
        acts[j][0] = d_gate
        acts[j][1] = d_up
        acts[j][2] = (silu * up).astype(BF16)
        grad = grad + dot_nt(d_gate, gate_w) + dot_nt(d_up, up_w)

    line = iota((8 * N_EXP, ROWS), 0)
    spread = (iota((8 * N_EXP, ROWS), 1) == (line >> 3) * PART + (line & 7)) & ((line & 7) < PART)
    back = dot(jnp.where(spread, 1.0, 0.0).astype(BF16), grad.astype(BF16)).reshape(N_EXP, 8, D)
    for t in range(N_TP):
        for h in range(2):
            at = 256 * t + 128 * h
            out_ref[:, t, 8 * h : 8 * h + 8, :] = back[:, :, at : at + 128].astype(BF16)


def experts(rows, weights):
    act = pltpu.HBM((3, ROWS, 256), BF16)
    return pl.pallas_call(
        expert_kernel,
        in_specs=[pl.BlockSpec(memory_space=pltpu.VMEM)] + [pl.BlockSpec(memory_space=pl.ANY)] * 16,
        out_shape=(pltpu.HBM((N_EXP, N_TP, 16, 128), BF16), act, act, act, act),
        scratch_shapes=[
            pltpu.VMEM((4, 3 * D, 256), BF16),
            pltpu.SemaphoreType.DMA((4, 4)),
        ],
        compiler_params=vmem(32),
        name="experts",
    )(*in_hbm(rows, *weights))


def weight_grad_kernel(*refs):
    rows, far, acts = refs[0:3], refs[3:5], refs[5:9]
    keep_g, send_g, keep_u, send_u, keep_d, send_d, xbuf, hbuf, sems = refs[9:]
    copies = []
    for n in range(4):
        at = pl.ds(ROWS * n, ROWS)
        if n < 3:
            copies.append(pltpu.make_async_copy(rows[n], xbuf.at[:, at, :], sems.at[0, n]))
        copies.append(pltpu.make_async_copy(acts[n], hbuf.at[:, at, :], sems.at[1, n]))
    for n in range(2):
        copies.append(pltpu.make_async_copy(far[n], xbuf.at[n, pl.ds(3 * ROWS, ROWS), :], sems.at[0, 3 + n]))
    for copy in copies:
        copy.start()
    for copy in copies:
        copy.wait()
    for n, (keep, send) in enumerate(((keep_g, send_g), (keep_u, send_u))):
        both = dot_tn(xbuf[0], hbuf[n])
        keep[...] = both[:, :128]
        send[...] = both[:, 128:]
    both = dot_tn(hbuf[2], xbuf[1])
    keep_d[...] = both[:128]
    send_d[...] = both[128:]


def weight_grads(rows, far, acts):
    tall = pltpu.HBM((D, 128), F32)
    wide = pltpu.HBM((128, D), F32)
    return pl.pallas_call(
        weight_grad_kernel,
        in_specs=[pl.BlockSpec(memory_space=pl.ANY)] * 9,
        out_shape=(tall, tall, tall, tall, wide, wide),
        scratch_shapes=[
            pltpu.VMEM((2, 4 * ROWS, D), BF16),
            pltpu.VMEM((3, 4 * ROWS, 256), BF16),
            pltpu.SemaphoreType.DMA((2, 5)),
        ],
        compiler_params=vmem(26),
        name="weight_grads",
    )(*in_hbm(*rows, *far, *acts))


def combine_kernel(tp_ref, place_ref, back_ref, cot_ref, out_ref):
    halves = [
        back_ref[:, 8 * h : 8 * h + 8, :].astype(F32).reshape(8 * N_TP * N_EXP, 128).astype(BF16) for h in range(2)
    ]
    routed = dot(place_ref[...], jnp.concatenate(halves, axis=1))
    out_ref[...] = (cot_ref[...].astype(F32) + routed).T.astype(BF16)


def combine(tp, placed, back, cotangent):
    cols = D // N_TP
    return pl.pallas_call(
        combine_kernel,
        grid_spec=pltpu.PrefetchScalarGridSpec(
            num_scalar_prefetch=1,
            grid=(1,),
            in_specs=[
                pl.BlockSpec(placed.shape, lambda n, s: (0, 0)),
                pl.BlockSpec(back.shape, lambda n, s: (0, 0, 0)),
                pl.BlockSpec((TOK, cols), lambda n, s: (0, s[0])),
            ],
            out_specs=pl.BlockSpec((cols, TOK), lambda n, s: (0, 0)),
        ),
        out_shape=jax.ShapeDtypeStruct((cols, TOK), BF16),
        compiler_params=vmem(12),
        name="combine",
    )(tp, *in_hbm(placed, back), cotangent)


def prepare_kernel(gate_ref, log_ref, before_ref, step_ref, mixed_ref, gelu_ref, slope_ref, prefix_ref):
    lane = iota((STRIP, TOK), 1)

    def strip(n, _):
        at = pl.ds(pl.multiple_of(n * STRIP, STRIP), STRIP)
        x = gate_ref[at, :].astype(F32)
        th = jnp.tanh(GELU_C * (x + GELU_A * (x * x * x)))
        gelu = 0.5 * x * (1.0 + th)
        back = 0.5 * (1.0 + th) + 0.5 * x * (1.0 - th * th) * (GELU_C * (1.0 + 3.0 * GELU_A * (x * x)))
        logs = log_ref[at, :]
        states = jnp.exp(logs) * before_ref[at, :] + step_ref[at, :].astype(F32)
        mixed_ref[at, :] = (gelu * states).astype(BF16)
        gelu_ref[at, :] = gelu
        slope_ref[at, :] = states * back
        total = logs
        d = 1
        while d < TOK:
            total = total + jnp.where(lane >= d, pltpu.roll(total, d, 1), 0.0)
            d *= 2
        prefix_ref[at, :] = jnp.exp(total)
        return 0

    lax.fori_loop(0, CH // STRIP, strip, 0)


def prepare(gate_pre, log_decay, state_before, step_input):
    shape = gate_pre.shape
    wide = pltpu.HBM(shape, F32)
    return pl.pallas_call(
        prepare_kernel,
        out_shape=(pltpu.HBM(shape, BF16), wide, wide, wide),
        compiler_params=vmem(8),
        name="prepare",
    )(gate_pre, log_decay, state_before, step_input)


def project_kernel(order_ref, *refs):
    grads, (proj_ref, mixed_ref, gelu_ref, slope_ref, prefix_ref) = refs[:8], refs[8:13]
    pieces, (ggp_ref, direct_ref, link_ref, block_ref, turn_ref) = refs[13:17], refs[17:]
    d_mixed = jnp.zeros((CH, TOK), F32)
    for k in range(N_TP):
        group = order_ref[k]
        grad = grads[k][...]
        cols = pl.ds(pl.multiple_of(group * 256, 256), 256)
        d_mixed = d_mixed + dot(proj_ref[:, cols], grad)
        block_ref[...] = dot(grad, mixed_ref[...])
        for m in range(4):
            at = pl.ds(pl.multiple_of(((order_ref[8] + m) & 3) * 64, 64), 64)
            pieces[m][pl.ds(group, 1)] = block_ref[at, :].astype(BF16)[None]
    ggp_ref[...] = (d_mixed * slope_ref[...]).astype(BF16)
    direct = d_mixed * gelu_ref[...]
    direct_ref[...] = direct
    turn_ref[...] = jnp.zeros_like(turn_ref)
    turn_ref[0:CH, 0:1] = prefix_ref[:, TOK - 1 : TOK]
    turn_ref[0:CH, 1:2] = jnp.sum(prefix_ref[...] * direct, axis=1, keepdims=True)
    link_ref[...] = turn_ref[...].T[0:2, 0:CH]


def project(order, grads, out_proj, mixed, gelu, slope, prefix):
    piece = pltpu.HBM((8, 64, CH), BF16)
    return pl.pallas_call(
        project_kernel,
        in_specs=[pl.BlockSpec(memory_space=pltpu.SMEM)] + [pl.BlockSpec(memory_space=pltpu.VMEM)] * 13,
        out_shape=(
            piece, piece, piece, piece,
            pltpu.HBM((CH, TOK), BF16),
            pltpu.HBM((CH, TOK), F32),
            pltpu.HBM((2, CH), F32),
        ),
        scratch_shapes=[pltpu.VMEM((256, CH), F32), pltpu.VMEM((TOK, 128), F32)],
        compiler_params=vmem(14),
        name="project",
    )(order, *grads, out_proj, mixed, gelu, slope, prefix)


def recur_kernel(at_ref, links_ref, direct_ref, log_ref, before_ref, step_ref, decay_ref, turn_ref, arrive_ref):
    mine = at_ref[0]
    arriving = jnp.zeros((1, CH), F32)
    for s in range(N_EXP - 1, 0, -1):
        arriving = jnp.where(s > mine, links_ref[s, 1:2, :] + links_ref[s, 0:1, :] * arriving, arriving)
    turn_ref[...] = jnp.zeros_like(turn_ref)
    turn_ref[0:1, 0:CH] = arriving
    arrive_ref[...] = turn_ref[...].T
    lane = iota((STRIP, TOK), 1)

    def strip(n, _):
        at = pl.ds(pl.multiple_of(n * STRIP, STRIP), STRIP)
        decays = jnp.exp(log_ref[at, :])
        a = jnp.where(lane < TOK - 1, pltpu.roll(decays, TOK - 1, 1), 1.0)
        b = direct_ref[at, :]
        d = 1
        while d < TOK:
            b = b + a * jnp.where(lane < TOK - d, pltpu.roll(b, TOK - d, 1), 0.0)
            a = a * jnp.where(lane < TOK - d, pltpu.roll(a, TOK - d, 1), 1.0)
            d *= 2
        g = b + a * arrive_ref[at, 0:1]
        step_ref[at, :] = g
        decay_ref[at, :] = g * decays * before_ref[at, :]
        return 0

    lax.fori_loop(0, CH // STRIP, strip, 0)


def recur(at, links, direct, log_decay, state_before):
    return pl.pallas_call(
        recur_kernel,
        in_specs=[pl.BlockSpec(memory_space=pltpu.SMEM)] + [pl.BlockSpec(memory_space=pltpu.VMEM)] * 4,
        out_shape=(
            jax.ShapeDtypeStruct((CH, TOK), F32),
            jax.ShapeDtypeStruct((CH, TOK), F32),
        ),
        scratch_shapes=[pltpu.VMEM((128, TOK), F32), pltpu.VMEM((TOK, 128), F32)],
        compiler_params=vmem(8),
        name="recur",
    )(at, links, direct, log_decay, state_before)


def shifted(value, axis, by):
    n = lax.axis_size(axis)
    return lax.ppermute(value, axis, [(i, (i + by) % n) for i in range(n)])


def on_device(resid, cotangent, routes, route_weight, w_gate, w_up, w_down, out_proj, gate_pre, log_decay,
              state_before, step_input):
    y, c = lax.axis_index("y"), lax.axis_index("c")
    tp = (2 * y + c).astype(jnp.int32)
    tp_vec = tp[None]

    own_a, own_b = pack(w_gate[0], w_up[0], w_down[0])
    prev_a = shifted(own_a, "y", 1)
    next_b = shifted(own_b, "y", -1)
    prev_b = shifted(own_b, "y", 1)
    next_a = shifted(own_a, "y", -1)
    far_a = shifted(prev_a, "y", 1)
    far_b = shifted(next_b, "y", -1)
    mine = (own_a, own_b, prev_a, prev_b, next_a, next_b, far_a, far_b)
    weights = mine + tuple(shifted(w, "c", 1) for w in mine)

    sent = dispatch(tp_vec, routes.T, route_weight.T, resid, cotangent)
    got = lax.all_to_all(sent, SP, split_axis=0, concat_axis=0, tiled=True)

    placed = place(routes)
    log_t, before_t = log_decay.T, state_before.T
    mixed, gelu, slope, prefix = prepare(gate_pre.T, log_t, before_t, step_input.T)
    mixed = mixed.T
    ys = jnp.stack([y, y - 1, y + 1, y + 2]) % 4
    order = jnp.concatenate([2 * ys + c, 2 * ys + 1 - c, lax.axis_index("x")[None]]).astype(jnp.int32)
    got, mixed, order = lax.optimization_barrier((got, mixed, order))

    rows = select(got)
    rows_after = shifted(rows, "y", -1)
    rows_before = shifted(rows, "y", 1)
    back, *acts = experts(rows, weights)
    acts = (acts[0], shifted(acts[1], "y", -1), shifted(acts[2], "y", 1), shifted(acts[3], "y", 2))
    back = lax.all_to_all(back.reshape(N_EXP * N_TP, 16, 128), ALL, split_axis=0, concat_axis=0, tiled=True)
    part = combine(tp_vec, placed, back, cotangent)

    near = (part, shifted(part, "y", 1), shifted(part, "y", -1), shifted(part, "y", 2))
    grads = (*near, *(shifted(g, "c", 1) for g in near))
    *pieces, grad_gate_pre, direct, link = project(order, grads, out_proj.T, mixed, gelu, slope, prefix)

    far_in, far_cot, pieces[0] = lax.optimization_barrier((rows_before[0], rows_after[1], pieces[0]))

    over_x = [pieces[0]]
    for m in (1, 2, 3):
        over_x.append(shifted(pieces[m], "x", m))
    link = jnp.broadcast_to(link, (N_EXP, *link.shape))
    links = lax.all_to_all(link, SP, split_axis=0, concat_axis=0, tiled=True)
    over_x = sum(p.astype(F32) for p in over_x).astype(BF16)
    over_z = lax.all_to_all(over_x, "z", split_axis=0, concat_axis=0, tiled=True)
    grad_proj = over_z.astype(F32).sum(axis=0)

    sp = (4 * lax.axis_index("z") + lax.axis_index("x")).astype(jnp.int32)
    grad_step_input, grad_log_decay = recur(sp[None], links, direct, log_t, before_t)

    far_in = shifted(far_in, "y", 1)
    far_cot = shifted(far_cot, "y", -1)
    far = (far_in, far_cot)
    keep_g, send_g, keep_u, send_u, keep_d, send_d = weight_grads(
        (rows, rows_after, rows_before), far, acts
    )
    grad_gate = keep_g + shifted(send_g, "c", 1)
    grad_up = keep_u + shifted(send_u, "c", 1)
    grad_down = keep_d + shifted(send_d, "c", 1)
    return (
        grad_gate[None],
        grad_up[None],
        grad_down[None],
        grad_proj,
        grad_gate_pre.T,
        grad_step_input.T,
        grad_log_decay.T,
    )


def solution(mesh):
    grid = Mesh(mesh.devices.reshape(8, 4, 4, 2), ALL)


    return jax.shard_map(
        on_device,
        mesh=grid,
        in_specs=(
            P(SP, None),
            P(SP, None),
            P(SP, None),
            P(SP, None),
            P(SP, None, TP),
            P(SP, None, TP),
            P(SP, TP, None),
            P(None, TP),
            P(SP, TP),
            P(SP, TP),
            P(SP, TP),
            P(SP, TP),
        ),
        out_specs=(
            P(SP, None, TP),
            P(SP, None, TP),
            P(SP, TP, None),
            P(SP, TP),
            P(SP, TP),
            P(SP, TP),
            P(SP, TP),
        ),
        check_vma=False,
    )
```

```python
import functools

import jax
import jax.numpy as jnp
from jax import lax
from jax.experimental import pallas as pl
from jax.experimental.pallas import tpu as pltpu
from jax.sharding import Mesh, PartitionSpec as P


BF16 = jnp.bfloat16
F32 = jnp.float32
SP = ("z", "x")
TP = ("y", "c")
ALL = ("z", "x", "y", "c")

TOK = 384
D = 2048
CAP = 48
N_EXP = 32
N_TP = 8
PART = CAP // N_TP
ROWS = N_EXP * PART
CH = 352
STRIP = 32
GELU_C = 0.7978845608028654
GELU_A = 0.044715


def iota(shape, dim):
    return lax.broadcasted_iota(jnp.int32, shape, dim)


def in_hbm(*arrays):
    held = tuple(pltpu.with_memory_space_constraint(a, pltpu.HBM) for a in arrays)
    return held if len(held) > 1 else held[0]


def vmem(mib):
    return pltpu.CompilerParams(vmem_limit_bytes=mib * 1024 * 1024)


def dot(a, b):
    return jnp.dot(a, b, preferred_element_type=F32)


def dot_nt(a, b):
    return lax.dot_general(a, b, (((1,), (1,)), ((), ())), preferred_element_type=F32)


def dot_tn(a, b):
    return lax.dot_general(a, b, (((0,), (0,)), ((), ())), preferred_element_type=F32)


FIRST = (6, 4, 2)


def pack_kernel(gate_ref, up_ref, down_ref, a_ref, b_ref, abuf, bbuf, down_buf, sems):
    third = D // 2
    loads = [
        pltpu.make_async_copy(down_ref, down_buf, sems.at[0]),
        pltpu.make_async_copy(gate_ref, abuf.at[pl.ds(0, D)], sems.at[1]),
        pltpu.make_async_copy(up_ref.at[pl.ds(0, third)], abuf.at[pl.ds(D, third)], sems.at[2]),
        pltpu.make_async_copy(up_ref.at[pl.ds(third, third)], bbuf.at[pl.ds(0, third)], sems.at[3]),
    ]
    for load in loads:
        load.start()
    loads[1].wait()
    loads[2].wait()
    out_a = pltpu.make_async_copy(abuf, a_ref, sems.at[4])
    out_a.start()
    loads[0].wait()
    bbuf[third:, :] = down_buf[...].T
    loads[3].wait()
    out_b = pltpu.make_async_copy(bbuf, b_ref, sems.at[5])
    out_b.start()
    out_a.wait()
    out_b.wait()


def pack(gate, up, down):
    anywhere = pl.BlockSpec(memory_space=pl.ANY)
    half = pltpu.HBM((3 * D // 2, 128), BF16)
    return pl.pallas_call(
        pack_kernel,
        in_specs=[anywhere] * 3,
        out_specs=(anywhere, anywhere),
        out_shape=(half, half),
        scratch_shapes=[
            pltpu.VMEM((3 * D // 2, 128), BF16),
            pltpu.VMEM((3 * D // 2, 128), BF16),
            pltpu.VMEM((128, D), BF16),
            pltpu.SemaphoreType.DMA((6,)),
        ],
        compiler_params=vmem(4),
        name="pack",
    )(*in_hbm(gate, up, down))


def dispatch_kernel(tp_ref, routes_ref, weight_ref, res_a, res_b, cot_a, cot_b, out_ref, pick_ref, scale_ref):
    @pl.when(pl.program_id(0) == 0)
    def _():
        r0, r1 = routes_ref[0:1, :], routes_ref[1:2, :]
        e = iota((N_EXP, TOK), 0)
        oh0, oh1 = e == r0, e == r1
        member = jnp.where(oh0 | oh1, 1.0, 0.0).astype(BF16)
        before = jnp.where(iota((TOK, TOK), 0) < iota((TOK, TOK), 1), 1.0, 0.0).astype(BF16)
        rank = dot(member, before)
        s0 = r0 * CAP + jnp.sum(jnp.where(oh0, rank, 0.0), axis=0, keepdims=True).astype(jnp.int32)
        s1 = r1 * CAP + jnp.sum(jnp.where(oh1, rank, 0.0), axis=0, keepdims=True).astype(jnp.int32)
        row = iota((8 * N_EXP, TOK), 0)
        q = row & 7
        for j in range(3):
            first = q < FIRST[j]
            i = 8 * j + q - jnp.where(first, 6 * j, 6 * (j + 1))
            slot = (row >> 3) * CAP + PART * tp_ref[0] + i
            m0, m1 = slot == s0, slot == s1
            hit = m0 | m1
            pick_ref[j, :, :TOK] = jnp.where(hit & first, 1.0, 0.0).astype(BF16)
            pick_ref[j, :, TOK:] = jnp.where(hit & ~first, 1.0, 0.0).astype(BF16)
            w = jnp.where(m0, weight_ref[0:1, :], 0.0) + jnp.where(m1, weight_ref[1:2, :], 0.0)
            w = jnp.sum(w, axis=1, keepdims=True)
            cot_row = (q[:, 0:1] < FIRST[j]) if j % 2 else (q[:, 0:1] >= FIRST[j])
            scale_ref[j] = jnp.broadcast_to(jnp.where(cot_row, w, 1.0), (8 * N_EXP, 128))

    classes = (res_a, cot_a, res_b, cot_b)
    for j in range(3):
        rhs = jnp.concatenate([classes[j][...], classes[j + 1][...]], axis=0)
        got = dot(pick_ref[j], rhs) * scale_ref[j][:, 0:1]
        out_ref[:, 8 * j : 8 * j + 8, :] = got.reshape(N_EXP, 8, got.shape[1]).astype(BF16)


def dispatch(tp, routes_t, weight_t, resid, cotangent):
    bn = 256
    half = D // 2 // bn
    return pl.pallas_call(
        dispatch_kernel,
        grid_spec=pltpu.PrefetchScalarGridSpec(
            num_scalar_prefetch=1,
            grid=(half,),
            in_specs=[
                pl.BlockSpec((2, TOK), lambda n, s: (0, 0)),
                pl.BlockSpec((2, TOK), lambda n, s: (0, 0)),
                pl.BlockSpec((TOK, bn), lambda n, s: (0, n)),
                pl.BlockSpec((TOK, bn), lambda n, s: (0, n + half)),
                pl.BlockSpec((TOK, bn), lambda n, s: (0, n)),
                pl.BlockSpec((TOK, bn), lambda n, s: (0, n + half)),
            ],
            out_specs=pl.BlockSpec((N_EXP, 24, bn), lambda n, s: (0, 0, n)),
            scratch_shapes=[
                pltpu.VMEM((3, 8 * N_EXP, 2 * TOK), BF16),
                pltpu.VMEM((3, 8 * N_EXP, 128), F32),
            ],
        ),
        out_shape=pltpu.HBM((N_EXP, 24, D // 2), BF16),
        compiler_params=vmem(14),
        name="dispatch",
    )(tp, routes_t, weight_t, resid, resid, cotangent, cotangent)


def place_kernel(routes_ref, out_ref):
    r0, r1 = routes_ref[:, 0:1], routes_ref[:, 1:2]
    e = iota((TOK, N_EXP), 1)
    oh0, oh1 = e == r0, e == r1
    member = jnp.where(oh0 | oh1, 1.0, 0.0).astype(BF16)
    before = jnp.where(iota((TOK, TOK), 1) < iota((TOK, TOK), 0), 1.0, 0.0).astype(BF16)
    rank = dot(before, member)

    def line(oh, r):
        k = jnp.sum(jnp.where(oh, rank, 0.0), axis=1, keepdims=True).astype(jnp.int32)
        t = (k * 43) >> 8
        return r * 64 + t * 8 + (k - t * PART)

    col = iota((TOK, 8 * N_TP * N_EXP), 1)
    hit = (col == line(oh0, r0)) | (col == line(oh1, r1))
    out_ref[...] = jnp.where(hit, 1.0, 0.0).astype(BF16)


def place(routes):
    return pl.pallas_call(
        place_kernel,
        out_shape=pltpu.HBM((TOK, 8 * N_TP * N_EXP), BF16),
        compiler_params=vmem(8),
        name="place",
    )(routes)


def select_kernel(got_ref, rows_ref):
    tiles = [
        got_ref[:, 8 * j : 8 * j + 8, :].astype(F32).reshape(8 * N_EXP, D // 2).astype(BF16) for j in range(3)
    ]
    k = iota((ROWS, 8 * N_EXP), 0)
    col = iota((ROWS, 8 * N_EXP), 1)
    source, q = col >> 3, col & 7
    for cls in range(4):
        total = None
        for j in (cls - 1, cls):
            if 0 <= j < 3:
                i = 8 * j + q - 6 * cls
                sel = jnp.where((k == source * PART + i) & (i >= 0) & (i < PART), 1.0, 0.0).astype(BF16)
                part = dot(sel, tiles[j])
                total = part if total is None else total + part
        rows_ref[cls % 2, :, (cls // 2) * (D // 2) : (cls // 2 + 1) * (D // 2)] = total.astype(BF16)


def select(got):
    return pl.pallas_call(
        select_kernel,
        out_shape=pltpu.HBM((2, ROWS, D), BF16),
        compiler_params=vmem(12),
        name="select",
    )(got)


def expert_kernel(rows_ref, *refs):
    weights, out_ref, acts_ref = refs[:16], refs[16], refs[17]
    gate_up, down, grads, sems = refs[18:]
    mid = D // 2
    copies = [[], [], [], []]
    for j in range(4):
        for side in range(2):
            part_a, part_b = weights[8 * side + 2 * j], weights[8 * side + 2 * j + 1]
            at = 128 * side
            g, u, d = pl.ds(512 * j + at, 128), pl.ds(512 * j + 256 + at, 128), pl.ds(256 * j + at, 128)
            moves = (
                (part_a.at[pl.ds(0, D)], gate_up.at[:, g]),
                (part_a.at[pl.ds(D, mid)], gate_up.at[pl.ds(0, mid), u]),
                (part_b.at[pl.ds(0, mid)], gate_up.at[pl.ds(mid, mid), u]),
                (part_b.at[pl.ds(mid, D)], down.at[:, d]),
            )
            for n, (src, dst) in enumerate(moves):
                copies[j].append(pltpu.make_async_copy(src, dst, sems.at[j, 4 * side + n]))
    for group in copies:
        for copy in group:
            copy.start()

    def chunk(j, _):
        for n in range(4):
            @pl.when(j == n)
            def _():
                for copy in copies[n]:
                    copy.wait()

        at = pl.multiple_of(512 * j, 512)
        both = dot(rows_ref[0], gate_up[:, pl.ds(at, 512)])
        gate, up = both[:, :256], both[:, 256:]
        d_hidden = dot(rows_ref[1], down[:, pl.ds(pl.multiple_of(256 * j, 256), 256)])
        sig = jax.nn.sigmoid(gate)
        silu = gate * sig
        d_gate = (d_hidden * up * (sig * (1.0 + gate * (1.0 - sig)))).astype(BF16)
        d_up = (d_hidden * silu).astype(BF16)
        acts_ref[j, 0] = d_gate
        acts_ref[j, 1] = d_up
        acts_ref[j, 2] = (silu * up).astype(BF16)
        grads[:, pl.ds(at, 256)] = d_gate
        grads[:, pl.ds(pl.multiple_of(at + 256, 256), 256)] = d_up
        return 0

    lax.fori_loop(0, 4, chunk, 0)
    line = iota((8 * N_EXP, ROWS), 0)
    spread = (iota((8 * N_EXP, ROWS), 1) == (line >> 3) * PART + (line & 7)) & ((line & 7) < PART)
    spread = jnp.where(spread, 1.0, 0.0).astype(BF16)

    def columns(t, _):
        rows = pl.ds(pl.multiple_of(256 * t, 256), 256)
        back = dot(spread, dot_nt(grads[...], gate_up[rows, :]).astype(BF16)).reshape(N_EXP, 8, 256)
        for h in range(2):
            out_ref[:, t, 8 * h : 8 * h + 8, :] = back[:, :, 128 * h : 128 * h + 128].astype(BF16)
        return 0

    lax.fori_loop(0, N_TP, columns, 0)


def experts(rows, weights):
    return pl.pallas_call(
        expert_kernel,
        in_specs=[pl.BlockSpec(memory_space=pltpu.VMEM)] + [pl.BlockSpec(memory_space=pl.ANY)] * 16,
        out_shape=(pltpu.HBM((N_EXP, N_TP, 16, 128), BF16), pltpu.HBM((4, 3, ROWS, 256), BF16)),
        scratch_shapes=[
            pltpu.VMEM((D, D), BF16),
            pltpu.VMEM((D, D // 2), BF16),
            pltpu.VMEM((ROWS, D), BF16),
            pltpu.SemaphoreType.DMA((4, 8)),
        ],
        compiler_params=vmem(32),
        name="experts",
    )(*in_hbm(rows, *weights))


def weight_grad_kernel(*refs):
    rows, far, acts = refs[0:3], refs[3:5], refs[5:9]
    keep_ref, send_ref, xbuf, hbuf, sems = refs[9:]
    copies = []
    for n in range(4):
        at = pl.ds(ROWS * n, ROWS)
        if n < 3:
            copies.append(pltpu.make_async_copy(rows[n], xbuf.at[:, at, :], sems.at[0, n]))
        act = acts[n].at[0] if n == 0 else acts[n]
        copies.append(pltpu.make_async_copy(act, hbuf.at[:, at, :], sems.at[1, n]))
    for n in range(2):
        copies.append(pltpu.make_async_copy(far[n], xbuf.at[n, pl.ds(3 * ROWS, ROWS), :], sems.at[0, 3 + n]))
    for copy in copies:
        copy.start()
    for copy in copies:
        copy.wait()

    def columns(t, _):
        cols = pl.ds(pl.multiple_of(256 * t, 256), 256)
        for n in range(2):
            both = dot_tn(xbuf[0, :, cols], hbuf[n])
            rows = pl.ds(pl.multiple_of(D * n + 256 * t, 256), 256)
            keep_ref[rows, :] = both[:, :128]
            send_ref[rows, :] = both[:, 128:]
        both = dot_tn(hbuf[2], xbuf[1, :, cols])
        for h in range(2):
            rows = pl.ds(pl.multiple_of(2 * D + 256 * t + 128 * h, 128), 128)
            keep_ref[rows, :] = both[:128, 128 * h : 128 * h + 128]
            send_ref[rows, :] = both[128:, 128 * h : 128 * h + 128]
        return 0

    lax.fori_loop(0, N_TP, columns, 0)


def weight_grads(rows, far, acts):
    part = pltpu.HBM((3 * D, 128), F32)
    return pl.pallas_call(
        weight_grad_kernel,
        in_specs=[pl.BlockSpec(memory_space=pl.ANY)] * 9,
        out_shape=(part, part),
        scratch_shapes=[
            pltpu.VMEM((2, 4 * ROWS, D), BF16),
            pltpu.VMEM((3, 4 * ROWS, 256), BF16),
            pltpu.SemaphoreType.DMA((2, 5)),
        ],
        compiler_params=vmem(26),
        name="weight_grads",
    )(*in_hbm(*rows, *far, *acts))


def finish_kernel(keep_g, keep_u, keep_d, got_g, got_u, got_d, gate_ref, up_ref, down_ref):
    gate_ref[...] = keep_g[...] + got_g[...]
    up_ref[...] = keep_u[...] + got_u[...]
    for n in range(4):
        rows = slice(128 * n, 128 * n + 128)
        down_ref[:, rows] = keep_d[rows, :] + got_d[rows, :]


def finish(keep, got):
    block = 512
    count = D // block
    tall = [pl.BlockSpec((block, 128), functools.partial(lambda k, n: (n + k * count, 0), k)) for k in range(3)]
    return pl.pallas_call(
        finish_kernel,
        grid=(count,),
        in_specs=tall + tall,
        out_specs=(tall[0], tall[0], pl.BlockSpec((128, block), lambda n: (0, n))),
        out_shape=(
            jax.ShapeDtypeStruct((D, 128), F32),
            jax.ShapeDtypeStruct((D, 128), F32),
            jax.ShapeDtypeStruct((128, D), F32),
        ),
        compiler_params=vmem(8),
        name="finish",
    )(*[in_hbm(keep)] * 3, *[in_hbm(got)] * 3)


def combine_kernel(tp_ref, place_ref, back_ref, cot_ref, out_ref):
    halves = [
        back_ref[:, 8 * h : 8 * h + 8, :].astype(F32).reshape(8 * N_TP * N_EXP, 128).astype(BF16) for h in range(2)
    ]
    routed = dot(place_ref[...], jnp.concatenate(halves, axis=1))
    out_ref[...] = (cot_ref[...].astype(F32) + routed).T.astype(BF16)


def combine(tp, placed, back, cotangent):
    cols = D // N_TP
    return pl.pallas_call(
        combine_kernel,
        grid_spec=pltpu.PrefetchScalarGridSpec(
            num_scalar_prefetch=1,
            grid=(1,),
            in_specs=[
                pl.BlockSpec(placed.shape, lambda n, s: (0, 0)),
                pl.BlockSpec(back.shape, lambda n, s: (0, 0, 0)),
                pl.BlockSpec((TOK, cols), lambda n, s: (0, s[0])),
            ],
            out_specs=pl.BlockSpec((cols, TOK), lambda n, s: (0, 0)),
        ),
        out_shape=jax.ShapeDtypeStruct((cols, TOK), BF16),
        compiler_params=vmem(12),
        name="combine",
    )(tp, in_hbm(placed), back, cotangent)


def prepare_kernel(gate_ref, log_ref, before_ref, step_ref, mixed_ref, gelu_ref, slope_ref, prefix_ref, suffix_ref, turn_ref):
    lane = iota((STRIP, TOK), 1)
    turn_ref[...] = jnp.zeros_like(turn_ref)

    def strip(n, _):
        at = pl.ds(pl.multiple_of(n * STRIP, STRIP), STRIP)
        x = gate_ref[at, :].astype(F32)
        th = jnp.tanh(GELU_C * (x + GELU_A * (x * x * x)))
        gelu = 0.5 * x * (1.0 + th)
        back = 0.5 * (1.0 + th) + 0.5 * x * (1.0 - th * th) * (GELU_C * (1.0 + 3.0 * GELU_A * (x * x)))
        logs = log_ref[at, :]
        states = jnp.exp(logs) * before_ref[at, :] + step_ref[at, :].astype(F32)
        turn_ref[at, :] = gelu * states
        gelu_ref[at, :] = gelu
        slope_ref[at, :] = states * back
        total = logs
        d = 1
        while d < TOK:
            total = total + jnp.where(lane >= d, pltpu.roll(total, d, 1), 0.0)
            d *= 2
        prefix_ref[at, :] = jnp.exp(total)
        suffix_ref[at, :] = jnp.exp(total[:, TOK - 1 : TOK] - total)
        return 0

    lax.fori_loop(0, CH // STRIP, strip, 0)
    mixed_ref[...] = turn_ref[...].T[:, :CH].astype(BF16)


def prepare(gate_pre, log_decay, state_before, step_input):
    shape = gate_pre.shape
    wide = pltpu.HBM(shape, F32)
    return pl.pallas_call(
        prepare_kernel,
        out_shape=(pltpu.HBM(shape[::-1], BF16), wide, wide, wide, wide),
        scratch_shapes=[pltpu.VMEM((TOK, TOK), F32)],
        compiler_params=vmem(8),
        name="prepare",
    )(gate_pre, log_decay, state_before, step_input)


def project_kernel(order_ref, *refs):
    grads, (proj_ref, mixed_ref, gelu_ref, slope_ref, prefix_ref) = refs[:8], refs[8:13]
    pieces, (ggp_ref, direct_ref, link_ref, block_ref, turn_ref) = refs[13:17], refs[17:]
    d_mixed = jnp.zeros((CH, TOK), F32)
    for k in range(N_TP):
        group = order_ref[k]
        grad = grads[k][...]
        cols = pl.ds(pl.multiple_of(group * 256, 256), 256)
        d_mixed = d_mixed + dot(proj_ref[:, cols], grad)
        block_ref[...] = dot(grad, mixed_ref[...])
        for m in range(4):
            at = pl.ds(pl.multiple_of(((order_ref[8] + m) & 3) * 64, 64), 64)
            pieces[m][pl.ds(group, 1)] = block_ref[at, :].astype(BF16)[None]
    ggp_ref[...] = (d_mixed * slope_ref[...]).astype(BF16)
    direct = d_mixed * gelu_ref[...]
    direct_ref[...] = direct
    turn_ref[...] = jnp.zeros_like(turn_ref)
    turn_ref[0:CH, 0:1] = prefix_ref[:, TOK - 1 : TOK]
    turn_ref[0:CH, 1:2] = jnp.sum(prefix_ref[...] * direct, axis=1, keepdims=True)
    link_ref[...] = turn_ref[...].T[0:2, 0:CH]


def project(order, grads, out_proj, mixed, gelu, slope, prefix):
    piece = pltpu.HBM((8, 64, CH), BF16)
    return pl.pallas_call(
        project_kernel,
        in_specs=[pl.BlockSpec(memory_space=pltpu.SMEM)] + [pl.BlockSpec(memory_space=pltpu.VMEM)] * 13,
        out_shape=(
            piece, piece, piece, piece,
            pltpu.HBM((CH, TOK), BF16),
            pltpu.HBM((CH, TOK), F32),
            pltpu.HBM((2, CH), F32),
        ),
        scratch_shapes=[pltpu.VMEM((256, CH), F32), pltpu.VMEM((TOK, 128), F32)],
        compiler_params=vmem(14),
        name="project",
    )(order, *grads, out_proj, mixed, gelu, slope, prefix)


def local_kernel(direct_ref, log_ref, out_ref):
    lane = iota((STRIP, TOK), 1)

    def strip(n, _):
        at = pl.ds(pl.multiple_of(n * STRIP, STRIP), STRIP)
        a = jnp.where(lane < TOK - 1, pltpu.roll(jnp.exp(log_ref[at, :]), TOK - 1, 1), 1.0)
        b = direct_ref[at, :]
        d = 1
        while d < TOK:
            b = b + a * jnp.where(lane < TOK - d, pltpu.roll(b, TOK - d, 1), 0.0)
            if 2 * d < TOK:
                a = a * jnp.where(lane < TOK - d, pltpu.roll(a, TOK - d, 1), 1.0)
            d *= 2
        out_ref[at, :] = b
        return 0

    lax.fori_loop(0, CH // STRIP, strip, 0)


def local_scan(direct, log_decay):
    return pl.pallas_call(
        local_kernel,
        out_shape=jax.ShapeDtypeStruct((CH, TOK), F32),
        compiler_params=vmem(6),
        name="local_scan",
    )(direct, log_decay)


def recur_kernel(at_ref, links_ref, local_ref, suffix_ref, log_ref, before_ref, step_ref, decay_ref, turn_ref):
    mine = at_ref[0]
    arriving = jnp.zeros((1, CH), F32)
    for s in range(N_EXP - 1, 0, -1):
        arriving = jnp.where(s > mine, links_ref[s, 1:2, :] + links_ref[s, 0:1, :] * arriving, arriving)
    turn_ref[...] = jnp.zeros_like(turn_ref)
    turn_ref[0:1, 0:CH] = arriving
    column = turn_ref[...].T[:CH, 0:1]
    g = local_ref[...] + suffix_ref[...] * column
    step_ref[...] = g
    decay_ref[...] = g * jnp.exp(log_ref[...]) * before_ref[...]


def recur(at, links, local, suffix, log_decay, state_before):
    return pl.pallas_call(
        recur_kernel,
        in_specs=[pl.BlockSpec(memory_space=pltpu.SMEM)] + [pl.BlockSpec(memory_space=pltpu.VMEM)] * 5,
        out_shape=(
            jax.ShapeDtypeStruct((CH, TOK), F32),
            jax.ShapeDtypeStruct((CH, TOK), F32),
        ),
        scratch_shapes=[pltpu.VMEM((128, TOK), F32)],
        compiler_params=vmem(8),
        name="recur",
    )(at, links, local, suffix, log_decay, state_before)


def shifted(value, axis, by):
    n = lax.axis_size(axis)
    return lax.ppermute(value, axis, [(i, (i + by) % n) for i in range(n)])


def on_device(resid, cotangent, routes, route_weight, w_gate, w_up, w_down, out_proj, gate_pre, log_decay,
              state_before, step_input):
    y, c = lax.axis_index("y"), lax.axis_index("c")
    tp = (2 * y + c).astype(jnp.int32)
    tp_vec = tp[None]

    own_a, own_b = pack(w_gate[0], w_up[0], w_down[0])
    prev_a = shifted(own_a, "y", 1)
    next_b = shifted(own_b, "y", -1)
    prev_b = shifted(own_b, "y", 1)
    next_a = shifted(own_a, "y", -1)
    far_a = shifted(prev_a, "y", 1)
    far_b = shifted(next_b, "y", -1)
    mine = (own_a, own_b, prev_a, prev_b, next_a, next_b, far_a, far_b)
    weights = mine + tuple(shifted(w, "c", 1) for w in mine)

    sent = dispatch(tp_vec, routes.T, route_weight.T, resid, cotangent)
    got = lax.all_to_all(sent, SP, split_axis=0, concat_axis=0, tiled=True)

    placed = place(routes)
    log_t, before_t = log_decay.T, state_before.T
    mixed, gelu, slope, prefix, suffix = prepare(gate_pre.T, log_t, before_t, step_input.T)
    ys = jnp.stack([y, y - 1, y + 1, y + 2]) % 4
    order = jnp.concatenate([2 * ys + c, 2 * ys + 1 - c, lax.axis_index("x")[None]]).astype(jnp.int32)
    got, order = lax.optimization_barrier((got, order))

    rows = select(got)
    rows_after = shifted(rows, "y", -1)
    rows_before = shifted(rows, "y", 1)
    back, acts = experts(rows, weights)
    back = lax.all_to_all(back.reshape(N_EXP * N_TP, 16, 128), ALL, split_axis=0, concat_axis=0, tiled=True)
    all_acts = [acts]
    for j, by in ((1, -1), (2, 1), (3, 2)):
        all_acts.append(shifted(acts[j], "y", by))
    part = combine(tp_vec, placed, back, cotangent)

    near = (part, shifted(part, "y", 1), shifted(part, "y", -1), shifted(part, "y", 2))
    grads = (*near, *(shifted(g, "c", 1) for g in near))
    *pieces, grad_gate_pre, direct, link = project(order, grads, out_proj.T, mixed, gelu, slope, prefix)

    far_in, far_cot, pieces[0] = lax.optimization_barrier((rows_before[0], rows_after[1], pieces[0]))

    over_x = [pieces[0]]
    for m in (1, 2, 3):
        over_x.append(shifted(pieces[m], "x", m))
    link = jnp.broadcast_to(link, (N_EXP, *link.shape))
    links = lax.all_to_all(link, SP, split_axis=0, concat_axis=0, tiled=True)
    over_x = sum(p.astype(F32) for p in over_x).astype(BF16)
    over_z = lax.all_to_all(over_x, "z", split_axis=0, concat_axis=0, tiled=True)
    grad_proj = over_z.astype(F32).sum(axis=0)

    sp = (4 * lax.axis_index("z") + lax.axis_index("x")).astype(jnp.int32)
    local = local_scan(direct, log_t)
    grad_step_input, grad_log_decay = recur(sp[None], links, local, suffix, log_t, before_t)

    far_in = shifted(far_in, "y", 1)
    far_cot = shifted(far_cot, "y", -1)
    far = (far_in, far_cot)
    keep, send = weight_grads((rows, rows_after, rows_before), far, all_acts)
    send = shifted(send, "c", 1)
    grad_gate, grad_up, grad_down = finish(keep, send)
    return (
        grad_gate[None],
        grad_up[None],
        grad_down[None],
        grad_proj,
        grad_gate_pre.T,
        grad_step_input.T,
        grad_log_decay.T,
    )


def solution(mesh):
    grid = Mesh(mesh.devices.reshape(8, 4, 4, 2), ALL)


    return jax.shard_map(
        on_device,
        mesh=grid,
        in_specs=(
            P(SP, None),
            P(SP, None),
            P(SP, None),
            P(SP, None),
            P(SP, None, TP),
            P(SP, None, TP),
            P(SP, TP, None),
            P(None, TP),
            P(SP, TP),
            P(SP, TP),
            P(SP, TP),
            P(SP, TP),
        ),
        out_specs=(
            P(SP, None, TP),
            P(SP, None, TP),
            P(SP, TP, None),
            P(SP, TP),
            P(SP, TP),
            P(SP, TP),
            P(SP, TP),
        ),
        check_vma=False,
    )
```

```python
import jax
import jax.numpy as jnp
from jax import lax
from jax.experimental import pallas as pl
from jax.experimental.pallas import tpu as pltpu
from jax.sharding import Mesh, PartitionSpec as P


BF16 = jnp.bfloat16
F32 = jnp.float32
SP = ("z", "x")
TP = ("y", "c")
ALL = ("z", "x", "y", "c")

TOK = 384
D = 2048
CAP = 48
N_EXP = 32
N_TP = 8
PART = CAP // N_TP
ROWS = N_EXP * PART
CH = 352
STRIP = 32
GELU_C = 0.7978845608028654
GELU_A = 0.044715


def iota(shape, dim):
    return lax.broadcasted_iota(jnp.int32, shape, dim)


def in_hbm(*arrays):
    held = tuple(pltpu.with_memory_space_constraint(a, pltpu.HBM) for a in arrays)
    return held if len(held) > 1 else held[0]


def vmem(mib):
    return pltpu.CompilerParams(vmem_limit_bytes=mib * 1024 * 1024)


def dot(a, b):
    return jnp.dot(a, b, preferred_element_type=F32)


def dot_nt(a, b):
    return lax.dot_general(a, b, (((1,), (1,)), ((), ())), preferred_element_type=F32)


def dot_tn(a, b):
    return lax.dot_general(a, b, (((0,), (0,)), ((), ())), preferred_element_type=F32)


FIRST = (6, 4, 2)


def pack_kernel(gate_ref, up_ref, down_ref, a_ref, b_ref, abuf, bbuf, down_buf, sems):
    third = D // 2
    loads = [
        pltpu.make_async_copy(down_ref, down_buf, sems.at[0]),
        pltpu.make_async_copy(gate_ref, abuf.at[pl.ds(0, D)], sems.at[1]),
        pltpu.make_async_copy(up_ref.at[pl.ds(0, third)], abuf.at[pl.ds(D, third)], sems.at[2]),
        pltpu.make_async_copy(up_ref.at[pl.ds(third, third)], bbuf.at[pl.ds(0, third)], sems.at[3]),
    ]
    for load in loads:
        load.start()
    loads[1].wait()
    loads[2].wait()
    out_a = pltpu.make_async_copy(abuf, a_ref, sems.at[4])
    out_a.start()
    loads[0].wait()
    bbuf[third:, :] = down_buf[...].T
    loads[3].wait()
    out_b = pltpu.make_async_copy(bbuf, b_ref, sems.at[5])
    out_b.start()
    out_a.wait()
    out_b.wait()


def pack(gate, up, down):
    anywhere = pl.BlockSpec(memory_space=pl.ANY)
    half = pltpu.HBM((3 * D // 2, 128), BF16)
    return pl.pallas_call(
        pack_kernel,
        in_specs=[anywhere] * 3,
        out_specs=(anywhere, anywhere),
        out_shape=(half, half),
        scratch_shapes=[
            pltpu.VMEM((3 * D // 2, 128), BF16),
            pltpu.VMEM((3 * D // 2, 128), BF16),
            pltpu.VMEM((128, D), BF16),
            pltpu.SemaphoreType.DMA((6,)),
        ],
        compiler_params=vmem(4),
        name="pack",
    )(*in_hbm(gate, up, down))


def dispatch_kernel(tp_ref, routes_ref, weight_ref, res_a, res_b, cot_a, cot_b, out_ref, pick_ref, scale_ref):
    @pl.when(pl.program_id(0) == 0)
    def _():
        r0, r1 = routes_ref[0:1, :], routes_ref[1:2, :]
        e = iota((N_EXP, TOK), 0)
        oh0, oh1 = e == r0, e == r1
        member = jnp.where(oh0 | oh1, 1.0, 0.0).astype(BF16)
        before = jnp.where(iota((TOK, TOK), 0) < iota((TOK, TOK), 1), 1.0, 0.0).astype(BF16)
        rank = dot(member, before)
        s0 = r0 * CAP + jnp.sum(jnp.where(oh0, rank, 0.0), axis=0, keepdims=True).astype(jnp.int32)
        s1 = r1 * CAP + jnp.sum(jnp.where(oh1, rank, 0.0), axis=0, keepdims=True).astype(jnp.int32)
        row = iota((8 * N_EXP, TOK), 0)
        q = row & 7
        for j in range(3):
            first = q < FIRST[j]
            i = 8 * j + q - jnp.where(first, 6 * j, 6 * (j + 1))
            slot = (row >> 3) * CAP + PART * tp_ref[0] + i
            m0, m1 = slot == s0, slot == s1
            hit = m0 | m1
            pick_ref[j, :, :TOK] = jnp.where(hit & first, 1.0, 0.0).astype(BF16)
            pick_ref[j, :, TOK:] = jnp.where(hit & ~first, 1.0, 0.0).astype(BF16)
            w = jnp.where(m0, weight_ref[0:1, :], 0.0) + jnp.where(m1, weight_ref[1:2, :], 0.0)
            w = jnp.sum(w, axis=1, keepdims=True)
            cot_row = (q[:, 0:1] < FIRST[j]) if j % 2 else (q[:, 0:1] >= FIRST[j])
            scale_ref[j] = jnp.broadcast_to(jnp.where(cot_row, w, 1.0), (8 * N_EXP, 128))

    classes = (res_a, cot_a, res_b, cot_b)
    for j in range(3):
        rhs = jnp.concatenate([classes[j][...], classes[j + 1][...]], axis=0)
        got = dot(pick_ref[j], rhs) * scale_ref[j][:, 0:1]
        out_ref[:, 8 * j : 8 * j + 8, :] = got.reshape(N_EXP, 8, got.shape[1]).astype(BF16)


def dispatch(tp, routes_t, weight_t, resid, cotangent):
    bn = 256
    half = D // 2 // bn
    return pl.pallas_call(
        dispatch_kernel,
        grid_spec=pltpu.PrefetchScalarGridSpec(
            num_scalar_prefetch=1,
            grid=(half,),
            in_specs=[
                pl.BlockSpec((2, TOK), lambda n, s: (0, 0)),
                pl.BlockSpec((2, TOK), lambda n, s: (0, 0)),
                pl.BlockSpec((TOK, bn), lambda n, s: (0, n)),
                pl.BlockSpec((TOK, bn), lambda n, s: (0, n + half)),
                pl.BlockSpec((TOK, bn), lambda n, s: (0, n)),
                pl.BlockSpec((TOK, bn), lambda n, s: (0, n + half)),
            ],
            out_specs=pl.BlockSpec((N_EXP, 24, bn), lambda n, s: (0, 0, n)),
            scratch_shapes=[
                pltpu.VMEM((3, 8 * N_EXP, 2 * TOK), BF16),
                pltpu.VMEM((3, 8 * N_EXP, 128), F32),
            ],
        ),
        out_shape=pltpu.HBM((N_EXP, 24, D // 2), BF16),
        compiler_params=vmem(14),
        name="dispatch",
    )(tp, routes_t, weight_t, *in_hbm(resid, resid, cotangent, cotangent))


def place_kernel(routes_ref, out_ref):
    r0, r1 = routes_ref[:, 0:1], routes_ref[:, 1:2]
    e = iota((TOK, N_EXP), 1)
    oh0, oh1 = e == r0, e == r1
    member = jnp.where(oh0 | oh1, 1.0, 0.0).astype(BF16)
    before = jnp.where(iota((TOK, TOK), 1) < iota((TOK, TOK), 0), 1.0, 0.0).astype(BF16)
    rank = dot(before, member)

    def line(oh, r):
        k = jnp.sum(jnp.where(oh, rank, 0.0), axis=1, keepdims=True).astype(jnp.int32)
        t = (k * 43) >> 8
        return r * 64 + t * 8 + (k - t * PART)

    col = iota((TOK, 8 * N_TP * N_EXP), 1)
    hit = (col == line(oh0, r0)) | (col == line(oh1, r1))
    out_ref[...] = jnp.where(hit, 1.0, 0.0).astype(BF16)


def place(routes):
    return pl.pallas_call(
        place_kernel,
        out_shape=pltpu.HBM((TOK, 8 * N_TP * N_EXP), BF16),
        compiler_params=vmem(8),
        name="place",
    )(routes)


def select_kernel(got_ref, rows_ref):
    tiles = [
        got_ref[:, 8 * j : 8 * j + 8, :].astype(F32).reshape(8 * N_EXP, D // 2).astype(BF16) for j in range(3)
    ]
    k = iota((ROWS, 8 * N_EXP), 0)
    col = iota((ROWS, 8 * N_EXP), 1)
    source, q = col >> 3, col & 7
    for cls in range(4):
        total = None
        for j in (cls - 1, cls):
            if 0 <= j < 3:
                i = 8 * j + q - 6 * cls
                sel = jnp.where((k == source * PART + i) & (i >= 0) & (i < PART), 1.0, 0.0).astype(BF16)
                part = dot(sel, tiles[j])
                total = part if total is None else total + part
        rows_ref[cls % 2, :, (cls // 2) * (D // 2) : (cls // 2 + 1) * (D // 2)] = total.astype(BF16)


def select(got):
    return pl.pallas_call(
        select_kernel,
        out_shape=pltpu.HBM((2, ROWS, D), BF16),
        compiler_params=vmem(12),
        name="select",
    )(got)


def expert_kernel(rows_ref, *refs):
    weights, out_ref, acts = refs[:16], refs[16], refs[17:21]
    gate_up, down, grads, sems = refs[21:]
    mid = D // 2
    copies = [[], [], [], []]
    for j in range(4):
        for side in range(2):
            part_a, part_b = weights[8 * side + 2 * j], weights[8 * side + 2 * j + 1]
            at = 128 * side
            g, u, d = pl.ds(512 * j + at, 128), pl.ds(512 * j + 256 + at, 128), pl.ds(256 * j + at, 128)
            moves = (
                (part_a.at[pl.ds(0, D)], gate_up.at[:, g]),
                (part_a.at[pl.ds(D, mid)], gate_up.at[pl.ds(0, mid), u]),
                (part_b.at[pl.ds(0, mid)], gate_up.at[pl.ds(mid, mid), u]),
                (part_b.at[pl.ds(mid, D)], down.at[:, d]),
            )
            for n, (src, dst) in enumerate(moves):
                copies[j].append(pltpu.make_async_copy(src, dst, sems.at[j, 4 * side + n]))
    for group in copies:
        for copy in group:
            copy.start()

    def chunk(j, _):
        for n in range(4):
            @pl.when(j == n)
            def _():
                for copy in copies[n]:
                    copy.wait()

        at = pl.multiple_of(512 * j, 512)
        both = dot(rows_ref[0], gate_up[:, pl.ds(at, 512)])
        gate, up = both[:, :256], both[:, 256:]
        d_hidden = dot(rows_ref[1], down[:, pl.ds(pl.multiple_of(256 * j, 256), 256)])
        sig = jax.nn.sigmoid(gate)
        silu = gate * sig
        d_gate = (d_hidden * up * (sig * (1.0 + gate * (1.0 - sig)))).astype(BF16)
        d_up = (d_hidden * silu).astype(BF16)
        made = (d_gate, d_up, (silu * up).astype(BF16))
        for n in range(4):
            @pl.when(j == n)
            def _():
                for k in range(3):
                    acts[n][k] = made[k]

        grads[:, pl.ds(at, 256)] = d_gate
        grads[:, pl.ds(pl.multiple_of(at + 256, 256), 256)] = d_up
        return 0

    lax.fori_loop(0, 4, chunk, 0)
    line = iota((8 * N_EXP, ROWS), 0)
    spread = (iota((8 * N_EXP, ROWS), 1) == (line >> 3) * PART + (line & 7)) & ((line & 7) < PART)
    spread = jnp.where(spread, 1.0, 0.0).astype(BF16)

    def columns(t, _):
        rows = pl.ds(pl.multiple_of(256 * t, 256), 256)
        back = dot(spread, dot_nt(grads[...], gate_up[rows, :]).astype(BF16)).reshape(N_EXP, 8, 256)
        for h in range(2):
            out_ref[:, t, 8 * h : 8 * h + 8, :] = back[:, :, 128 * h : 128 * h + 128].astype(BF16)
        return 0

    lax.fori_loop(0, N_TP, columns, 0)


def experts(rows, weights):
    act = pltpu.HBM((3, ROWS, 256), BF16)
    return pl.pallas_call(
        expert_kernel,
        in_specs=[pl.BlockSpec(memory_space=pltpu.VMEM)] + [pl.BlockSpec(memory_space=pl.ANY)] * 16,
        out_shape=(pltpu.HBM((N_EXP, N_TP, 16, 128), BF16), act, act, act, act),
        scratch_shapes=[
            pltpu.VMEM((D, D), BF16),
            pltpu.VMEM((D, D // 2), BF16),
            pltpu.VMEM((ROWS, D), BF16),
            pltpu.SemaphoreType.DMA((4, 8)),
        ],
        compiler_params=vmem(32),
        name="experts",
    )(*in_hbm(rows, *weights))


def weight_grad_kernel(*refs):
    rows, acts = refs[0:3], refs[3:6]
    keep_ref, send_ref, xbuf, hbuf, sems = refs[6:]
    copies = []
    for n in range(3):
        at = pl.ds(ROWS * n, ROWS)
        copies.append(pltpu.make_async_copy(rows[n], xbuf.at[:, at, :], sems.at[0, n]))
        copies.append(pltpu.make_async_copy(acts[n], hbuf.at[:, at, :], sems.at[1, n]))
    for copy in copies:
        copy.start()
    for copy in copies:
        copy.wait()

    def columns(t, _):
        cols = pl.ds(pl.multiple_of(256 * t, 256), 256)
        for n in range(2):
            both = dot_tn(xbuf[0, :, cols], hbuf[n])
            keep_ref[n, cols, :] = both[:, :128]
            send_ref[n, cols, :] = both[:, 128:]
        both = dot_tn(hbuf[2], xbuf[1, :, cols])
        for h in range(2):
            at = pl.ds(pl.multiple_of(256 * t + 128 * h, 128), 128)
            keep_ref[2, at, :] = both[:128, 128 * h : 128 * h + 128]
            send_ref[2, at, :] = both[128:, 128 * h : 128 * h + 128]
        return 0

    lax.fori_loop(0, N_TP, columns, 0)


def weight_grads(rows, acts):
    part = pltpu.HBM((3, D, 128), F32)
    return pl.pallas_call(
        weight_grad_kernel,
        in_specs=[pl.BlockSpec(memory_space=pl.ANY)] * 6,
        out_shape=(part, part),
        scratch_shapes=[
            pltpu.VMEM((2, 3 * ROWS, D), BF16),
            pltpu.VMEM((3, 3 * ROWS, 256), BF16),
            pltpu.SemaphoreType.DMA((2, 3)),
        ],
        compiler_params=vmem(22),
        name="weight_grads",
    )(*in_hbm(*rows, *acts))


def far_grad_kernel(in_ref, cot_ref, act_ref, keep_in, send_in, keep_ref, send_ref):
    for n in range(2):
        both = dot_tn(in_ref[...], act_ref[n])
        keep_ref[n] = keep_in[n] + both[:, :128]
        send_ref[n] = send_in[n] + both[:, 128:]
    both = dot_tn(act_ref[2], cot_ref[...])
    for h in range(both.shape[1] // 128):
        at = slice(128 * h, 128 * h + 128)
        keep_ref[2, at, :] = keep_in[2, at, :] + both[:128, at]
        send_ref[2, at, :] = send_in[2, at, :] + both[128:, at]


def far_grads(far_in, far_cot, act, keep, send):
    block = 512
    part = pltpu.HBM((3, D, 128), F32)
    cols = pl.BlockSpec((ROWS, block), lambda t: (0, t))
    sums = pl.BlockSpec((3, block, 128), lambda t: (0, t, 0))
    return pl.pallas_call(
        far_grad_kernel,
        grid=(D // block,),
        in_specs=[cols, cols, pl.BlockSpec(act.shape, lambda t: (0, 0, 0)), sums, sums],
        out_specs=(sums, sums),
        out_shape=(part, part),
        compiler_params=vmem(12),
        name="far_grads",
    )(far_in, far_cot, act, *in_hbm(keep, send))


def finish_kernel(keep_ref, got_ref, gate_ref, up_ref, down_ref):
    gate_ref[...] = keep_ref[0] + got_ref[0]
    up_ref[...] = keep_ref[1] + got_ref[1]
    for n in range(keep_ref.shape[1] // 128):
        at = slice(128 * n, 128 * n + 128)
        down_ref[:, at] = keep_ref[2, at, :] + got_ref[2, at, :]


def finish(keep, got):
    block = 512
    sums = pl.BlockSpec((3, block, 128), lambda t: (0, t, 0))
    tall = pl.BlockSpec((block, 128), lambda t: (t, 0))
    return pl.pallas_call(
        finish_kernel,
        grid=(D // block,),
        in_specs=[sums, sums],
        out_specs=(tall, tall, pl.BlockSpec((128, block), lambda t: (0, t))),
        out_shape=(
            jax.ShapeDtypeStruct((D, 128), F32),
            jax.ShapeDtypeStruct((D, 128), F32),
            jax.ShapeDtypeStruct((128, D), F32),
        ),
        compiler_params=vmem(8),
        name="finish",
    )(*in_hbm(keep, got))


def combine_kernel(tp_ref, place_ref, back_ref, cot_ref, out_ref):
    halves = [
        back_ref[:, 8 * h : 8 * h + 8, :].astype(F32).reshape(8 * N_TP * N_EXP, 128).astype(BF16) for h in range(2)
    ]
    routed = dot(place_ref[...], jnp.concatenate(halves, axis=1))
    out_ref[...] = (cot_ref[...].astype(F32) + routed).T.astype(BF16)


def combine(tp, placed, back, cotangent):
    cols = D // N_TP
    return pl.pallas_call(
        combine_kernel,
        grid_spec=pltpu.PrefetchScalarGridSpec(
            num_scalar_prefetch=1,
            grid=(1,),
            in_specs=[
                pl.BlockSpec(placed.shape, lambda n, s: (0, 0)),
                pl.BlockSpec(back.shape, lambda n, s: (0, 0, 0)),
                pl.BlockSpec((TOK, cols), lambda n, s: (0, s[0])),
            ],
            out_specs=pl.BlockSpec((cols, TOK), lambda n, s: (0, 0)),
        ),
        out_shape=jax.ShapeDtypeStruct((cols, TOK), BF16),
        compiler_params=vmem(12),
        name="combine",
    )(tp, in_hbm(placed), back, cotangent)


def prepare_kernel(gate_ref, log_ref, before_ref, step_ref, mixed_ref, gelu_ref, slope_ref, prefix_ref, suffix_ref, turn_ref):
    lane = iota((STRIP, TOK), 1)
    turn_ref[...] = jnp.zeros_like(turn_ref)

    def strip(n, _):
        at = pl.ds(pl.multiple_of(n * STRIP, STRIP), STRIP)
        x = gate_ref[at, :].astype(F32)
        th = jnp.tanh(GELU_C * (x + GELU_A * (x * x * x)))
        gelu = 0.5 * x * (1.0 + th)
        back = 0.5 * (1.0 + th) + 0.5 * x * (1.0 - th * th) * (GELU_C * (1.0 + 3.0 * GELU_A * (x * x)))
        logs = log_ref[at, :]
        states = jnp.exp(logs) * before_ref[at, :] + step_ref[at, :].astype(F32)
        turn_ref[at, :] = gelu * states
        gelu_ref[at, :] = gelu
        slope_ref[at, :] = states * back
        total = logs
        d = 1
        while d < TOK:
            total = total + jnp.where(lane >= d, pltpu.roll(total, d, 1), 0.0)
            d *= 2
        prefix_ref[at, :] = jnp.exp(total)
        suffix_ref[at, :] = jnp.exp(total[:, TOK - 1 : TOK] - total)
        return 0

    lax.fori_loop(0, CH // STRIP, strip, 0)
    mixed_ref[...] = turn_ref[...].T[:, :CH].astype(BF16)


def prepare(gate_pre, log_decay, state_before, step_input):
    shape = gate_pre.shape
    wide = pltpu.HBM(shape, F32)
    return pl.pallas_call(
        prepare_kernel,
        out_shape=(pltpu.HBM(shape[::-1], BF16), wide, wide, wide, wide),
        scratch_shapes=[pltpu.VMEM((TOK, TOK), F32)],
        compiler_params=vmem(8),
        name="prepare",
    )(gate_pre, log_decay, state_before, step_input)


def project_kernel(order_ref, *refs):
    grads, (proj_ref, mixed_ref, gelu_ref, slope_ref, prefix_ref) = refs[:8], refs[8:13]
    pieces, (ggp_ref, direct_ref, link_ref, block_ref, turn_ref) = refs[13:17], refs[17:]
    d_mixed = jnp.zeros((CH, TOK), F32)
    for k in range(N_TP):
        group = order_ref[k]
        grad = grads[k][...]
        cols = pl.ds(pl.multiple_of(group * 256, 256), 256)
        d_mixed = d_mixed + dot(proj_ref[:, cols], grad)
        block_ref[...] = dot(grad, mixed_ref[...])
        for m in range(4):
            at = pl.ds(pl.multiple_of(((order_ref[8] + m) & 3) * 64, 64), 64)
            pieces[m][pl.ds(group, 1)] = block_ref[at, :].astype(BF16)[None]
    ggp_ref[...] = (d_mixed * slope_ref[...]).astype(BF16)
    direct = d_mixed * gelu_ref[...]
    direct_ref[...] = direct
    turn_ref[...] = jnp.zeros_like(turn_ref)
    turn_ref[0:CH, 0:1] = prefix_ref[:, TOK - 1 : TOK]
    turn_ref[0:CH, 1:2] = jnp.sum(prefix_ref[...] * direct, axis=1, keepdims=True)
    link_ref[...] = turn_ref[...].T[0:2, 0:CH]


def project(order, grads, out_proj, mixed, gelu, slope, prefix):
    piece = pltpu.HBM((8, 64, CH), BF16)
    return pl.pallas_call(
        project_kernel,
        in_specs=[pl.BlockSpec(memory_space=pltpu.SMEM)] + [pl.BlockSpec(memory_space=pltpu.VMEM)] * 13,
        out_shape=(
            piece, piece, piece, piece,
            pltpu.HBM((CH, TOK), BF16),
            pltpu.HBM((CH, TOK), F32),
            pltpu.HBM((2, CH), F32),
        ),
        scratch_shapes=[pltpu.VMEM((256, CH), F32), pltpu.VMEM((TOK, 128), F32)],
        compiler_params=vmem(14),
        name="project",
    )(order, *grads, out_proj, mixed, gelu, slope, prefix)


def local_kernel(direct_ref, log_ref, out_ref):
    lane = iota((STRIP, TOK), 1)

    def strip(n, _):
        at = pl.ds(pl.multiple_of(n * STRIP, STRIP), STRIP)
        a = jnp.where(lane < TOK - 1, pltpu.roll(jnp.exp(log_ref[at, :]), TOK - 1, 1), 1.0)
        b = direct_ref[at, :]
        d = 1
        while d < TOK:
            b = b + a * jnp.where(lane < TOK - d, pltpu.roll(b, TOK - d, 1), 0.0)
            if 2 * d < TOK:
                a = a * jnp.where(lane < TOK - d, pltpu.roll(a, TOK - d, 1), 1.0)
            d *= 2
        out_ref[at, :] = b
        return 0

    lax.fori_loop(0, CH // STRIP, strip, 0)


def local_scan(direct, log_decay):
    return pl.pallas_call(
        local_kernel,
        out_shape=jax.ShapeDtypeStruct((CH, TOK), F32),
        compiler_params=vmem(6),
        name="local_scan",
    )(direct, log_decay)


def recur_kernel(at_ref, links_ref, local_ref, suffix_ref, log_ref, before_ref, step_ref, decay_ref, turn_ref):
    mine = at_ref[0]
    arriving = jnp.zeros((1, CH), F32)
    for s in range(N_EXP - 1, 0, -1):
        arriving = jnp.where(s > mine, links_ref[s, 1:2, :] + links_ref[s, 0:1, :] * arriving, arriving)
    turn_ref[...] = jnp.zeros_like(turn_ref)
    turn_ref[0:1, 0:CH] = arriving
    column = turn_ref[...].T[:CH, 0:1]
    g = local_ref[...] + suffix_ref[...] * column
    step_ref[...] = g
    decay_ref[...] = g * jnp.exp(log_ref[...]) * before_ref[...]


def recur(at, links, local, suffix, log_decay, state_before):
    return pl.pallas_call(
        recur_kernel,
        in_specs=[pl.BlockSpec(memory_space=pltpu.SMEM)] + [pl.BlockSpec(memory_space=pltpu.VMEM)] * 5,
        out_shape=(
            jax.ShapeDtypeStruct((CH, TOK), F32),
            jax.ShapeDtypeStruct((CH, TOK), F32),
        ),
        scratch_shapes=[pltpu.VMEM((128, TOK), F32)],
        compiler_params=vmem(8),
        name="recur",
    )(at, links, local, suffix, log_decay, state_before)


def shifted(value, axis, by):
    n = lax.axis_size(axis)
    return lax.ppermute(value, axis, [(i, (i + by) % n) for i in range(n)])


def on_device(resid, cotangent, routes, route_weight, w_gate, w_up, w_down, out_proj, gate_pre, log_decay,
              state_before, step_input):
    y, c = lax.axis_index("y"), lax.axis_index("c")
    tp = (2 * y + c).astype(jnp.int32)
    tp_vec = tp[None]

    own_a, own_b = pack(w_gate[0], w_up[0], w_down[0])
    prev_a = shifted(own_a, "y", 1)
    next_b = shifted(own_b, "y", -1)
    prev_b = shifted(own_b, "y", 1)
    next_a = shifted(own_a, "y", -1)
    far_a = shifted(prev_a, "y", 1)
    far_b = shifted(next_b, "y", -1)
    mine = (own_a, own_b, prev_a, prev_b, next_a, next_b, far_a, far_b)
    weights = mine + tuple(shifted(w, "c", 1) for w in mine)

    sent = dispatch(tp_vec, routes.T, route_weight.T, resid, cotangent)
    got = lax.all_to_all(sent, SP, split_axis=0, concat_axis=0, tiled=True)

    placed = place(routes)
    log_t, before_t = log_decay.T, state_before.T
    mixed, gelu, slope, prefix, suffix = prepare(gate_pre.T, log_t, before_t, step_input.T)
    ys = jnp.stack([y, y - 1, y + 1, y + 2]) % 4
    order = jnp.concatenate([2 * ys + c, 2 * ys + 1 - c, lax.axis_index("x")[None]]).astype(jnp.int32)
    got, order = lax.optimization_barrier((got, order))

    rows = select(got)
    rows_after = shifted(rows, "y", -1)
    rows_before = shifted(rows, "y", 1)
    back, *acts = experts(rows, weights)
    back = lax.all_to_all(back.reshape(N_EXP * N_TP, 16, 128), ALL, split_axis=0, concat_axis=0, tiled=True)
    all_acts = [acts[0]]
    for j, by in ((1, -1), (2, 1), (3, 2)):
        all_acts.append(shifted(acts[j], "y", by))
    keep, send = weight_grads((rows, rows_after, rows_before), all_acts[:3])
    part = combine(tp_vec, placed, back, cotangent)

    near = (part, shifted(part, "y", 1), shifted(part, "y", -1), shifted(part, "y", 2))
    grads = (*near, *(shifted(g, "c", 1) for g in near))
    *pieces, grad_gate_pre, direct, link = project(order, grads, out_proj.T, mixed, gelu, slope, prefix)

    far_in, far_cot, pieces[0] = lax.optimization_barrier((rows_before[0], rows_after[1], pieces[0]))

    over_x = [pieces[0]]
    for m in (1, 2, 3):
        over_x.append(shifted(pieces[m], "x", m))
    link = jnp.broadcast_to(link, (N_EXP, *link.shape))
    links = lax.all_to_all(link, SP, split_axis=0, concat_axis=0, tiled=True)
    over_x = sum(p.astype(F32) for p in over_x).astype(BF16)
    over_z = lax.all_to_all(over_x, "z", split_axis=0, concat_axis=0, tiled=True)
    grad_proj = over_z.astype(F32).sum(axis=0)

    sp = (4 * lax.axis_index("z") + lax.axis_index("x")).astype(jnp.int32)
    local = local_scan(direct, log_t)
    grad_step_input, grad_log_decay = recur(sp[None], links, local, suffix, log_t, before_t)

    far_in = shifted(far_in, "y", 1)
    far_cot = shifted(far_cot, "y", -1)
    keep, send = far_grads(far_in, far_cot, all_acts[3], keep, send)
    send = shifted(send, "c", 1)
    grad_gate, grad_up, grad_down = finish(keep, send)
    return (
        grad_gate[None],
        grad_up[None],
        grad_down[None],
        grad_proj,
        grad_gate_pre.T,
        grad_step_input.T,
        grad_log_decay.T,
    )


def solution(mesh):
    grid = Mesh(mesh.devices.reshape(8, 4, 4, 2), ALL)


    return jax.shard_map(
        on_device,
        mesh=grid,
        in_specs=(
            P(SP, None),
            P(SP, None),
            P(SP, None),
            P(SP, None),
            P(SP, None, TP),
            P(SP, None, TP),
            P(SP, TP, None),
            P(None, TP),
            P(SP, TP),
            P(SP, TP),
            P(SP, TP),
            P(SP, TP),
        ),
        out_specs=(
            P(SP, None, TP),
            P(SP, None, TP),
            P(SP, TP, None),
            P(SP, TP),
            P(SP, TP),
            P(SP, TP),
            P(SP, TP),
        ),
        check_vma=False,
    )
```

```python
import jax
import jax.numpy as jnp
from jax import lax
from jax.experimental import pallas as pl
from jax.experimental.pallas import tpu as pltpu
from jax.sharding import Mesh, PartitionSpec as P


BF16 = jnp.bfloat16
F32 = jnp.float32
SP = ("z", "x")
TP = ("y", "c")
ALL = ("z", "x", "y", "c")

TOK = 384
D = 2048
CAP = 48
N_EXP = 32
N_TP = 8
PART = CAP // N_TP
ROWS = N_EXP * PART
CH = 352
STRIP = 32
GELU_C = 0.7978845608028654
GELU_A = 0.044715


def iota(shape, dim):
    return lax.broadcasted_iota(jnp.int32, shape, dim)


def in_hbm(*arrays):
    held = tuple(pltpu.with_memory_space_constraint(a, pltpu.HBM) for a in arrays)
    return held if len(held) > 1 else held[0]


def vmem(mib):
    return pltpu.CompilerParams(vmem_limit_bytes=mib * 1024 * 1024)


def dot(a, b):
    return jnp.dot(a, b, preferred_element_type=F32)


def dot_nt(a, b):
    return lax.dot_general(a, b, (((1,), (1,)), ((), ())), preferred_element_type=F32)


def dot_tn(a, b):
    return lax.dot_general(a, b, (((0,), (0,)), ((), ())), preferred_element_type=F32)


FIRST = (6, 4, 2)


def pack_kernel(gate_ref, up_ref, down_ref, a_ref, b_ref, abuf, bbuf, down_buf, sems):
    third = D // 2
    loads = [
        pltpu.make_async_copy(down_ref, down_buf, sems.at[0]),
        pltpu.make_async_copy(gate_ref, abuf.at[pl.ds(0, D)], sems.at[1]),
        pltpu.make_async_copy(up_ref.at[pl.ds(0, third)], abuf.at[pl.ds(D, third)], sems.at[2]),
        pltpu.make_async_copy(up_ref.at[pl.ds(third, third)], bbuf.at[pl.ds(0, third)], sems.at[3]),
    ]
    for load in loads:
        load.start()
    loads[1].wait()
    loads[2].wait()
    out_a = pltpu.make_async_copy(abuf, a_ref, sems.at[4])
    out_a.start()
    loads[0].wait()
    bbuf[third:, :] = down_buf[...].T
    loads[3].wait()
    out_b = pltpu.make_async_copy(bbuf, b_ref, sems.at[5])
    out_b.start()
    out_a.wait()
    out_b.wait()


def pack(gate, up, down):
    anywhere = pl.BlockSpec(memory_space=pl.ANY)
    half = pltpu.HBM((3 * D // 2, 128), BF16)
    return pl.pallas_call(
        pack_kernel,
        in_specs=[anywhere] * 3,
        out_specs=(anywhere, anywhere),
        out_shape=(half, half),
        scratch_shapes=[
            pltpu.VMEM((3 * D // 2, 128), BF16),
            pltpu.VMEM((3 * D // 2, 128), BF16),
            pltpu.VMEM((128, D), BF16),
            pltpu.SemaphoreType.DMA((6,)),
        ],
        compiler_params=vmem(4),
        name="pack",
    )(*in_hbm(gate, up, down))


def dispatch_kernel(tp_ref, routes_ref, weight_ref, res_a, res_b, cot_a, cot_b, out_ref, pick_ref, scale_ref):
    @pl.when(pl.program_id(0) == 0)
    def _():
        r0, r1 = routes_ref[0:1, :], routes_ref[1:2, :]
        e = iota((N_EXP, TOK), 0)
        oh0, oh1 = e == r0, e == r1
        member = jnp.where(oh0 | oh1, 1.0, 0.0).astype(BF16)
        before = jnp.where(iota((TOK, TOK), 0) < iota((TOK, TOK), 1), 1.0, 0.0).astype(BF16)
        rank = dot(member, before)
        s0 = r0 * CAP + jnp.sum(jnp.where(oh0, rank, 0.0), axis=0, keepdims=True).astype(jnp.int32)
        s1 = r1 * CAP + jnp.sum(jnp.where(oh1, rank, 0.0), axis=0, keepdims=True).astype(jnp.int32)
        row = iota((8 * N_EXP, TOK), 0)
        q = row & 7
        for j in range(3):
            first = q < FIRST[j]
            i = 8 * j + q - jnp.where(first, 6 * j, 6 * (j + 1))
            slot = (row >> 3) * CAP + PART * tp_ref[0] + i
            m0, m1 = slot == s0, slot == s1
            hit = m0 | m1
            pick_ref[j, :, :TOK] = jnp.where(hit & first, 1.0, 0.0).astype(BF16)
            pick_ref[j, :, TOK:] = jnp.where(hit & ~first, 1.0, 0.0).astype(BF16)
            w = jnp.where(m0, weight_ref[0:1, :], 0.0) + jnp.where(m1, weight_ref[1:2, :], 0.0)
            w = jnp.sum(w, axis=1, keepdims=True)
            cot_row = (q[:, 0:1] < FIRST[j]) if j % 2 else (q[:, 0:1] >= FIRST[j])
            scale_ref[j] = jnp.broadcast_to(jnp.where(cot_row, w, 1.0), (8 * N_EXP, 128))

    classes = (res_a, cot_a, res_b, cot_b)
    for j in range(3):
        rhs = jnp.concatenate([classes[j][...], classes[j + 1][...]], axis=0)
        got = dot(pick_ref[j], rhs) * scale_ref[j][:, 0:1]
        out_ref[:, 8 * j : 8 * j + 8, :] = got.reshape(N_EXP, 8, got.shape[1]).astype(BF16)


def dispatch(tp, routes_t, weight_t, resid, cotangent):
    bn = 256
    half = D // 2 // bn
    return pl.pallas_call(
        dispatch_kernel,
        grid_spec=pltpu.PrefetchScalarGridSpec(
            num_scalar_prefetch=1,
            grid=(half,),
            in_specs=[
                pl.BlockSpec((2, TOK), lambda n, s: (0, 0)),
                pl.BlockSpec((2, TOK), lambda n, s: (0, 0)),
                pl.BlockSpec((TOK, bn), lambda n, s: (0, n)),
                pl.BlockSpec((TOK, bn), lambda n, s: (0, n + half)),
                pl.BlockSpec((TOK, bn), lambda n, s: (0, n)),
                pl.BlockSpec((TOK, bn), lambda n, s: (0, n + half)),
            ],
            out_specs=pl.BlockSpec((N_EXP, 24, bn), lambda n, s: (0, 0, n)),
            scratch_shapes=[
                pltpu.VMEM((3, 8 * N_EXP, 2 * TOK), BF16),
                pltpu.VMEM((3, 8 * N_EXP, 128), F32),
            ],
        ),
        out_shape=pltpu.HBM((N_EXP, 24, D // 2), BF16),
        compiler_params=vmem(14),
        name="dispatch",
    )(tp, routes_t, weight_t, resid, resid, cotangent, cotangent)


def place_kernel(routes_ref, out_ref):
    r0, r1 = routes_ref[:, 0:1], routes_ref[:, 1:2]
    e = iota((TOK, N_EXP), 1)
    oh0, oh1 = e == r0, e == r1
    member = jnp.where(oh0 | oh1, 1.0, 0.0).astype(BF16)
    before = jnp.where(iota((TOK, TOK), 1) < iota((TOK, TOK), 0), 1.0, 0.0).astype(BF16)
    rank = dot(before, member)

    def line(oh, r):
        k = jnp.sum(jnp.where(oh, rank, 0.0), axis=1, keepdims=True).astype(jnp.int32)
        t = (k * 43) >> 8
        return r * 64 + t * 8 + (k - t * PART)

    col = iota((TOK, 8 * N_TP * N_EXP), 1)
    hit = (col == line(oh0, r0)) | (col == line(oh1, r1))
    out_ref[...] = jnp.where(hit, 1.0, 0.0).astype(BF16)


def place(routes):
    return pl.pallas_call(
        place_kernel,
        out_shape=pltpu.HBM((TOK, 8 * N_TP * N_EXP), BF16),
        compiler_params=vmem(8),
        name="place",
    )(routes)


def select_kernel(got_ref, rows_ref):
    tiles = [
        got_ref[:, 8 * j : 8 * j + 8, :].astype(F32).reshape(8 * N_EXP, D // 2).astype(BF16) for j in range(3)
    ]
    k = iota((ROWS, 8 * N_EXP), 0)
    col = iota((ROWS, 8 * N_EXP), 1)
    source, q = col >> 3, col & 7
    for cls in range(4):
        total = None
        for j in (cls - 1, cls):
            if 0 <= j < 3:
                i = 8 * j + q - 6 * cls
                sel = jnp.where((k == source * PART + i) & (i >= 0) & (i < PART), 1.0, 0.0).astype(BF16)
                part = dot(sel, tiles[j])
                total = part if total is None else total + part
        rows_ref[cls % 2, :, (cls // 2) * (D // 2) : (cls // 2 + 1) * (D // 2)] = total.astype(BF16)


def select(got):
    return pl.pallas_call(
        select_kernel,
        out_shape=pltpu.HBM((2, ROWS, D), BF16),
        compiler_params=vmem(12),
        name="select",
    )(got)


def expert_kernel(rows_ref, *refs):
    weights, out_ref, acts_ref = refs[:16], refs[16], refs[17]
    gate_up, down, grads, sems = refs[18:]
    mid = D // 2
    copies = [[], [], [], []]
    for j in range(4):
        for side in range(2):
            part_a, part_b = weights[8 * side + 2 * j], weights[8 * side + 2 * j + 1]
            at = 128 * side
            g, u, d = pl.ds(512 * j + at, 128), pl.ds(512 * j + 256 + at, 128), pl.ds(256 * j + at, 128)
            moves = (
                (part_a.at[pl.ds(0, D)], gate_up.at[:, g]),
                (part_a.at[pl.ds(D, mid)], gate_up.at[pl.ds(0, mid), u]),
                (part_b.at[pl.ds(0, mid)], gate_up.at[pl.ds(mid, mid), u]),
                (part_b.at[pl.ds(mid, D)], down.at[:, d]),
            )
            for n, (src, dst) in enumerate(moves):
                copies[j].append(pltpu.make_async_copy(src, dst, sems.at[j, 4 * side + n]))
    for group in copies:
        for copy in group:
            copy.start()

    def chunk(j, _):
        for n in range(4):
            @pl.when(j == n)
            def _():
                for copy in copies[n]:
                    copy.wait()

        at = pl.multiple_of(512 * j, 512)
        both = dot(rows_ref[0], gate_up[:, pl.ds(at, 512)])
        gate, up = both[:, :256], both[:, 256:]
        d_hidden = dot(rows_ref[1], down[:, pl.ds(pl.multiple_of(256 * j, 256), 256)])
        sig = jax.nn.sigmoid(gate)
        silu = gate * sig
        d_gate = (d_hidden * up * (sig * (1.0 + gate * (1.0 - sig)))).astype(BF16)
        d_up = (d_hidden * silu).astype(BF16)
        acts_ref[j, 0] = d_gate
        acts_ref[j, 1] = d_up
        acts_ref[j, 2] = (silu * up).astype(BF16)
        grads[:, pl.ds(at, 256)] = d_gate
        grads[:, pl.ds(pl.multiple_of(at + 256, 256), 256)] = d_up
        return 0

    lax.fori_loop(0, 4, chunk, 0)
    line = iota((8 * N_EXP, ROWS), 0)
    spread = (iota((8 * N_EXP, ROWS), 1) == (line >> 3) * PART + (line & 7)) & ((line & 7) < PART)
    spread = jnp.where(spread, 1.0, 0.0).astype(BF16)

    def columns(t, _):
        rows = pl.ds(pl.multiple_of(256 * t, 256), 256)
        back = dot(spread, dot_nt(grads[...], gate_up[rows, :]).astype(BF16)).reshape(N_EXP, 8, 256)
        for h in range(2):
            out_ref[:, t, 8 * h : 8 * h + 8, :] = back[:, :, 128 * h : 128 * h + 128].astype(BF16)
        return 0

    lax.fori_loop(0, N_TP, columns, 0)


def experts(rows, weights):
    return pl.pallas_call(
        expert_kernel,
        in_specs=[pl.BlockSpec(memory_space=pltpu.VMEM)] + [pl.BlockSpec(memory_space=pl.ANY)] * 16,
        out_shape=(pltpu.HBM((N_EXP, N_TP, 16, 128), BF16), pltpu.HBM((4, 3, ROWS, 256), BF16)),
        scratch_shapes=[
            pltpu.VMEM((D, D), BF16),
            pltpu.VMEM((D, D // 2), BF16),
            pltpu.VMEM((ROWS, D), BF16),
            pltpu.SemaphoreType.DMA((4, 8)),
        ],
        compiler_params=vmem(32),
        name="experts",
    )(*in_hbm(rows, *weights))


def weight_grad_kernel(*refs):
    rows, far, acts = refs[0:3], refs[3:5], refs[5:9]
    keep_ref, send_ref, xbuf, hbuf, turned, sems = refs[9:]
    copies = []
    for n in range(4):
        at = pl.ds(ROWS * n, ROWS)
        if n < 3:
            copies.append(pltpu.make_async_copy(rows[n], xbuf.at[:, at, :], sems.at[3, n]))
        act = acts[n].at[0] if n == 0 else acts[n]
        for k in range(3):
            copies.append(pltpu.make_async_copy(act.at[k], hbuf.at[at, pl.ds(256 * k, 256)], sems.at[k, n]))
    for n in range(2):
        copies.append(pltpu.make_async_copy(far[n], xbuf.at[n, pl.ds(3 * ROWS, ROWS), :], sems.at[4, n]))
    for copy in copies:
        copy.start()
    for copy in copies:
        copy.wait()
    turned[...] = hbuf[:, 512:].T

    def columns(t, _):
        cols = pl.ds(pl.multiple_of(256 * t, 256), 256)
        both = dot_tn(xbuf[0, :, cols], hbuf[:, :512])
        for n in range(2):
            keep_ref[n, cols, :] = both[:, 256 * n : 256 * n + 128]
            send_ref[n, cols, :] = both[:, 256 * n + 128 : 256 * n + 256].astype(BF16)
        both = dot(turned[...], xbuf[1, :, cols])
        for h in range(2):
            at = pl.ds(pl.multiple_of(256 * t + 128 * h, 128), 128)
            keep_ref[2, at, :] = both[:128, 128 * h : 128 * h + 128]
            send_ref[2, at, :] = both[128:, 128 * h : 128 * h + 128].astype(BF16)
        return 0

    lax.fori_loop(0, N_TP, columns, 0)


def weight_grads(rows, far, acts):
    return pl.pallas_call(
        weight_grad_kernel,
        in_specs=[pl.BlockSpec(memory_space=pl.ANY)] * 9,
        out_shape=(pltpu.HBM((3, D, 128), F32), pltpu.HBM((3, D, 128), BF16)),
        scratch_shapes=[
            pltpu.VMEM((2, 4 * ROWS, D), BF16),
            pltpu.VMEM((4 * ROWS, 768), BF16),
            pltpu.VMEM((256, 4 * ROWS), BF16),
            pltpu.SemaphoreType.DMA((5, 4)),
        ],
        compiler_params=vmem(24),
        name="weight_grads",
    )(*in_hbm(*rows, *far, *acts))


def finish_kernel(keep_ref, got_ref, gate_ref, up_ref, down_ref):
    gate_ref[...] = keep_ref[0] + got_ref[0].astype(F32)
    up_ref[...] = keep_ref[1] + got_ref[1].astype(F32)
    for n in range(keep_ref.shape[1] // 128):
        at = slice(128 * n, 128 * n + 128)
        down_ref[:, at] = keep_ref[2, at, :] + got_ref[2, at, :].astype(F32)


def finish(keep, got):
    block = 512
    sums = pl.BlockSpec((3, block, 128), lambda t: (0, t, 0))
    tall = pl.BlockSpec((block, 128), lambda t: (t, 0))
    return pl.pallas_call(
        finish_kernel,
        grid=(D // block,),
        in_specs=[sums, sums],
        out_specs=(tall, tall, pl.BlockSpec((128, block), lambda t: (0, t))),
        out_shape=(
            jax.ShapeDtypeStruct((D, 128), F32),
            jax.ShapeDtypeStruct((D, 128), F32),
            jax.ShapeDtypeStruct((128, D), F32),
        ),
        compiler_params=vmem(8),
        name="finish",
    )(in_hbm(keep), got)


def combine_kernel(tp_ref, place_ref, back_ref, cot_ref, out_ref):
    halves = [
        back_ref[:, 8 * h : 8 * h + 8, :].astype(F32).reshape(8 * N_TP * N_EXP, 128).astype(BF16) for h in range(2)
    ]
    routed = dot(place_ref[...], jnp.concatenate(halves, axis=1))
    out_ref[...] = (cot_ref[...].astype(F32) + routed).T.astype(BF16)


def combine(tp, placed, back, cotangent):
    cols = D // N_TP
    return pl.pallas_call(
        combine_kernel,
        grid_spec=pltpu.PrefetchScalarGridSpec(
            num_scalar_prefetch=1,
            grid=(1,),
            in_specs=[
                pl.BlockSpec(placed.shape, lambda n, s: (0, 0)),
                pl.BlockSpec(back.shape, lambda n, s: (0, 0, 0)),
                pl.BlockSpec((TOK, cols), lambda n, s: (0, s[0])),
            ],
            out_specs=pl.BlockSpec((cols, TOK), lambda n, s: (0, 0)),
        ),
        out_shape=jax.ShapeDtypeStruct((cols, TOK), BF16),
        compiler_params=vmem(12),
        name="combine",
    )(tp, in_hbm(placed), back, cotangent)


def prepare_kernel(gate_ref, log_ref, before_ref, step_ref, mixed_ref, gelu_ref, slope_ref, prefix_ref, suffix_ref, turn_ref):
    lane = iota((STRIP, TOK), 1)
    turn_ref[...] = jnp.zeros_like(turn_ref)

    def strip(n, _):
        at = pl.ds(pl.multiple_of(n * STRIP, STRIP), STRIP)
        x = gate_ref[at, :].astype(F32)
        th = jnp.tanh(GELU_C * (x + GELU_A * (x * x * x)))
        gelu = 0.5 * x * (1.0 + th)
        back = 0.5 * (1.0 + th) + 0.5 * x * (1.0 - th * th) * (GELU_C * (1.0 + 3.0 * GELU_A * (x * x)))
        logs = log_ref[at, :]
        states = jnp.exp(logs) * before_ref[at, :] + step_ref[at, :].astype(F32)
        turn_ref[at, :] = gelu * states
        gelu_ref[at, :] = gelu
        slope_ref[at, :] = states * back
        total = logs
        d = 1
        while d < TOK:
            total = total + jnp.where(lane >= d, pltpu.roll(total, d, 1), 0.0)
            d *= 2
        prefix_ref[at, :] = jnp.exp(total)
        suffix_ref[at, :] = jnp.exp(total[:, TOK - 1 : TOK] - total)
        return 0

    lax.fori_loop(0, CH // STRIP, strip, 0)
    mixed_ref[...] = turn_ref[...].T[:, :CH].astype(BF16)


def prepare(gate_pre, log_decay, state_before, step_input):
    shape = gate_pre.shape
    wide = pltpu.HBM(shape, F32)
    return pl.pallas_call(
        prepare_kernel,
        out_shape=(pltpu.HBM(shape[::-1], BF16), wide, wide, wide, wide),
        scratch_shapes=[pltpu.VMEM((TOK, TOK), F32)],
        compiler_params=vmem(8),
        name="prepare",
    )(gate_pre, log_decay, state_before, step_input)


def project_kernel(order_ref, *refs):
    grads, (proj_ref, mixed_ref, gelu_ref, slope_ref, prefix_ref) = refs[:8], refs[8:13]
    pieces, (ggp_ref, direct_ref, link_ref, block_ref, turn_ref) = refs[13:17], refs[17:]
    d_mixed = jnp.zeros((CH, TOK), F32)
    for k in range(N_TP):
        group = order_ref[k]
        grad = grads[k][...]
        cols = pl.ds(pl.multiple_of(group * 256, 256), 256)
        d_mixed = d_mixed + dot(proj_ref[:, cols], grad)
        block_ref[...] = dot(grad, mixed_ref[...])
        for m in range(4):
            at = pl.ds(pl.multiple_of(((order_ref[8] + m) & 3) * 64, 64), 64)
            pieces[m][pl.ds(group, 1)] = block_ref[at, :].astype(BF16)[None]
    ggp_ref[...] = (d_mixed * slope_ref[...]).astype(BF16)
    direct = d_mixed * gelu_ref[...]
    direct_ref[...] = direct
    turn_ref[...] = jnp.zeros_like(turn_ref)
    turn_ref[0:CH, 0:1] = prefix_ref[:, TOK - 1 : TOK]
    turn_ref[0:CH, 1:2] = jnp.sum(prefix_ref[...] * direct, axis=1, keepdims=True)
    link_ref[...] = turn_ref[...].T[0:2, 0:CH]


def project(order, grads, out_proj, mixed, gelu, slope, prefix):
    piece = pltpu.HBM((8, 64, CH), BF16)
    return pl.pallas_call(
        project_kernel,
        in_specs=[pl.BlockSpec(memory_space=pltpu.SMEM)] + [pl.BlockSpec(memory_space=pltpu.VMEM)] * 13,
        out_shape=(
            piece, piece, piece, piece,
            pltpu.HBM((CH, TOK), BF16),
            pltpu.HBM((CH, TOK), F32),
            pltpu.HBM((2, CH), F32),
        ),
        scratch_shapes=[pltpu.VMEM((256, CH), F32), pltpu.VMEM((TOK, 128), F32)],
        compiler_params=vmem(14),
        name="project",
    )(order, *grads, out_proj, mixed, gelu, slope, prefix)


def local_kernel(direct_ref, log_ref, out_ref):
    lane = iota((STRIP, TOK), 1)

    def strip(n, _):
        at = pl.ds(pl.multiple_of(n * STRIP, STRIP), STRIP)
        a = jnp.where(lane < TOK - 1, pltpu.roll(jnp.exp(log_ref[at, :]), TOK - 1, 1), 1.0)
        b = direct_ref[at, :]
        d = 1
        while d < TOK:
            b = b + a * jnp.where(lane < TOK - d, pltpu.roll(b, TOK - d, 1), 0.0)
            if 2 * d < TOK:
                a = a * jnp.where(lane < TOK - d, pltpu.roll(a, TOK - d, 1), 1.0)
            d *= 2
        out_ref[at, :] = b
        return 0

    lax.fori_loop(0, CH // STRIP, strip, 0)


def local_scan(direct, log_decay):
    return pl.pallas_call(
        local_kernel,
        out_shape=jax.ShapeDtypeStruct((CH, TOK), F32),
        compiler_params=vmem(6),
        name="local_scan",
    )(in_hbm(direct), log_decay)


def recur_kernel(at_ref, links_ref, local_ref, suffix_ref, log_ref, before_ref, step_ref, decay_ref, turn_ref):
    mine = at_ref[0]
    arriving = jnp.zeros((1, CH), F32)
    for s in range(N_EXP - 1, 0, -1):
        arriving = jnp.where(s > mine, links_ref[s, 1:2, :] + links_ref[s, 0:1, :] * arriving, arriving)
    turn_ref[...] = jnp.zeros_like(turn_ref)
    turn_ref[0:1, 0:CH] = arriving
    column = turn_ref[...].T[:CH, 0:1]
    g = local_ref[...] + suffix_ref[...] * column
    step_ref[...] = g
    decay_ref[...] = g * jnp.exp(log_ref[...]) * before_ref[...]


def recur(at, links, local, suffix, log_decay, state_before):
    return pl.pallas_call(
        recur_kernel,
        in_specs=[pl.BlockSpec(memory_space=pltpu.SMEM)] + [pl.BlockSpec(memory_space=pltpu.VMEM)] * 5,
        out_shape=(
            jax.ShapeDtypeStruct((CH, TOK), F32),
            jax.ShapeDtypeStruct((CH, TOK), F32),
        ),
        scratch_shapes=[pltpu.VMEM((128, TOK), F32)],
        compiler_params=vmem(8),
        name="recur",
    )(at, links, local, in_hbm(suffix), log_decay, state_before)


def shifted(value, axis, by):
    n = lax.axis_size(axis)
    return lax.ppermute(value, axis, [(i, (i + by) % n) for i in range(n)])


def on_device(resid, cotangent, routes, route_weight, w_gate, w_up, w_down, out_proj, gate_pre, log_decay,
              state_before, step_input):
    y, c = lax.axis_index("y"), lax.axis_index("c")
    tp = (2 * y + c).astype(jnp.int32)
    tp_vec = tp[None]

    own_a, own_b = pack(w_gate[0], w_up[0], w_down[0])
    prev_a = shifted(own_a, "y", 1)
    next_b = shifted(own_b, "y", -1)
    prev_b = shifted(own_b, "y", 1)
    next_a = shifted(own_a, "y", -1)
    far_a = shifted(prev_a, "y", 1)
    far_b = shifted(next_b, "y", -1)
    mine = (own_a, own_b, prev_a, prev_b, next_a, next_b, far_a, far_b)
    weights = mine + tuple(shifted(w, "c", 1) for w in mine)

    sent = dispatch(tp_vec, routes.T, route_weight.T, resid, cotangent)
    got = lax.all_to_all(sent, SP, split_axis=0, concat_axis=0, tiled=True)

    placed = place(routes)
    log_t, before_t = log_decay.T, state_before.T
    mixed, gelu, slope, prefix, suffix = prepare(gate_pre.T, log_t, before_t, step_input.T)
    ys = jnp.stack([y, y - 1, y + 1, y + 2]) % 4
    order = jnp.concatenate([2 * ys + c, 2 * ys + 1 - c, lax.axis_index("x")[None]]).astype(jnp.int32)
    got, order = lax.optimization_barrier((got, order))

    rows = select(got)
    rows_after = shifted(rows, "y", -1)
    rows_before = shifted(rows, "y", 1)
    back, acts = experts(rows, weights)
    back = lax.all_to_all(back.reshape(N_EXP * N_TP, 16, 128), ALL, split_axis=0, concat_axis=0, tiled=True)
    all_acts = [acts]
    for j, by in ((1, -1), (2, 1), (3, 2)):
        all_acts.append(shifted(acts[j], "y", by))
    far_in, far_cot, back = lax.optimization_barrier((rows_before[0], rows_after[1], back))
    part = combine(tp_vec, placed, back, cotangent)

    near = (part, shifted(part, "y", 1), shifted(part, "y", -1), shifted(part, "y", 2))
    grads = (*near, *(shifted(g, "c", 1) for g in near))
    *pieces, grad_gate_pre, direct, link = project(order, grads, out_proj.T, mixed, gelu, slope, prefix)

    far_in, far_cot, pieces[0] = lax.optimization_barrier((far_in, far_cot, pieces[0]))

    over_x = [pieces[0]]
    for m in (1, 2, 3):
        over_x.append(shifted(pieces[m], "x", m))
    link = jnp.broadcast_to(link, (N_EXP, *link.shape))
    links = lax.all_to_all(link, SP, split_axis=0, concat_axis=0, tiled=True)
    over_x = sum(p.astype(F32) for p in over_x).astype(BF16)
    over_z = lax.all_to_all(over_x, "z", split_axis=0, concat_axis=0, tiled=True)
    grad_proj = over_z.astype(F32).sum(axis=0)

    sp = (4 * lax.axis_index("z") + lax.axis_index("x")).astype(jnp.int32)
    local = local_scan(direct, log_t)
    grad_step_input, grad_log_decay = recur(sp[None], links, local, suffix, log_t, before_t)

    far_in = shifted(far_in, "y", 1)
    far_cot = shifted(far_cot, "y", -1)
    far = (far_in, far_cot)
    keep, send = weight_grads((rows, rows_after, rows_before), far, all_acts)
    send = shifted(send, "c", 1)
    grad_gate, grad_up, grad_down = finish(keep, send)
    return (
        grad_gate[None],
        grad_up[None],
        grad_down[None],
        grad_proj,
        grad_gate_pre.T,
        grad_step_input.T,
        grad_log_decay.T,
    )


def solution(mesh):
    grid = Mesh(mesh.devices.reshape(8, 4, 4, 2), ALL)


    return jax.shard_map(
        on_device,
        mesh=grid,
        in_specs=(
            P(SP, None),
            P(SP, None),
            P(SP, None),
            P(SP, None),
            P(SP, None, TP),
            P(SP, None, TP),
            P(SP, TP, None),
            P(None, TP),
            P(SP, TP),
            P(SP, TP),
            P(SP, TP),
            P(SP, TP),
        ),
        out_specs=(
            P(SP, None, TP),
            P(SP, None, TP),
            P(SP, TP, None),
            P(SP, TP),
            P(SP, TP),
            P(SP, TP),
            P(SP, TP),
        ),
        check_vma=False,
    )
```

```python
import jax
import jax.numpy as jnp
from jax import lax
from jax.experimental import pallas as pl
from jax.experimental.pallas import tpu as pltpu
from jax.sharding import Mesh, PartitionSpec as P


BF16 = jnp.bfloat16
F32 = jnp.float32
SP = ("z", "x")
TP = ("y", "c")
ALL = ("z", "x", "y", "c")

TOK = 384
D = 2048
CAP = 48
N_EXP = 32
N_TP = 8
PART = CAP // N_TP
ROWS = N_EXP * PART
CH = 352
STRIP = 32
GELU_C = 0.7978845608028654
GELU_A = 0.044715


def iota(shape, dim):
    return lax.broadcasted_iota(jnp.int32, shape, dim)


def in_hbm(*arrays):
    held = tuple(pltpu.with_memory_space_constraint(a, pltpu.HBM) for a in arrays)
    return held if len(held) > 1 else held[0]


def vmem(mib):
    return pltpu.CompilerParams(vmem_limit_bytes=mib * 1024 * 1024)


def dot(a, b):
    return jnp.dot(a, b, preferred_element_type=F32)


def dot_nt(a, b):
    return lax.dot_general(a, b, (((1,), (1,)), ((), ())), preferred_element_type=F32)


def dot_tn(a, b):
    return lax.dot_general(a, b, (((0,), (0,)), ((), ())), preferred_element_type=F32)


FIRST = (6, 4, 2)


def pack_kernel(gate_ref, up_ref, down_ref, a_ref, b_ref, abuf, bbuf, down_buf, sems):
    third = D // 2
    loads = [
        pltpu.make_async_copy(down_ref, down_buf, sems.at[0]),
        pltpu.make_async_copy(gate_ref, abuf.at[pl.ds(0, D)], sems.at[1]),
        pltpu.make_async_copy(up_ref.at[pl.ds(0, third)], abuf.at[pl.ds(D, third)], sems.at[2]),
        pltpu.make_async_copy(up_ref.at[pl.ds(third, third)], bbuf.at[pl.ds(0, third)], sems.at[3]),
    ]
    for load in loads:
        load.start()
    loads[1].wait()
    loads[2].wait()
    out_a = pltpu.make_async_copy(abuf, a_ref, sems.at[4])
    out_a.start()
    loads[0].wait()
    bbuf[third:, :] = down_buf[...].T
    loads[3].wait()
    out_b = pltpu.make_async_copy(bbuf, b_ref, sems.at[5])
    out_b.start()
    out_a.wait()
    out_b.wait()


def pack(gate, up, down):
    anywhere = pl.BlockSpec(memory_space=pl.ANY)
    half = pltpu.HBM((3 * D // 2, 128), BF16)
    return pl.pallas_call(
        pack_kernel,
        in_specs=[anywhere] * 3,
        out_specs=(anywhere, anywhere),
        out_shape=(half, half),
        scratch_shapes=[
            pltpu.VMEM((3 * D // 2, 128), BF16),
            pltpu.VMEM((3 * D // 2, 128), BF16),
            pltpu.VMEM((128, D), BF16),
            pltpu.SemaphoreType.DMA((6,)),
        ],
        compiler_params=vmem(4),
        name="pack",
    )(*in_hbm(gate, up, down))


def dispatch_kernel(tp_ref, routes_ref, weight_ref, res_a, res_b, cot_a, cot_b, out_ref, pick_ref, scale_ref):
    @pl.when(pl.program_id(0) == 0)
    def _():
        r0, r1 = routes_ref[0:1, :], routes_ref[1:2, :]
        e = iota((N_EXP, TOK), 0)
        oh0, oh1 = e == r0, e == r1
        member = jnp.where(oh0 | oh1, 1.0, 0.0).astype(BF16)
        before = jnp.where(iota((TOK, TOK), 0) < iota((TOK, TOK), 1), 1.0, 0.0).astype(BF16)
        rank = dot(member, before)
        s0 = r0 * CAP + jnp.sum(jnp.where(oh0, rank, 0.0), axis=0, keepdims=True).astype(jnp.int32)
        s1 = r1 * CAP + jnp.sum(jnp.where(oh1, rank, 0.0), axis=0, keepdims=True).astype(jnp.int32)
        row = iota((8 * N_EXP, TOK), 0)
        q = row & 7
        for j in range(3):
            first = q < FIRST[j]
            i = 8 * j + q - jnp.where(first, 6 * j, 6 * (j + 1))
            slot = (row >> 3) * CAP + PART * tp_ref[0] + i
            m0, m1 = slot == s0, slot == s1
            hit = m0 | m1
            pick_ref[j, :, :TOK] = jnp.where(hit & first, 1.0, 0.0).astype(BF16)
            pick_ref[j, :, TOK:] = jnp.where(hit & ~first, 1.0, 0.0).astype(BF16)
            w = jnp.where(m0, weight_ref[0:1, :], 0.0) + jnp.where(m1, weight_ref[1:2, :], 0.0)
            w = jnp.sum(w, axis=1, keepdims=True)
            cot_row = (q[:, 0:1] < FIRST[j]) if j % 2 else (q[:, 0:1] >= FIRST[j])
            scale_ref[j] = jnp.broadcast_to(jnp.where(cot_row, w, 1.0), (8 * N_EXP, 128))

    classes = (res_a, cot_a, res_b, cot_b)
    for j in range(3):
        rhs = jnp.concatenate([classes[j][...], classes[j + 1][...]], axis=0)
        got = dot(pick_ref[j], rhs) * scale_ref[j][:, 0:1]
        out_ref[:, 8 * j : 8 * j + 8, :] = got.reshape(N_EXP, 8, got.shape[1]).astype(BF16)


def dispatch(tp, routes_t, weight_t, resid, cotangent):
    bn = 256
    half = D // 2 // bn
    return pl.pallas_call(
        dispatch_kernel,
        grid_spec=pltpu.PrefetchScalarGridSpec(
            num_scalar_prefetch=1,
            grid=(half,),
            in_specs=[
                pl.BlockSpec((2, TOK), lambda n, s: (0, 0)),
                pl.BlockSpec((2, TOK), lambda n, s: (0, 0)),
                pl.BlockSpec((TOK, bn), lambda n, s: (0, n)),
                pl.BlockSpec((TOK, bn), lambda n, s: (0, n + half)),
                pl.BlockSpec((TOK, bn), lambda n, s: (0, n)),
                pl.BlockSpec((TOK, bn), lambda n, s: (0, n + half)),
            ],
            out_specs=pl.BlockSpec((N_EXP, 24, bn), lambda n, s: (0, 0, n)),
            scratch_shapes=[
                pltpu.VMEM((3, 8 * N_EXP, 2 * TOK), BF16),
                pltpu.VMEM((3, 8 * N_EXP, 128), F32),
            ],
        ),
        out_shape=pltpu.HBM((N_EXP, 24, D // 2), BF16),
        compiler_params=vmem(14),
        name="dispatch",
    )(tp, routes_t, weight_t, resid, resid, cotangent, cotangent)


def place_kernel(routes_ref, out_ref):
    r0, r1 = routes_ref[:, 0:1], routes_ref[:, 1:2]
    e = iota((TOK, N_EXP), 1)
    oh0, oh1 = e == r0, e == r1
    member = jnp.where(oh0 | oh1, 1.0, 0.0).astype(BF16)
    before = jnp.where(iota((TOK, TOK), 1) < iota((TOK, TOK), 0), 1.0, 0.0).astype(BF16)
    rank = dot(before, member)

    def line(oh, r):
        k = jnp.sum(jnp.where(oh, rank, 0.0), axis=1, keepdims=True).astype(jnp.int32)
        t = (k * 43) >> 8
        return r * 64 + t * 8 + (k - t * PART)

    col = iota((TOK, 8 * N_TP * N_EXP), 1)
    hit = (col == line(oh0, r0)) | (col == line(oh1, r1))
    out_ref[...] = jnp.where(hit, 1.0, 0.0).astype(BF16)


def place(routes):
    return pl.pallas_call(
        place_kernel,
        out_shape=pltpu.HBM((TOK, 8 * N_TP * N_EXP), BF16),
        compiler_params=vmem(8),
        name="place",
    )(routes)


def select_kernel(got_ref, rows_ref):
    tiles = [
        got_ref[:, 8 * j : 8 * j + 8, :].astype(F32).reshape(8 * N_EXP, D // 2).astype(BF16) for j in range(3)
    ]
    k = iota((ROWS, 8 * N_EXP), 0)
    col = iota((ROWS, 8 * N_EXP), 1)
    source, q = col >> 3, col & 7
    for cls in range(4):
        total = None
        for j in (cls - 1, cls):
            if 0 <= j < 3:
                i = 8 * j + q - 6 * cls
                sel = jnp.where((k == source * PART + i) & (i >= 0) & (i < PART), 1.0, 0.0).astype(BF16)
                part = dot(sel, tiles[j])
                total = part if total is None else total + part
        rows_ref[cls % 2, :, (cls // 2) * (D // 2) : (cls // 2 + 1) * (D // 2)] = total.astype(BF16)


def select(got):
    return pl.pallas_call(
        select_kernel,
        out_shape=pltpu.HBM((2, ROWS, D), BF16),
        compiler_params=vmem(12),
        name="select",
    )(got)


def expert_kernel(rows_hbm, *refs):
    weights, out_ref, acts = refs[:16], refs[16], refs[17:21]
    rows_ref, gate_up, down, grads, made, sems, row_sems, act_sems = refs[21:]
    mid = D // 2
    copies = [[], [], [], []]
    for j in range(4):
        for side in range(2):
            part_a, part_b = weights[8 * side + 2 * j], weights[8 * side + 2 * j + 1]
            at = 128 * side
            g, u, d = pl.ds(512 * j + at, 128), pl.ds(512 * j + 256 + at, 128), pl.ds(256 * j + at, 128)
            moves = (
                (part_a.at[pl.ds(0, D)], gate_up.at[:, g]),
                (part_a.at[pl.ds(D, mid)], gate_up.at[pl.ds(0, mid), u]),
                (part_b.at[pl.ds(0, mid)], gate_up.at[pl.ds(mid, mid), u]),
                (part_b.at[pl.ds(mid, D)], down.at[:, d]),
            )
            for n, (src, dst) in enumerate(moves):
                copies[j].append(pltpu.make_async_copy(src, dst, sems.at[j, 4 * side + n]))
    rows_in = [pltpu.make_async_copy(rows_hbm.at[n], rows_ref.at[n], row_sems.at[n]) for n in range(2)]
    acts_out = [pltpu.make_async_copy(made.at[n], acts[n], act_sems.at[n]) for n in range(4)]
    for copy in [rows_in[0], *copies[0], rows_in[1]]:
        copy.start()
    for copy in rows_in:
        copy.wait()

    def chunk(j, _):
        for n in range(4):
            @pl.when(j == n)
            def _():
                for copy in copies[n]:
                    copy.wait()
                if n < 3:
                    for copy in copies[n + 1]:
                        copy.start()

        at = pl.multiple_of(512 * j, 512)
        both = dot(rows_ref[0], gate_up[:, pl.ds(at, 512)])
        gate, up = both[:, :256], both[:, 256:]
        d_hidden = dot(rows_ref[1], down[:, pl.ds(pl.multiple_of(256 * j, 256), 256)])
        sig = jax.nn.sigmoid(gate)
        silu = gate * sig
        d_gate = (d_hidden * up * (sig * (1.0 + gate * (1.0 - sig)))).astype(BF16)
        d_up = (d_hidden * silu).astype(BF16)
        made[j, 0] = d_gate
        made[j, 1] = d_up
        made[j, 2] = (silu * up).astype(BF16)
        grads[:, pl.ds(at, 256)] = d_gate
        grads[:, pl.ds(pl.multiple_of(at + 256, 256), 256)] = d_up
        return 0

    lax.fori_loop(0, 4, chunk, 0)
    for copy in acts_out:
        copy.start()
    line = iota((8 * N_EXP, ROWS), 0)
    spread = (iota((8 * N_EXP, ROWS), 1) == (line >> 3) * PART + (line & 7)) & ((line & 7) < PART)
    spread = jnp.where(spread, 1.0, 0.0).astype(BF16)

    def columns(t, _):
        rows = pl.ds(pl.multiple_of(256 * t, 256), 256)
        back = dot(spread, dot_nt(grads[...], gate_up[rows, :]).astype(BF16)).reshape(N_EXP, 8, 256)
        for h in range(2):
            out_ref[:, t, 8 * h : 8 * h + 8, :] = back[:, :, 128 * h : 128 * h + 128].astype(BF16)
        return 0

    lax.fori_loop(0, N_TP, columns, 0)
    for copy in acts_out:
        copy.wait()


def experts(rows, weights):
    act = pltpu.HBM((3, ROWS, 256), BF16)
    anywhere = pl.BlockSpec(memory_space=pl.ANY)
    return pl.pallas_call(
        expert_kernel,
        in_specs=[anywhere] * 17,
        out_specs=(pl.BlockSpec(memory_space=pltpu.VMEM), anywhere, anywhere, anywhere, anywhere),
        out_shape=(pltpu.HBM((N_EXP, N_TP, 16, 128), BF16), act, act, act, act),
        scratch_shapes=[
            pltpu.VMEM((2, ROWS, D), BF16),
            pltpu.VMEM((D, D), BF16),
            pltpu.VMEM((D, D // 2), BF16),
            pltpu.VMEM((ROWS, D), BF16),
            pltpu.VMEM((4, 3, ROWS, 256), BF16),
            pltpu.SemaphoreType.DMA((4, 8)),
            pltpu.SemaphoreType.DMA((2,)),
            pltpu.SemaphoreType.DMA((4,)),
        ],
        compiler_params=vmem(32),
        name="experts",
    )(*in_hbm(rows, *weights))


def weight_grad_kernel(rows_0, rows_1, rows_2, far_in, far_cot, act_0, act_1, act_2, act_3,
                       keep_ref, send_ref, hbuf, turned):
    @pl.when(pl.program_id(0) == 0)
    def _():
        for n, act in enumerate((act_0, act_1, act_2, act_3)):
            for k in range(3):
                hbuf[ROWS * n : ROWS * (n + 1), 256 * k : 256 * (k + 1)] = act[k]
        turned[...] = hbuf[:, 512:].T

    near = (rows_0, rows_1, rows_2)
    both = dot_tn(jnp.concatenate([*(r[0] for r in near), far_in[...]], axis=0), hbuf[:, :512])
    for n in range(2):
        keep_ref[n] = both[:, 256 * n : 256 * n + 128]
        send_ref[n] = both[:, 256 * n + 128 : 256 * n + 256].astype(BF16)
    both = dot(turned[...], jnp.concatenate([*(r[1] for r in near), far_cot[...]], axis=0))
    for h in range(both.shape[1] // 128):
        at = slice(128 * h, 128 * h + 128)
        keep_ref[2, at, :] = both[:128, at]
        send_ref[2, at, :] = both[128:, at].astype(BF16)


def weight_grads(rows, far, acts):
    block = 256
    sums = pl.BlockSpec((3, block, 128), lambda t: (0, t, 0))
    return pl.pallas_call(
        weight_grad_kernel,
        grid=(D // block,),
        in_specs=[pl.BlockSpec((2, ROWS, block), lambda t: (0, 0, t))] * 3
        + [pl.BlockSpec((ROWS, block), lambda t: (0, t))] * 2
        + [pl.BlockSpec((3, ROWS, 256), lambda t: (0, 0, 0))] * 4,
        out_specs=(sums, sums),
        out_shape=(pltpu.HBM((3, D, 128), F32), pltpu.HBM((3, D, 128), BF16)),
        scratch_shapes=[
            pltpu.VMEM((4 * ROWS, 768), BF16),
            pltpu.VMEM((256, 4 * ROWS), BF16),
        ],
        compiler_params=vmem(12),
        name="weight_grads",
    )(*rows, *far, *acts)


def finish_kernel(keep_ref, got_ref, gate_ref, up_ref, down_ref):
    gate_ref[...] = keep_ref[0] + got_ref[0].astype(F32)
    up_ref[...] = keep_ref[1] + got_ref[1].astype(F32)
    for n in range(keep_ref.shape[1] // 128):
        at = slice(128 * n, 128 * n + 128)
        down_ref[:, at] = keep_ref[2, at, :] + got_ref[2, at, :].astype(F32)


def finish(keep, got):
    block = 512
    sums = pl.BlockSpec((3, block, 128), lambda t: (0, t, 0))
    tall = pl.BlockSpec((block, 128), lambda t: (t, 0))
    return pl.pallas_call(
        finish_kernel,
        grid=(D // block,),
        in_specs=[sums, sums],
        out_specs=(tall, tall, pl.BlockSpec((128, block), lambda t: (0, t))),
        out_shape=(
            jax.ShapeDtypeStruct((D, 128), F32),
            jax.ShapeDtypeStruct((D, 128), F32),
            jax.ShapeDtypeStruct((128, D), F32),
        ),
        compiler_params=vmem(8),
        name="finish",
    )(in_hbm(keep), got)


def combine_kernel(tp_ref, place_ref, back_ref, cot_ref, out_ref):
    halves = [
        back_ref[:, 8 * h : 8 * h + 8, :].astype(F32).reshape(8 * N_TP * N_EXP, 128).astype(BF16) for h in range(2)
    ]
    routed = dot(place_ref[...], jnp.concatenate(halves, axis=1))
    out_ref[...] = (cot_ref[...].astype(F32) + routed).T.astype(BF16)


def combine(tp, placed, back, cotangent):
    cols = D // N_TP
    return pl.pallas_call(
        combine_kernel,
        grid_spec=pltpu.PrefetchScalarGridSpec(
            num_scalar_prefetch=1,
            grid=(1,),
            in_specs=[
                pl.BlockSpec(placed.shape, lambda n, s: (0, 0)),
                pl.BlockSpec(back.shape, lambda n, s: (0, 0, 0)),
                pl.BlockSpec((TOK, cols), lambda n, s: (0, s[0])),
            ],
            out_specs=pl.BlockSpec((cols, TOK), lambda n, s: (0, 0)),
        ),
        out_shape=jax.ShapeDtypeStruct((cols, TOK), BF16),
        compiler_params=vmem(12),
        name="combine",
    )(tp, in_hbm(placed), back, cotangent)


def prepare_kernel(gate_ref, log_ref, before_ref, step_ref, mixed_ref, gelu_ref, slope_ref, prefix_ref, suffix_ref, turn_ref):
    lane = iota((STRIP, TOK), 1)
    turn_ref[...] = jnp.zeros_like(turn_ref)

    def strip(n, _):
        at = pl.ds(pl.multiple_of(n * STRIP, STRIP), STRIP)
        x = gate_ref[at, :].astype(F32)
        th = jnp.tanh(GELU_C * (x + GELU_A * (x * x * x)))
        gelu = 0.5 * x * (1.0 + th)
        back = 0.5 * (1.0 + th) + 0.5 * x * (1.0 - th * th) * (GELU_C * (1.0 + 3.0 * GELU_A * (x * x)))
        logs = log_ref[at, :]
        states = jnp.exp(logs) * before_ref[at, :] + step_ref[at, :].astype(F32)
        turn_ref[at, :] = gelu * states
        gelu_ref[at, :] = gelu
        slope_ref[at, :] = states * back
        total = logs
        d = 1
        while d < TOK:
            total = total + jnp.where(lane >= d, pltpu.roll(total, d, 1), 0.0)
            d *= 2
        prefix_ref[at, :] = jnp.exp(total)
        suffix_ref[at, :] = jnp.exp(total[:, TOK - 1 : TOK] - total)
        return 0

    lax.fori_loop(0, CH // STRIP, strip, 0)
    mixed_ref[...] = turn_ref[...].T[:, :CH].astype(BF16)


def prepare(gate_pre, log_decay, state_before, step_input):
    shape = gate_pre.shape
    wide = pltpu.HBM(shape, F32)
    return pl.pallas_call(
        prepare_kernel,
        out_shape=(pltpu.HBM(shape[::-1], BF16), wide, wide, wide, wide),
        scratch_shapes=[pltpu.VMEM((TOK, TOK), F32)],
        compiler_params=vmem(8),
        name="prepare",
    )(gate_pre, log_decay, state_before, step_input)


def project_kernel(order_ref, *refs):
    grads, (proj_ref, mixed_ref, gelu_ref, slope_ref, prefix_ref) = refs[:8], refs[8:13]
    pieces, (ggp_ref, direct_ref, link_ref, block_ref, turn_ref) = refs[13:17], refs[17:]
    d_mixed = jnp.zeros((CH, TOK), F32)
    for k in range(N_TP):
        group = order_ref[k]
        grad = grads[k][...]
        cols = pl.ds(pl.multiple_of(group * 256, 256), 256)
        d_mixed = d_mixed + dot(proj_ref[:, cols], grad)
        block_ref[...] = dot(grad, mixed_ref[...])
        for m in range(4):
            at = pl.ds(pl.multiple_of(((order_ref[8] + m) & 3) * 64, 64), 64)
            pieces[m][pl.ds(group, 1)] = block_ref[at, :].astype(BF16)[None]
    ggp_ref[...] = (d_mixed * slope_ref[...]).astype(BF16)
    direct = d_mixed * gelu_ref[...]
    direct_ref[...] = direct
    turn_ref[...] = jnp.zeros_like(turn_ref)
    turn_ref[0:CH, 0:1] = prefix_ref[:, TOK - 1 : TOK]
    turn_ref[0:CH, 1:2] = jnp.sum(prefix_ref[...] * direct, axis=1, keepdims=True)
    link_ref[...] = turn_ref[...].T[0:2, 0:CH]


def project(order, grads, out_proj, mixed, gelu, slope, prefix):
    piece = pltpu.HBM((8, 64, CH), BF16)
    return pl.pallas_call(
        project_kernel,
        in_specs=[pl.BlockSpec(memory_space=pltpu.SMEM)] + [pl.BlockSpec(memory_space=pltpu.VMEM)] * 13,
        out_shape=(
            piece, piece, piece, piece,
            pltpu.HBM((CH, TOK), BF16),
            pltpu.HBM((CH, TOK), F32),
            pltpu.HBM((2, CH), F32),
        ),
        scratch_shapes=[pltpu.VMEM((256, CH), F32), pltpu.VMEM((TOK, 128), F32)],
        compiler_params=vmem(14),
        name="project",
    )(order, *grads, out_proj, mixed, gelu, slope, prefix)


def local_kernel(direct_ref, log_ref, out_ref):
    lane = iota((STRIP, TOK), 1)

    def strip(n, _):
        at = pl.ds(pl.multiple_of(n * STRIP, STRIP), STRIP)
        a = jnp.where(lane < TOK - 1, pltpu.roll(jnp.exp(log_ref[at, :]), TOK - 1, 1), 1.0)
        b = direct_ref[at, :]
        d = 1
        while d < TOK:
            b = b + a * jnp.where(lane < TOK - d, pltpu.roll(b, TOK - d, 1), 0.0)
            if 2 * d < TOK:
                a = a * jnp.where(lane < TOK - d, pltpu.roll(a, TOK - d, 1), 1.0)
            d *= 2
        out_ref[at, :] = b
        return 0

    lax.fori_loop(0, CH // STRIP, strip, 0)


def local_scan(direct, log_decay):
    return pl.pallas_call(
        local_kernel,
        out_shape=jax.ShapeDtypeStruct((CH, TOK), F32),
        compiler_params=vmem(6),
        name="local_scan",
    )(in_hbm(direct), log_decay)


def recur_kernel(at_ref, links_ref, local_ref, suffix_ref, log_ref, before_ref, step_ref, decay_ref, turn_ref):
    mine = at_ref[0]
    arriving = jnp.zeros((1, CH), F32)
    for s in range(N_EXP - 1, 0, -1):
        arriving = jnp.where(s > mine, links_ref[s, 1:2, :] + links_ref[s, 0:1, :] * arriving, arriving)
    turn_ref[...] = jnp.zeros_like(turn_ref)
    turn_ref[0:1, 0:CH] = arriving
    column = turn_ref[...].T[:CH, 0:1]
    g = local_ref[...] + suffix_ref[...] * column
    step_ref[...] = g
    decay_ref[...] = g * jnp.exp(log_ref[...]) * before_ref[...]


def recur(at, links, local, suffix, log_decay, state_before):
    return pl.pallas_call(
        recur_kernel,
        in_specs=[pl.BlockSpec(memory_space=pltpu.SMEM)] + [pl.BlockSpec(memory_space=pltpu.VMEM)] * 5,
        out_shape=(
            jax.ShapeDtypeStruct((CH, TOK), F32),
            jax.ShapeDtypeStruct((CH, TOK), F32),
        ),
        scratch_shapes=[pltpu.VMEM((128, TOK), F32)],
        compiler_params=vmem(8),
        name="recur",
    )(at, links, local, in_hbm(suffix), log_decay, state_before)


def shifted(value, axis, by):
    n = lax.axis_size(axis)
    return lax.ppermute(value, axis, [(i, (i + by) % n) for i in range(n)])


def on_device(resid, cotangent, routes, route_weight, w_gate, w_up, w_down, out_proj, gate_pre, log_decay,
              state_before, step_input):
    y, c = lax.axis_index("y"), lax.axis_index("c")
    tp = (2 * y + c).astype(jnp.int32)
    tp_vec = tp[None]

    own_a, own_b = pack(w_gate[0], w_up[0], w_down[0])
    prev_a = shifted(own_a, "y", 1)
    next_b = shifted(own_b, "y", -1)
    prev_b = shifted(own_b, "y", 1)
    next_a = shifted(own_a, "y", -1)
    far_a = shifted(prev_a, "y", 1)
    far_b = shifted(next_b, "y", -1)
    mine = (own_a, own_b, prev_a, prev_b, next_a, next_b, far_a, far_b)
    weights = mine + tuple(shifted(w, "c", 1) for w in mine)

    sent = dispatch(tp_vec, routes.T, route_weight.T, resid, cotangent)
    got = lax.all_to_all(sent, SP, split_axis=0, concat_axis=0, tiled=True)

    placed = place(routes)
    log_t, before_t = log_decay.T, state_before.T
    mixed, gelu, slope, prefix, suffix = prepare(gate_pre.T, log_t, before_t, step_input.T)
    ys = jnp.stack([y, y - 1, y + 1, y + 2]) % 4
    order = jnp.concatenate([2 * ys + c, 2 * ys + 1 - c, lax.axis_index("x")[None]]).astype(jnp.int32)
    got, order = lax.optimization_barrier((got, order))

    rows = select(got)
    rows_after = shifted(rows, "y", -1)
    rows_before = shifted(rows, "y", 1)
    back, *acts = experts(rows, weights)
    back = lax.all_to_all(back.reshape(N_EXP * N_TP, 16, 128), ALL, split_axis=0, concat_axis=0, tiled=True)
    all_acts = [acts[0]]
    for j, by in ((1, -1), (2, 1), (3, 2)):
        all_acts.append(shifted(acts[j], "y", by))
    far_in, far_cot, back = lax.optimization_barrier((rows_before[0], rows_after[1], back))
    part = combine(tp_vec, placed, back, cotangent)

    near = (part, shifted(part, "y", 1), shifted(part, "y", -1), shifted(part, "y", 2))
    grads = (*near, *(shifted(g, "c", 1) for g in near))
    *pieces, grad_gate_pre, direct, link = project(order, grads, out_proj.T, mixed, gelu, slope, prefix)

    far_in, far_cot, pieces[0] = lax.optimization_barrier((far_in, far_cot, pieces[0]))

    over_x = [pieces[0]]
    for m in (1, 2, 3):
        over_x.append(shifted(pieces[m], "x", m))
    link = jnp.broadcast_to(link, (N_EXP, *link.shape))
    links = lax.all_to_all(link, SP, split_axis=0, concat_axis=0, tiled=True)
    over_x = sum(p.astype(F32) for p in over_x).astype(BF16)
    over_z = lax.all_to_all(over_x, "z", split_axis=0, concat_axis=0, tiled=True)
    grad_proj = over_z.astype(F32).sum(axis=0)

    sp = (4 * lax.axis_index("z") + lax.axis_index("x")).astype(jnp.int32)
    local = local_scan(direct, log_t)
    grad_step_input, grad_log_decay = recur(sp[None], links, local, suffix, log_t, before_t)

    far_in = shifted(far_in, "y", 1)
    far_cot = shifted(far_cot, "y", -1)
    far = (far_in, far_cot)
    keep, send = weight_grads((rows, rows_after, rows_before), far, all_acts)
    send = shifted(send, "c", 1)
    grad_gate, grad_up, grad_down = finish(keep, send)
    return (
        grad_gate[None],
        grad_up[None],
        grad_down[None],
        grad_proj,
        grad_gate_pre.T,
        grad_step_input.T,
        grad_log_decay.T,
    )


def solution(mesh):
    grid = Mesh(mesh.devices.reshape(8, 4, 4, 2), ALL)


    return jax.shard_map(
        on_device,
        mesh=grid,
        in_specs=(
            P(SP, None),
            P(SP, None),
            P(SP, None),
            P(SP, None),
            P(SP, None, TP),
            P(SP, None, TP),
            P(SP, TP, None),
            P(None, TP),
            P(SP, TP),
            P(SP, TP),
            P(SP, TP),
            P(SP, TP),
        ),
        out_specs=(
            P(SP, None, TP),
            P(SP, None, TP),
            P(SP, TP, None),
            P(SP, TP),
            P(SP, TP),
            P(SP, TP),
            P(SP, TP),
        ),
        check_vma=False,
    )
```

```python
import jax
import jax.numpy as jnp
from jax import lax
from jax.experimental import pallas as pl
from jax.experimental.pallas import tpu as pltpu
from jax.sharding import Mesh, PartitionSpec as P


BF16 = jnp.bfloat16
F32 = jnp.float32
SP = ("z", "x")
TP = ("y", "c")
ALL = ("z", "x", "y", "c")

TOK = 384
D = 2048
CAP = 48
N_EXP = 32
N_TP = 8
PART = CAP // N_TP
ROWS = N_EXP * PART
CH = 352
STRIP = 32
GELU_C = 0.7978845608028654
GELU_A = 0.044715


def iota(shape, dim):
    return lax.broadcasted_iota(jnp.int32, shape, dim)


def in_hbm(*arrays):
    held = tuple(pltpu.with_memory_space_constraint(a, pltpu.HBM) for a in arrays)
    return held if len(held) > 1 else held[0]


def vmem(mib):
    return pltpu.CompilerParams(vmem_limit_bytes=mib * 1024 * 1024)


def dot(a, b):
    return jnp.dot(a, b, preferred_element_type=F32)


def dot_nt(a, b):
    return lax.dot_general(a, b, (((1,), (1,)), ((), ())), preferred_element_type=F32)


def dot_tn(a, b):
    return lax.dot_general(a, b, (((0,), (0,)), ((), ())), preferred_element_type=F32)


FIRST = (6, 4, 2)


def pack_kernel(gate_ref, up_ref, down_ref, a_ref, b_ref, abuf, bbuf, down_buf, sems):
    third = D // 2
    loads = [
        pltpu.make_async_copy(down_ref, down_buf, sems.at[0]),
        pltpu.make_async_copy(gate_ref, abuf.at[pl.ds(0, D)], sems.at[1]),
        pltpu.make_async_copy(up_ref.at[pl.ds(0, third)], abuf.at[pl.ds(D, third)], sems.at[2]),
        pltpu.make_async_copy(up_ref.at[pl.ds(third, third)], bbuf.at[pl.ds(0, third)], sems.at[3]),
    ]
    for load in loads:
        load.start()
    loads[1].wait()
    loads[2].wait()
    out_a = pltpu.make_async_copy(abuf, a_ref, sems.at[4])
    out_a.start()
    loads[0].wait()
    bbuf[third:, :] = down_buf[...].T
    loads[3].wait()
    out_b = pltpu.make_async_copy(bbuf, b_ref, sems.at[5])
    out_b.start()
    out_a.wait()
    out_b.wait()


def pack(gate, up, down):
    anywhere = pl.BlockSpec(memory_space=pl.ANY)
    half = pltpu.HBM((3 * D // 2, 128), BF16)
    return pl.pallas_call(
        pack_kernel,
        in_specs=[anywhere] * 3,
        out_specs=(anywhere, anywhere),
        out_shape=(half, half),
        scratch_shapes=[
            pltpu.VMEM((3 * D // 2, 128), BF16),
            pltpu.VMEM((3 * D // 2, 128), BF16),
            pltpu.VMEM((128, D), BF16),
            pltpu.SemaphoreType.DMA((6,)),
        ],
        compiler_params=vmem(4),
        name="pack",
    )(*in_hbm(gate, up, down))


def dispatch_kernel(tp_ref, routes_ref, weight_ref, res_a, res_b, cot_a, cot_b, out_ref, pick_ref, scale_ref):
    @pl.when(pl.program_id(0) == 0)
    def _():
        r0, r1 = routes_ref[0:1, :], routes_ref[1:2, :]
        e = iota((N_EXP, TOK), 0)
        oh0, oh1 = e == r0, e == r1
        member = jnp.where(oh0 | oh1, 1.0, 0.0).astype(BF16)
        before = jnp.where(iota((TOK, TOK), 0) < iota((TOK, TOK), 1), 1.0, 0.0).astype(BF16)
        rank = dot(member, before)
        s0 = r0 * CAP + jnp.sum(jnp.where(oh0, rank, 0.0), axis=0, keepdims=True).astype(jnp.int32)
        s1 = r1 * CAP + jnp.sum(jnp.where(oh1, rank, 0.0), axis=0, keepdims=True).astype(jnp.int32)
        row = iota((8 * N_EXP, TOK), 0)
        q = row & 7
        for j in range(3):
            first = q < FIRST[j]
            i = 8 * j + q - jnp.where(first, 6 * j, 6 * (j + 1))
            slot = (row >> 3) * CAP + PART * tp_ref[0] + i
            m0, m1 = slot == s0, slot == s1
            hit = m0 | m1
            pick_ref[j, :, :TOK] = jnp.where(hit & first, 1.0, 0.0).astype(BF16)
            pick_ref[j, :, TOK:] = jnp.where(hit & ~first, 1.0, 0.0).astype(BF16)
            w = jnp.where(m0, weight_ref[0:1, :], 0.0) + jnp.where(m1, weight_ref[1:2, :], 0.0)
            w = jnp.sum(w, axis=1, keepdims=True)
            cot_row = (q[:, 0:1] < FIRST[j]) if j % 2 else (q[:, 0:1] >= FIRST[j])
            scale_ref[j] = jnp.broadcast_to(jnp.where(cot_row, w, 1.0), (8 * N_EXP, 128))

    classes = (res_a, cot_a, res_b, cot_b)
    for j in range(3):
        rhs = jnp.concatenate([classes[j][...], classes[j + 1][...]], axis=0)
        got = dot(pick_ref[j], rhs) * scale_ref[j][:, 0:1]
        out_ref[:, 8 * j : 8 * j + 8, :] = got.reshape(N_EXP, 8, got.shape[1]).astype(BF16)


def dispatch(tp, routes_t, weight_t, resid, cotangent):
    bn = 256
    half = D // 2 // bn
    return pl.pallas_call(
        dispatch_kernel,
        grid_spec=pltpu.PrefetchScalarGridSpec(
            num_scalar_prefetch=1,
            grid=(half,),
            in_specs=[
                pl.BlockSpec((2, TOK), lambda n, s: (0, 0)),
                pl.BlockSpec((2, TOK), lambda n, s: (0, 0)),
                pl.BlockSpec((TOK, bn), lambda n, s: (0, n)),
                pl.BlockSpec((TOK, bn), lambda n, s: (0, n + half)),
                pl.BlockSpec((TOK, bn), lambda n, s: (0, n)),
                pl.BlockSpec((TOK, bn), lambda n, s: (0, n + half)),
            ],
            out_specs=pl.BlockSpec((N_EXP, 24, bn), lambda n, s: (0, 0, n)),
            scratch_shapes=[
                pltpu.VMEM((3, 8 * N_EXP, 2 * TOK), BF16),
                pltpu.VMEM((3, 8 * N_EXP, 128), F32),
            ],
        ),
        out_shape=pltpu.HBM((N_EXP, 24, D // 2), BF16),
        compiler_params=vmem(14),
        name="dispatch",
    )(tp, routes_t, weight_t, resid, resid, cotangent, cotangent)


def place_kernel(routes_ref, out_ref):
    r0, r1 = routes_ref[:, 0:1], routes_ref[:, 1:2]
    e = iota((TOK, N_EXP), 1)
    oh0, oh1 = e == r0, e == r1
    member = jnp.where(oh0 | oh1, 1.0, 0.0).astype(BF16)
    before = jnp.where(iota((TOK, TOK), 1) < iota((TOK, TOK), 0), 1.0, 0.0).astype(BF16)
    rank = dot(before, member)

    def line(oh, r):
        k = jnp.sum(jnp.where(oh, rank, 0.0), axis=1, keepdims=True).astype(jnp.int32)
        t = (k * 43) >> 8
        return r * 64 + t * 8 + (k - t * PART)

    col = iota((TOK, 8 * N_TP * N_EXP), 1)
    hit = (col == line(oh0, r0)) | (col == line(oh1, r1))
    out_ref[...] = jnp.where(hit, 1.0, 0.0).astype(BF16)


def place(routes):
    return pl.pallas_call(
        place_kernel,
        out_shape=pltpu.HBM((TOK, 8 * N_TP * N_EXP), BF16),
        compiler_params=vmem(8),
        name="place",
    )(routes)


def select_kernel(got_ref, rows_ref):
    tiles = [
        got_ref[:, 8 * j : 8 * j + 8, :].astype(F32).reshape(8 * N_EXP, D // 2).astype(BF16) for j in range(3)
    ]
    k = iota((ROWS, 8 * N_EXP), 0)
    col = iota((ROWS, 8 * N_EXP), 1)
    source, q = col >> 3, col & 7
    for cls in range(4):
        total = None
        for j in (cls - 1, cls):
            if 0 <= j < 3:
                i = 8 * j + q - 6 * cls
                sel = jnp.where((k == source * PART + i) & (i >= 0) & (i < PART), 1.0, 0.0).astype(BF16)
                part = dot(sel, tiles[j])
                total = part if total is None else total + part
        rows_ref[cls % 2, :, (cls // 2) * (D // 2) : (cls // 2 + 1) * (D // 2)] = total.astype(BF16)


def select(got):
    return pl.pallas_call(
        select_kernel,
        out_shape=pltpu.HBM((2, ROWS, D), BF16),
        compiler_params=vmem(12),
        name="select",
    )(got)


def expert_kernel(rows_hbm, *refs):
    weights, out_ref, acts = refs[:16], refs[16], refs[17:21]
    rows_ref, gate_up, down, grads, made, sems, row_sems, act_sems = refs[21:]
    mid = D // 2
    copies = [[], [], [], []]
    for j in range(4):
        for side in range(2):
            part_a, part_b = weights[8 * side + 2 * j], weights[8 * side + 2 * j + 1]
            at = 128 * side
            g, u, d = pl.ds(512 * j + at, 128), pl.ds(512 * j + 256 + at, 128), pl.ds(256 * j + at, 128)
            moves = (
                (part_a.at[pl.ds(0, D)], gate_up.at[:, g]),
                (part_a.at[pl.ds(D, mid)], gate_up.at[pl.ds(0, mid), u]),
                (part_b.at[pl.ds(0, mid)], gate_up.at[pl.ds(mid, mid), u]),
                (part_b.at[pl.ds(mid, D)], down.at[:, d]),
            )
            for n, (src, dst) in enumerate(moves):
                copies[j].append(pltpu.make_async_copy(src, dst, sems.at[j, 4 * side + n]))
    rows_in = [pltpu.make_async_copy(rows_hbm.at[n], rows_ref.at[n], row_sems.at[n]) for n in range(2)]
    acts_out = [pltpu.make_async_copy(made.at[n], acts[n], act_sems.at[n]) for n in range(4)]
    for copy in [rows_in[0], *copies[0], rows_in[1], *copies[1], *copies[2], *copies[3]]:
        copy.start()
    for copy in rows_in:
        copy.wait()

    def chunk(j, _):
        for n in range(4):
            @pl.when(j == n)
            def _():
                for copy in copies[n]:
                    copy.wait()

        at = pl.multiple_of(512 * j, 512)
        both = dot(rows_ref[0], gate_up[:, pl.ds(at, 512)])
        gate, up = both[:, :256], both[:, 256:]
        d_hidden = dot(rows_ref[1], down[:, pl.ds(pl.multiple_of(256 * j, 256), 256)])
        sig = jax.nn.sigmoid(gate)
        silu = gate * sig
        d_gate = (d_hidden * up * (sig * (1.0 + gate * (1.0 - sig)))).astype(BF16)
        d_up = (d_hidden * silu).astype(BF16)
        made[j, 0] = d_gate
        made[j, 1] = d_up
        made[j, 2] = (silu * up).astype(BF16)
        grads[:, pl.ds(at, 256)] = d_gate
        grads[:, pl.ds(pl.multiple_of(at + 256, 256), 256)] = d_up
        return 0

    lax.fori_loop(0, 4, chunk, 0)
    for copy in acts_out:
        copy.start()
    line = iota((8 * N_EXP, ROWS), 0)
    spread = (iota((8 * N_EXP, ROWS), 1) == (line >> 3) * PART + (line & 7)) & ((line & 7) < PART)
    spread = jnp.where(spread, 1.0, 0.0).astype(BF16)

    def columns(t, _):
        rows = pl.ds(pl.multiple_of(256 * t, 256), 256)
        back = dot(spread, dot_nt(grads[...], gate_up[rows, :]).astype(BF16)).reshape(N_EXP, 8, 256)
        for h in range(2):
            out_ref[:, t, 8 * h : 8 * h + 8, :] = back[:, :, 128 * h : 128 * h + 128].astype(BF16)
        return 0

    lax.fori_loop(0, N_TP, columns, 0)
    for copy in acts_out:
        copy.wait()


def experts(rows, weights):
    act = pltpu.HBM((3, ROWS, 256), BF16)
    anywhere = pl.BlockSpec(memory_space=pl.ANY)
    return pl.pallas_call(
        expert_kernel,
        in_specs=[anywhere] * 17,
        out_specs=(pl.BlockSpec(memory_space=pltpu.VMEM), anywhere, anywhere, anywhere, anywhere),
        out_shape=(pltpu.HBM((N_EXP, N_TP, 16, 128), BF16), act, act, act, act),
        scratch_shapes=[
            pltpu.VMEM((2, ROWS, D), BF16),
            pltpu.VMEM((D, D), BF16),
            pltpu.VMEM((D, D // 2), BF16),
            pltpu.VMEM((ROWS, D), BF16),
            pltpu.VMEM((4, 3, ROWS, 256), BF16),
            pltpu.SemaphoreType.DMA((4, 8)),
            pltpu.SemaphoreType.DMA((2,)),
            pltpu.SemaphoreType.DMA((4,)),
        ],
        compiler_params=vmem(32),
        name="experts",
    )(*in_hbm(rows, *weights))


def weight_grad_kernel(rows_0, rows_1, rows_2, far_in, far_cot, act_0, act_1, act_2, act_3,
                       keep_ref, send_ref, hbuf, turned):
    @pl.when(pl.program_id(0) == 0)
    def _():
        for n, act in enumerate((act_0, act_1, act_2, act_3)):
            for k in range(3):
                hbuf[ROWS * n : ROWS * (n + 1), 256 * k : 256 * (k + 1)] = act[k]
        turned[...] = hbuf[:, 512:].T

    near = (rows_0, rows_1, rows_2)
    both = dot_tn(jnp.concatenate([*(r[0] for r in near), far_in[...]], axis=0), hbuf[:, :512])
    for n in range(2):
        keep_ref[n] = both[:, 256 * n : 256 * n + 128]
        send_ref[n] = both[:, 256 * n + 128 : 256 * n + 256].astype(BF16)
    both = dot(turned[...], jnp.concatenate([*(r[1] for r in near), far_cot[...]], axis=0))
    for h in range(both.shape[1] // 128):
        at = slice(128 * h, 128 * h + 128)
        keep_ref[2, at, :] = both[:128, at]
        send_ref[2, at, :] = both[128:, at].astype(BF16)


def weight_grads(rows, far, acts):
    block = 512
    sums = pl.BlockSpec((3, block, 128), lambda t: (0, t, 0))
    return pl.pallas_call(
        weight_grad_kernel,
        grid=(D // block,),
        in_specs=[pl.BlockSpec((2, ROWS, block), lambda t: (0, 0, t))] * 3
        + [pl.BlockSpec((ROWS, block), lambda t: (0, t))] * 2
        + [pl.BlockSpec((3, ROWS, 256), lambda t: (0, 0, 0))] * 4,
        out_specs=(sums, sums),
        out_shape=(pltpu.HBM((3, D, 128), F32), pltpu.HBM((3, D, 128), BF16)),
        scratch_shapes=[
            pltpu.VMEM((4 * ROWS, 768), BF16),
            pltpu.VMEM((256, 4 * ROWS), BF16),
        ],
        compiler_params=vmem(20),
        name="weight_grads",
    )(*rows, *far, *acts)


def finish_kernel(keep_ref, got_ref, gate_ref, up_ref, down_ref):
    gate_ref[...] = keep_ref[0] + got_ref[0].astype(F32)
    up_ref[...] = keep_ref[1] + got_ref[1].astype(F32)
    for n in range(keep_ref.shape[1] // 128):
        at = slice(128 * n, 128 * n + 128)
        down_ref[:, at] = keep_ref[2, at, :] + got_ref[2, at, :].astype(F32)


def finish(keep, got):
    block = 512
    sums = pl.BlockSpec((3, block, 128), lambda t: (0, t, 0))
    tall = pl.BlockSpec((block, 128), lambda t: (t, 0))
    return pl.pallas_call(
        finish_kernel,
        grid=(D // block,),
        in_specs=[sums, sums],
        out_specs=(tall, tall, pl.BlockSpec((128, block), lambda t: (0, t))),
        out_shape=(
            jax.ShapeDtypeStruct((D, 128), F32),
            jax.ShapeDtypeStruct((D, 128), F32),
            jax.ShapeDtypeStruct((128, D), F32),
        ),
        compiler_params=vmem(8),
        name="finish",
    )(in_hbm(keep), got)


def combine_kernel(tp_ref, place_ref, back_ref, cot_ref, out_ref):
    halves = [
        back_ref[:, 8 * h : 8 * h + 8, :].astype(F32).reshape(8 * N_TP * N_EXP, 128).astype(BF16) for h in range(2)
    ]
    routed = dot(place_ref[...], jnp.concatenate(halves, axis=1))
    out_ref[...] = (cot_ref[...].astype(F32) + routed).T.astype(BF16)


def combine(tp, placed, back, cotangent):
    cols = D // N_TP
    return pl.pallas_call(
        combine_kernel,
        grid_spec=pltpu.PrefetchScalarGridSpec(
            num_scalar_prefetch=1,
            grid=(1,),
            in_specs=[
                pl.BlockSpec(placed.shape, lambda n, s: (0, 0)),
                pl.BlockSpec(back.shape, lambda n, s: (0, 0, 0)),
                pl.BlockSpec((TOK, cols), lambda n, s: (0, s[0])),
            ],
            out_specs=pl.BlockSpec((cols, TOK), lambda n, s: (0, 0)),
        ),
        out_shape=jax.ShapeDtypeStruct((cols, TOK), BF16),
        compiler_params=vmem(12),
        name="combine",
    )(tp, in_hbm(placed), back, cotangent)


def prepare_kernel(gate_ref, log_ref, before_ref, step_ref, mixed_ref, gelu_ref, slope_ref, prefix_ref, suffix_ref, turn_ref):
    lane = iota((STRIP, TOK), 1)
    turn_ref[...] = jnp.zeros_like(turn_ref)

    def strip(n, _):
        at = pl.ds(pl.multiple_of(n * STRIP, STRIP), STRIP)
        x = gate_ref[at, :].astype(F32)
        th = jnp.tanh(GELU_C * (x + GELU_A * (x * x * x)))
        gelu = 0.5 * x * (1.0 + th)
        back = 0.5 * (1.0 + th) + 0.5 * x * (1.0 - th * th) * (GELU_C * (1.0 + 3.0 * GELU_A * (x * x)))
        logs = log_ref[at, :]
        states = jnp.exp(logs) * before_ref[at, :] + step_ref[at, :].astype(F32)
        turn_ref[at, :] = gelu * states
        gelu_ref[at, :] = gelu
        slope_ref[at, :] = states * back
        total = logs
        d = 1
        while d < TOK:
            total = total + jnp.where(lane >= d, pltpu.roll(total, d, 1), 0.0)
            d *= 2
        prefix_ref[at, :] = jnp.exp(total)
        suffix_ref[at, :] = jnp.exp(total[:, TOK - 1 : TOK] - total)
        return 0

    lax.fori_loop(0, CH // STRIP, strip, 0)
    mixed_ref[...] = turn_ref[...].T[:, :CH].astype(BF16)


def prepare(gate_pre, log_decay, state_before, step_input):
    shape = gate_pre.shape
    wide = pltpu.HBM(shape, F32)
    return pl.pallas_call(
        prepare_kernel,
        out_shape=(pltpu.HBM(shape[::-1], BF16), wide, wide, wide, wide),
        scratch_shapes=[pltpu.VMEM((TOK, TOK), F32)],
        compiler_params=vmem(8),
        name="prepare",
    )(gate_pre, log_decay, state_before, step_input)


def project_kernel(order_ref, *refs):
    grads, (proj_ref, mixed_ref, gelu_ref, slope_ref, prefix_ref) = refs[:8], refs[8:13]
    pieces, (ggp_ref, direct_ref, link_ref, block_ref, turn_ref) = refs[13:17], refs[17:]
    d_mixed = jnp.zeros((CH, TOK), F32)
    for k in range(N_TP):
        group = order_ref[k]
        grad = grads[k][...]
        cols = pl.ds(pl.multiple_of(group * 256, 256), 256)
        d_mixed = d_mixed + dot(proj_ref[:, cols], grad)
        block_ref[...] = dot(grad, mixed_ref[...])
        for m in range(4):
            at = pl.ds(pl.multiple_of(((order_ref[8] + m) & 3) * 64, 64), 64)
            pieces[m][pl.ds(group, 1)] = block_ref[at, :].astype(BF16)[None]
    ggp_ref[...] = (d_mixed * slope_ref[...]).astype(BF16)
    direct = d_mixed * gelu_ref[...]
    direct_ref[...] = direct
    turn_ref[...] = jnp.zeros_like(turn_ref)
    turn_ref[0:CH, 0:1] = prefix_ref[:, TOK - 1 : TOK]
    turn_ref[0:CH, 1:2] = jnp.sum(prefix_ref[...] * direct, axis=1, keepdims=True)
    link_ref[...] = turn_ref[...].T[0:2, 0:CH]


def project(order, grads, out_proj, mixed, gelu, slope, prefix):
    piece = pltpu.HBM((8, 64, CH), BF16)
    return pl.pallas_call(
        project_kernel,
        in_specs=[pl.BlockSpec(memory_space=pltpu.SMEM)] + [pl.BlockSpec(memory_space=pltpu.VMEM)] * 13,
        out_shape=(
            piece, piece, piece, piece,
            pltpu.HBM((CH, TOK), BF16),
            pltpu.HBM((CH, TOK), F32),
            pltpu.HBM((2, CH), F32),
        ),
        scratch_shapes=[pltpu.VMEM((256, CH), F32), pltpu.VMEM((TOK, 128), F32)],
        compiler_params=vmem(14),
        name="project",
    )(order, *grads, out_proj, mixed, gelu, slope, prefix)


def local_kernel(direct_ref, log_ref, out_ref):
    lane = iota((STRIP, TOK), 1)

    def strip(n, _):
        at = pl.ds(pl.multiple_of(n * STRIP, STRIP), STRIP)
        a = jnp.where(lane < TOK - 1, pltpu.roll(jnp.exp(log_ref[at, :]), TOK - 1, 1), 1.0)
        b = direct_ref[at, :]
        d = 1
        while d < TOK:
            b = b + a * jnp.where(lane < TOK - d, pltpu.roll(b, TOK - d, 1), 0.0)
            if 2 * d < TOK:
                a = a * jnp.where(lane < TOK - d, pltpu.roll(a, TOK - d, 1), 1.0)
            d *= 2
        out_ref[at, :] = b
        return 0

    lax.fori_loop(0, CH // STRIP, strip, 0)


def local_scan(direct, log_decay):
    return pl.pallas_call(
        local_kernel,
        out_shape=jax.ShapeDtypeStruct((CH, TOK), F32),
        compiler_params=vmem(6),
        name="local_scan",
    )(in_hbm(direct), log_decay)


def recur_kernel(at_ref, links_ref, local_ref, suffix_ref, log_ref, before_ref, step_ref, decay_ref, turn_ref):
    mine = at_ref[0]
    arriving = jnp.zeros((1, CH), F32)
    for s in range(N_EXP - 1, 0, -1):
        arriving = jnp.where(s > mine, links_ref[s, 1:2, :] + links_ref[s, 0:1, :] * arriving, arriving)
    turn_ref[...] = jnp.zeros_like(turn_ref)
    turn_ref[0:1, 0:CH] = arriving
    column = turn_ref[...].T[:CH, 0:1]
    g = local_ref[...] + suffix_ref[...] * column
    step_ref[...] = g
    decay_ref[...] = g * jnp.exp(log_ref[...]) * before_ref[...]


def recur(at, links, local, suffix, log_decay, state_before):
    return pl.pallas_call(
        recur_kernel,
        in_specs=[pl.BlockSpec(memory_space=pltpu.SMEM)] + [pl.BlockSpec(memory_space=pltpu.VMEM)] * 5,
        out_shape=(
            jax.ShapeDtypeStruct((CH, TOK), F32),
            jax.ShapeDtypeStruct((CH, TOK), F32),
        ),
        scratch_shapes=[pltpu.VMEM((128, TOK), F32)],
        compiler_params=vmem(8),
        name="recur",
    )(at, links, local, in_hbm(suffix), log_decay, state_before)


def shifted(value, axis, by):
    n = lax.axis_size(axis)
    return lax.ppermute(value, axis, [(i, (i + by) % n) for i in range(n)])


def on_device(resid, cotangent, routes, route_weight, w_gate, w_up, w_down, out_proj, gate_pre, log_decay,
              state_before, step_input):
    y, c = lax.axis_index("y"), lax.axis_index("c")
    tp = (2 * y + c).astype(jnp.int32)
    tp_vec = tp[None]

    own_a, own_b = pack(w_gate[0], w_up[0], w_down[0])
    prev_a = shifted(own_a, "y", 1)
    next_b = shifted(own_b, "y", -1)
    prev_b = shifted(own_b, "y", 1)
    next_a = shifted(own_a, "y", -1)
    far_a = shifted(prev_a, "y", 1)
    far_b = shifted(next_b, "y", -1)
    mine = (own_a, own_b, prev_a, prev_b, next_a, next_b, far_a, far_b)
    weights = mine + tuple(shifted(w, "c", 1) for w in mine)

    sent = dispatch(tp_vec, routes.T, route_weight.T, resid, cotangent)
    got = lax.all_to_all(sent, SP, split_axis=0, concat_axis=0, tiled=True)

    placed = place(routes)
    log_t, before_t = log_decay.T, state_before.T
    mixed, gelu, slope, prefix, suffix = prepare(gate_pre.T, log_t, before_t, step_input.T)
    ys = jnp.stack([y, y - 1, y + 1, y + 2]) % 4
    order = jnp.concatenate([2 * ys + c, 2 * ys + 1 - c, lax.axis_index("x")[None]]).astype(jnp.int32)
    got, order = lax.optimization_barrier((got, order))

    rows = select(got)
    rows_after = shifted(rows, "y", -1)
    rows_before = shifted(rows, "y", 1)
    back, *acts = experts(rows, weights)
    back = lax.all_to_all(back.reshape(N_EXP * N_TP, 16, 128), ALL, split_axis=0, concat_axis=0, tiled=True)
    all_acts = [acts[0]]
    for j, by in ((1, -1), (2, 1), (3, 2)):
        all_acts.append(shifted(acts[j], "y", by))
    far_in, far_cot, back = lax.optimization_barrier((rows_before[0], rows_after[1], back))
    part = combine(tp_vec, placed, back, cotangent)

    near = (part, shifted(part, "y", 1), shifted(part, "y", -1), shifted(part, "y", 2))
    grads = (*near, *(shifted(g, "c", 1) for g in near))
    *pieces, grad_gate_pre, direct, link = project(order, grads, out_proj.T, mixed, gelu, slope, prefix)

    far_in, far_cot, pieces[0] = lax.optimization_barrier((far_in, far_cot, pieces[0]))

    over_x = [pieces[0]]
    for m in (1, 2, 3):
        over_x.append(shifted(pieces[m], "x", m))
    link = jnp.broadcast_to(link, (N_EXP, *link.shape))
    links = lax.all_to_all(link, SP, split_axis=0, concat_axis=0, tiled=True)
    over_x = sum(p.astype(F32) for p in over_x).astype(BF16)
    over_z = lax.all_to_all(over_x, "z", split_axis=0, concat_axis=0, tiled=True)
    grad_proj = over_z.astype(F32).sum(axis=0)

    sp = (4 * lax.axis_index("z") + lax.axis_index("x")).astype(jnp.int32)
    local = local_scan(direct, log_t)
    grad_step_input, grad_log_decay = recur(sp[None], links, local, suffix, log_t, before_t)

    far_in = shifted(far_in, "y", 1)
    far_cot = shifted(far_cot, "y", -1)
    far = (far_in, far_cot)
    keep, send = weight_grads((rows, rows_after, rows_before), far, all_acts)
    send = shifted(send, "c", 1)
    grad_gate, grad_up, grad_down = finish(keep, send)
    return (
        grad_gate[None],
        grad_up[None],
        grad_down[None],
        grad_proj,
        grad_gate_pre.T,
        grad_step_input.T,
        grad_log_decay.T,
    )


def solution(mesh):
    grid = Mesh(mesh.devices.reshape(8, 4, 4, 2), ALL)


    return jax.shard_map(
        on_device,
        mesh=grid,
        in_specs=(
            P(SP, None),
            P(SP, None),
            P(SP, None),
            P(SP, None),
            P(SP, None, TP),
            P(SP, None, TP),
            P(SP, TP, None),
            P(None, TP),
            P(SP, TP),
            P(SP, TP),
            P(SP, TP),
            P(SP, TP),
        ),
        out_specs=(
            P(SP, None, TP),
            P(SP, None, TP),
            P(SP, TP, None),
            P(SP, TP),
            P(SP, TP),
            P(SP, TP),
            P(SP, TP),
        ),
        check_vma=False,
    )
```
